32 devices in a mesh: sp: 4 (over z), fs: 4 (over y, x), tp: 2 (over core).
Axes of the slice: x: 2, y: 2, z: 4, core: 2. Of those that a mesh axis runs over, the one named last changes fastest.
Arguments:
- tokens: bfloat16 [4, 1024, 2048], P('fs', 'sp'), may hold values from -6 to 6
- norm_gain: float32 [2048], replicated, may hold values from 0.1 to 1.9
- query_weight: bfloat16 [2048, 1024], P(('sp', 'fs'), 'tp'), may hold values from -0.125 to 0.125
- key_weight: bfloat16 [2048, 1024], P(('sp', 'fs'), 'tp'), may hold values from -0.125 to 0.125
- value_weight: bfloat16 [2048, 1024], P(('sp', 'fs'), 'tp'), may hold values from -0.125 to 0.125
- outgate_weight: bfloat16 [2048, 1024], P(('sp', 'fs'), 'tp'), may hold values from -0.125 to 0.125
- gate_weight: bfloat16 [4, 8, 2048], P(None, 'tp'), may hold values from -0.125 to 0.125
- gate_bias: float32 [4, 8], P(None, 'tp'), may hold values from -1 to 100
- decay_extra: float32 [4, 2, 8, 1024], P('fs', None, 'tp', 'sp'), may hold values from -0.75 to 0
- init_memory: float32 [4, 2, 8, 128, 128], P('fs', None, 'tp'), may hold values from -48 to 48
- init_normalizer: float32 [4, 2, 8, 128], P('fs', None, 'tp'), may hold values from -48 to 48
- head_gain: float32 [8, 128], P('tp'), may hold values from 0.1 to 1.9
- pool_weight: bfloat16 [2048, 2048], P(('sp', 'fs'), 'tp'), may hold values from -0.125 to 0.125
- mem_out_weight: bfloat16 [2048, 1024], P(('sp', 'fs'), 'tp'), may hold values from -0.1875 to 0.1875
- pool_out_weight: bfloat16 [2048, 2048], P(('sp', 'fs'), 'tp'), may hold values from -0.125 to 0.125
Outputs:
- mixed: bfloat16 [4, 1024, 2048], P('fs', ('sp', 'tp'))
The draws below stay inside these ranges and needn't reach their ends.
All inputs are finite; a program needn't handle non-finite values.
Results may differ from the reference program's by a relative error of at most 0.014.
Values may be sent and summed in bfloat16 or wider, within the bound.
A program may use at most 64 MiB of HBM per device.

```python
import math
from functools import partial
import jax
import jax.numpy as jnp
from jax import lax

D = 2048
MEMORY_HEADS = 8
HEAD_DIM = 128
HALO = 8
T_DEV = 256
MEM_W = 1024
TOKEN_LENGTH = 1024
SEQUENCE_COUNT = 4
N_TP = 2


def draw_gate_bias(key, part):
    rank_key, slow_key, fast_key, input_key, pick_key, strong_key = jax.random.split(key, 6)
    ranking = jax.random.permutation(rank_key, MEMORY_HEADS)
    picking = jax.random.permutation(pick_key, MEMORY_HEADS)
    slow_heads = ranking < MEMORY_HEADS // 2
    strong_heads = picking < 0
    slow_bias = math.log(3.3 * TOKEN_LENGTH) + jax.random.uniform(slow_key, (2, MEMORY_HEADS), jnp.float32, 0.0, 0.5)
    fast_bias = jax.random.uniform(fast_key, (2, MEMORY_HEADS), jnp.float32, math.log(50.0), math.log(165.0))
    forget_bias = jnp.where(slow_heads[None, :], slow_bias, fast_bias)
    gentle = jax.random.uniform(input_key, (2, MEMORY_HEADS), jnp.float32, -1.0, 1.0)
    strong_bias = jax.random.uniform(strong_key, (2, MEMORY_HEADS), jnp.float32, 80.0, 100.0)
    input_bias = jnp.where(strong_heads[None, :], strong_bias, gentle)
    return jnp.stack([input_bias[0], forget_bias[0], input_bias[1], forget_bias[1]]).astype(jnp.float32)


def draw_decay_extra(key, part):
    speed_key, spike_key, penalty_key = jax.random.split(key, 3)
    block_count = TOKEN_LENGTH // T_DEV
    rates = jnp.exp(jax.random.uniform(speed_key, (SEQUENCE_COUNT, 2, MEMORY_HEADS, block_count), jnp.float32, math.log(0.25), math.log(2.0)))
    stable_values = -0.5 / TOKEN_LENGTH * jnp.repeat(rates, T_DEV, axis=-1)
    spike_values = jax.random.bernoulli(spike_key, 2.0 / TOKEN_LENGTH, (SEQUENCE_COUNT, 2, MEMORY_HEADS, TOKEN_LENGTH))
    penalty_values = jax.random.uniform(penalty_key, (SEQUENCE_COUNT, 2, MEMORY_HEADS, TOKEN_LENGTH), jnp.float32, math.log(0.5), math.log(0.8))
    return (stable_values + jnp.where(spike_values, penalty_values, 0.0)).astype(jnp.float32)


def shard_levels(rng, shape, shards, least, high):
    def one(position, shards_of):
        steps = jax.random.uniform(jax.random.fold_in(jax.random.fold_in(rng, 6), position), (shards_of,), jnp.float32, least / len(shards), high / len(shards))
        return jnp.repeat(jnp.exp(steps), shape[position] // shards_of).reshape((-1,) + (1,) * (len(shape) - position - 1))

    level = one(*shards[0])
    for cut in shards[1:]:
        level = level * one(*cut)
    return level


def gaussian(key, extent, spread, bound, cuts=(), held_as=jnp.bfloat16):
    gain = shard_levels(key, extent, cuts, -0.22, 0.18) if cuts else 1.0
    drawn = jax.random.normal(key, extent, jnp.float32) * spread * gain
    return jnp.minimum(jnp.maximum(drawn, -bound), bound).astype(held_as)


def setup_inputs(seed: int = 0) -> dict:
    streams_of = jax.random.split(jax.random.key(seed), 16)
    tokens = gaussian(streams_of[0], (SEQUENCE_COUNT, TOKEN_LENGTH, D), 1.0, 6.0, ((0, 4), (1, 4)))
    norm_gain = jnp.clip(1.0 + 0.18 * jax.random.normal(streams_of[1], (D,), jnp.float32), 0.1, 1.9)
    query_weight = gaussian(streams_of[2], (D, MEM_W), D ** -0.5, 0.125, ((0, 16), (1, 2)))
    key_weight = gaussian(streams_of[3], (D, MEM_W), D ** -0.5, 0.125, ((0, 16), (1, 2)))
    value_weight = gaussian(streams_of[4], (D, MEM_W), D ** -0.5, 0.125, ((0, 16), (1, 2)))
    outgate_weight = gaussian(streams_of[5], (D, MEM_W), D ** -0.5, 0.125, ((0, 16), (1, 2)))
    gate_weight = gaussian(streams_of[6], (4, MEMORY_HEADS, D), D ** -0.5, 0.125, ((1, 2),))
    gate_bias = draw_gate_bias(jax.random.fold_in(streams_of[15], 71), 0)
    decay_extra = draw_decay_extra(jax.random.fold_in(streams_of[15], 71), 0)
    init_memory = gaussian(streams_of[9], (SEQUENCE_COUNT, 2, MEMORY_HEADS, HEAD_DIM, HEAD_DIM), (0.25 * TOKEN_LENGTH ** 0.5), 48.0, ((0, 4), (2, 2)), jnp.float32)
    init_normalizer = gaussian(streams_of[10], (SEQUENCE_COUNT, 2, MEMORY_HEADS, HEAD_DIM), (0.25 * TOKEN_LENGTH ** 0.5), 48.0, ((0, 4), (2, 2)), jnp.float32)
    head_gain = jnp.clip(1.0 + 0.18 * jax.random.normal(streams_of[11], (MEMORY_HEADS, HEAD_DIM), jnp.float32), 0.1, 1.9)
    pool_weight = gaussian(streams_of[12], (D, D), D ** -0.5, 0.125, ((0, 16), (1, 2)))
    mem_out_weight = gaussian(streams_of[13], (D, MEM_W), MEM_W ** -0.5, 0.1875, ((0, 16), (1, 2)))
    pool_out_weight = gaussian(streams_of[14], (D, D), D ** -0.5, 0.125, ((0, 16), (1, 2)))
    return dict(tokens=tokens, norm_gain=norm_gain, query_weight=query_weight, key_weight=key_weight, value_weight=value_weight, outgate_weight=outgate_weight, gate_weight=gate_weight, gate_bias=gate_bias, decay_extra=decay_extra, init_memory=init_memory, init_normalizer=init_normalizer, head_gain=head_gain, pool_weight=pool_weight, mem_out_weight=mem_out_weight, pool_out_weight=pool_out_weight)


norm_eps = 1e-06
exact_mode = lax.Precision.HIGHEST

def block_output(query_rows, key_rows, value_rows, input_gate, log_forget, memory, normalizer, stabilizer):
    block_len = query_rows.shape[1]
    key_scale = key_rows.shape[-1] ** (-0.5)
    lower_mask = jnp.tril(jnp.ones((block_len, block_len), dtype=bool))
    summed = jnp.cumsum(log_forget, axis=-1)
    log_decay = jnp.where(lower_mask, summed[:, :, None] - summed[:, None, :] + input_gate[:, None, :], -jnp.inf)
    log_carry = stabilizer[:, None] + summed
    running_max = jnp.maximum(log_carry, lax.optimization_barrier(jnp.max(log_decay, axis=-1)))
    query_wide = query_rows.astype(jnp.float32)
    scores = jnp.einsum('btd,bsd->bts', query_wide, key_rows.astype(jnp.float32), precision=exact_mode) * key_scale
    inner_weight = jnp.exp(log_decay - running_max[:, :, None]) * scores
    weight_rounded = lax.optimization_barrier(inner_weight.astype(jnp.bfloat16))
    carry_weight = jnp.exp(log_carry - running_max)
    numerator = carry_weight[:, :, None] * jnp.einsum('bed,btd->bte', memory, query_wide, precision=exact_mode)
    numerator = numerator + jnp.einsum('bts,bse->bte', weight_rounded.astype(jnp.float32), value_rows.astype(jnp.float32), precision=exact_mode)
    denominator = carry_weight * jnp.einsum('bd,btd->bt', normalizer, query_wide, precision=exact_mode)
    denominator = denominator + lax.optimization_barrier(jnp.sum(inner_weight, axis=-1))
    return numerator / jnp.maximum(jnp.abs(denominator), jnp.exp(-running_max))[:, :, None]

def block_summary(key_rows, value_rows, input_gate, log_forget):
    key_wide = key_rows.astype(jnp.float32) * key_rows.shape[-1] ** (-0.5)
    summed = jnp.cumsum(log_forget, axis=-1)
    forget_total = summed[:, -1]
    log_weight = forget_total[:, None] - summed + input_gate
    running_max = lax.optimization_barrier(jnp.max(log_weight, axis=-1))
    weights = jnp.exp(log_weight - running_max[:, None])
    memory = jnp.einsum('bse,bsd->bed', weights[:, :, None] * value_rows.astype(jnp.float32), key_wide, precision=exact_mode)
    normalizer = jnp.einsum('bs,bsd->bd', weights, key_wide, precision=exact_mode)
    return (memory, normalizer, running_max, forget_total)

def combine(earlier, latter):
    early_memory, early_norm, early_max, early_total = earlier
    late_memory, late_norm, late_max, late_total = latter
    joint_max = jnp.maximum(early_max + late_total, late_max)
    early_scale = jnp.exp(early_max + late_total - joint_max)
    late_scale = jnp.exp(late_max - joint_max)
    memory = early_scale[:, None, None] * early_memory + late_scale[:, None, None] * late_memory
    normalizer = early_scale[:, None] * early_norm + late_scale[:, None] * late_norm
    return (memory, normalizer, joint_max, early_total + late_total)

def span_sweep(query_rows, key_rows, value_rows, input_gate, log_forget, memory, normalizer, stabilizer, span):
    block_count = query_rows.shape[1] // span

    def to_blocks(array):
        shaped = array.reshape((array.shape[0], block_count, span) + array.shape[2:])
        return jnp.moveaxis(shaped, 1, 0)

    def advance(carried, pieces):
        query_blk, key_blk, value_blk, gate_blk, forget_blk = pieces
        result = block_output(query_blk, key_blk, value_blk, gate_blk, forget_blk, carried[0], carried[1], carried[2])
        return (combine(carried, block_summary(key_blk, value_blk, gate_blk, forget_blk)), result)
    initial = (memory, normalizer, stabilizer, jnp.zeros_like(stabilizer))
    ignored, outputs = lax.scan(advance, initial, tuple((to_blocks(array) for array in (query_rows, key_rows, value_rows, input_gate, log_forget))))
    return jnp.moveaxis(outputs, 0, 1).reshape(query_rows.shape[:2] + (value_rows.shape[2],))

def direction_sweep(query_rows, key_rows, value_rows, input_gate, log_forget, memory, normalizer):
    zero_rows = jnp.zeros((memory.shape[0],), jnp.float32)
    return span_sweep(query_rows, key_rows, value_rows, input_gate, log_forget, memory, normalizer, zero_rows, math.gcd(T_DEV, 256))

def reverse_time(array):
    return jnp.flip(array, axis=1)

def pool_window(padded, positions, channels, seq_len, group_size):
    row_count = positions.shape[0]
    group_index = channels // group_size
    reach_left = jnp.left_shift(jnp.ones_like(group_index), group_index)
    reach_right = reach_left - 1
    window_sum = jnp.zeros((row_count, channels.shape[0]), jnp.float32)
    for offset in range(-HALO, HALO):
        inside = ((offset >= -reach_left) & (offset <= reach_right)).astype(jnp.float32)
        window_sum = window_sum + inside * padded[HALO + offset:HALO + offset + row_count]
    first_pos = jnp.maximum(positions[:, None] - reach_left[None, :], 0)
    last_pos = jnp.minimum(positions[:, None] + reach_right[None, :], seq_len - 1)
    counted = (last_pos - first_pos + 1).astype(jnp.float32)
    centre = padded[HALO:HALO + row_count]
    return (window_sum / counted - centre).astype(jnp.bfloat16)

def output_project(memory_out, pool_out, mem_out_weight, pool_out_weight):
    row_count = memory_out.shape[0]
    model_width = pool_out.shape[1]

    def grouped(matrix):
        return jnp.moveaxis(matrix.reshape(matrix.shape[0], N_TP, matrix.shape[1] // N_TP), 1, 0)

    def accumulate(running, pieces):
        mem_rows, pool_rows, mem_cols, pool_cols = pieces
        group_sum = lax.dot_general(mem_rows, mem_cols, (((1,), (1,)), ((), ())), preferred_element_type=jnp.float32)
        group_sum = group_sum + lax.dot_general(pool_rows, pool_cols, (((1,), (1,)), ((), ())), preferred_element_type=jnp.float32)
        rounded = lax.optimization_barrier(group_sum.astype(jnp.bfloat16))
        return (running + rounded.astype(jnp.float32), None)
    running, ignored = lax.scan(accumulate, jnp.zeros((row_count, model_width), jnp.float32), (grouped(memory_out), grouped(pool_out), grouped(mem_out_weight), grouped(pool_out_weight)))
    return running.astype(jnp.bfloat16)

def reference(tokens, norm_gain, query_weight, key_weight, value_weight, outgate_weight, gate_weight, gate_bias, decay_extra, init_memory, init_normalizer, head_gain, pool_weight, mem_out_weight, pool_out_weight):
    seq_count, seq_len, model_width = tokens.shape
    head_count, head_width = head_gain.shape
    flattened = tokens.reshape(seq_count * seq_len, model_width).astype(jnp.float32)
    normed = (flattened * lax.rsqrt(lax.optimization_barrier(jnp.mean(flattened * flattened, axis=-1, keepdims=True)) + norm_eps) * norm_gain).astype(jnp.bfloat16)

    def project(weight):
        return jnp.dot(normed, weight, preferred_element_type=jnp.float32).astype(jnp.bfloat16)
    query_proj = project(query_weight)
    key_proj = project(key_weight)
    value_proj = project(value_weight)
    outgate = project(outgate_weight)
    pool_input = project(pool_weight)
    gate_pre = lax.dot_general(normed, gate_weight.reshape(4 * head_count, model_width), (((1,), (1,)), ((), ())), preferred_element_type=jnp.float32) + gate_bias.reshape(4 * head_count)
    gate_pre = gate_pre.reshape(seq_count, seq_len, 4, head_count).transpose(2, 0, 3, 1).reshape(4, seq_count * head_count, seq_len)

    def to_heads(matrix):
        shaped = matrix.reshape(seq_count, seq_len, head_count, head_width).transpose(0, 2, 1, 3)
        return shaped.reshape(seq_count * head_count, seq_len, head_width)
    query_heads = to_heads(query_proj)
    key_heads = to_heads(key_proj)
    value_heads = to_heads(value_proj)
    extra_decay = decay_extra.transpose(1, 0, 2, 3).reshape(2, seq_count * head_count, seq_len)
    forward_forget = jax.nn.log_sigmoid(gate_pre[1]) + extra_decay[0]
    backward_forget = jax.nn.log_sigmoid(gate_pre[3]) + extra_decay[1]
    start_memory = init_memory.reshape(seq_count, 2, head_count, head_width, head_width)
    start_norm = init_normalizer.reshape(seq_count, 2, head_count, head_width)
    forward = direction_sweep(query_heads, key_heads, value_heads, gate_pre[0], forward_forget, start_memory[:, 0].reshape(-1, head_width, head_width), start_norm[:, 0].reshape(-1, head_width))
    backward = reverse_time(direction_sweep(reverse_time(query_heads), reverse_time(key_heads), reverse_time(value_heads), reverse_time(gate_pre[2]), reverse_time(backward_forget), start_memory[:, 1].reshape(-1, head_width, head_width), start_norm[:, 1].reshape(-1, head_width)))
    summed_dirs = (forward + backward).reshape(seq_count, head_count, seq_len, head_width).transpose(0, 2, 1, 3)
    summed_dirs = summed_dirs.reshape(seq_count * seq_len, head_count, head_width)
    normed_heads = summed_dirs * lax.rsqrt(lax.optimization_barrier(jnp.mean(summed_dirs * summed_dirs, axis=-1, keepdims=True)) + norm_eps) * head_gain
    out_gate = jax.nn.sigmoid(outgate.astype(jnp.float32).reshape(seq_count * seq_len, head_count, head_width))
    memory_out = (normed_heads * out_gate).astype(jnp.bfloat16).reshape(seq_count * seq_len, head_count * head_width)
    padded = jnp.pad(pool_input.reshape(seq_count, seq_len, model_width).astype(jnp.float32), ((0, 0), (HALO, HALO), (0, 0)))
    window_fn = partial(pool_window, positions=jnp.arange(seq_len, dtype=jnp.int32), channels=jnp.arange(model_width, dtype=jnp.int32), seq_len=seq_len, group_size=model_width // 4)
    pool_out = jax.vmap(window_fn)(padded).reshape(seq_count * seq_len, model_width)
    mixed = output_project(memory_out, pool_out, mem_out_weight, pool_out_weight)
    return mixed.reshape(seq_count, seq_len, model_width)
```

```python
import functools
import math

import jax
import jax.numpy as jnp
from jax import lax
from jax.experimental import pallas as pl
from jax.experimental.pallas import tpu as pltpu
from jax.sharding import PartitionSpec as P

MESH = pl.DeviceIdType.MESH

HALO = 8


norm_eps = 1e-06
exact_mode = lax.Precision.HIGHEST


def carried_in(x, axis, combine, identity, reverse):
    length, position = (lax.axis_size(axis), lax.axis_index(axis))
    everything = jax.tree.map(lambda part: lax.all_gather(part, axis), x)
    start = jax.tree.map(
        lambda part, zero: jnp.broadcast_to(jnp.asarray(zero, part.dtype), part.shape), x, identity
    )

    def lap(k, before):
        at = length - 1 - k if reverse else k
        reached = at > position if reverse else at < position
        new = combine(before, jax.tree.map(lambda part: part[at], everything))
        return jax.tree.map(lambda a, b: jnp.where(reached, a, b), new, before)

    return lax.fori_loop(0, length, lap, start)


def padded_2(block, sides, width):
    for axis, dim in sides:
        count = lax.axis_size(axis)
        forward = [(i, i + 1) for i in range(count - 1)]
        backward = [(target, source) for source, target in forward]
        low = lax.ppermute(
            lax.slice_in_dim(block, block.shape[dim] - width, None, axis=dim), axis, forward
        )
        high = lax.ppermute(lax.slice_in_dim(block, 0, width, axis=dim), axis, backward)
        block = jnp.concatenate([low, block, high], axis=dim)
    return block


def block_output(
    query_rows, key_rows, value_rows, input_gate, log_forget, memory, normalizer, stabilizer
):
    block_len = query_rows.shape[1]
    key_scale = key_rows.shape[-1] ** (-0.5)
    lower_mask = jnp.tril(jnp.ones((block_len, block_len), dtype=bool))
    summed = jnp.cumsum(log_forget, axis=-1)
    log_decay = jnp.where(
        lower_mask, summed[:, :, None] - summed[:, None, :] + input_gate[:, None, :], -jnp.inf
    )
    log_carry = stabilizer[:, None] + summed
    running_max = jnp.maximum(log_carry, jnp.max(log_decay, axis=-1))
    scores = (
        jnp.einsum("btd,bsd->bts", query_rows, key_rows, preferred_element_type=jnp.float32)
        * key_scale
    )
    inner_weight = jnp.exp(log_decay - running_max[:, :, None]) * scores
    weight_rounded = inner_weight.astype(jnp.bfloat16)
    carry_weight = jnp.exp(log_carry - running_max)
    query_wide = query_rows.astype(jnp.float32)
    numerator = carry_weight[:, :, None] * jnp.einsum(
        "bed,btd->bte", memory, query_wide, precision=exact_mode
    )
    numerator = numerator + jnp.einsum(
        "bts,bse->bte", weight_rounded, value_rows, preferred_element_type=jnp.float32
    )
    denominator = carry_weight * jnp.einsum(
        "bd,btd->bt", normalizer, query_wide, precision=exact_mode
    )
    denominator = denominator + jnp.sum(inner_weight, axis=-1)
    return numerator / jnp.maximum(jnp.abs(denominator), jnp.exp(-running_max))[:, :, None]


def block_summary(key_rows, value_rows, input_gate, log_forget):
    key_wide = key_rows.astype(jnp.float32) * key_rows.shape[-1] ** (-0.5)
    summed = jnp.cumsum(log_forget, axis=-1)
    forget_total = summed[:, -1]
    log_weight = forget_total[:, None] - summed + input_gate
    running_max = jnp.max(log_weight, axis=-1)
    weights = jnp.exp(log_weight - running_max[:, None])
    memory = jnp.einsum(
        "bse,bsd->bed",
        weights[:, :, None] * value_rows.astype(jnp.float32),
        key_wide,
        precision=exact_mode,
    )
    normalizer = jnp.einsum("bs,bsd->bd", weights, key_wide, precision=exact_mode)
    return (memory, normalizer, running_max, forget_total)


def combine(earlier, latter):
    early_memory, early_norm, early_max, early_total = earlier
    late_memory, late_norm, late_max, late_total = latter
    joint_max = jnp.maximum(early_max + late_total, late_max)
    early_scale = jnp.exp(early_max + late_total - joint_max)
    late_scale = jnp.exp(late_max - joint_max)
    memory = early_scale[:, None, None] * early_memory + late_scale[:, None, None] * late_memory
    normalizer = early_scale[:, None] * early_norm + late_scale[:, None] * late_norm
    return (memory, normalizer, joint_max, early_total + late_total)


def span_sweep(
    query_rows, key_rows, value_rows, input_gate, log_forget, memory, normalizer, stabilizer, span
):
    block_count = query_rows.shape[1] // span

    def to_blocks(array):
        shaped = array.reshape((array.shape[0], block_count, span) + array.shape[2:])
        return jnp.moveaxis(shaped, 1, 0)

    def advance(carried, pieces):
        query_blk, key_blk, value_blk, gate_blk, forget_blk = pieces
        result = block_output(
            query_blk, key_blk, value_blk, gate_blk, forget_blk, carried[0], carried[1], carried[2]
        )
        return (combine(carried, block_summary(key_blk, value_blk, gate_blk, forget_blk)), result)

    initial = (memory, normalizer, stabilizer, jnp.zeros_like(stabilizer))
    ignored, outputs = lax.scan(
        advance,
        initial,
        tuple(
            (
                to_blocks(array)
                for array in (query_rows, key_rows, value_rows, input_gate, log_forget)
            )
        ),
    )
    return jnp.moveaxis(outputs, 0, 1).reshape(query_rows.shape[:2] + (value_rows.shape[2],))


def reverse_time(array):
    return jnp.flip(array, axis=1)


def to_heads(matrix, head_count):
    shaped = matrix.reshape(matrix.shape[0], head_count, matrix.shape[1] // head_count)
    return shaped.transpose(1, 0, 2)


def pool_window(padded, positions, channels, seq_len, group_size):
    row_count = positions.shape[0]
    group_index = channels // group_size
    reach_left = jnp.left_shift(jnp.ones_like(group_index), group_index)
    reach_right = reach_left - 1
    window_sum = jnp.zeros((row_count, channels.shape[0]), jnp.float32)
    for offset in range(-HALO, HALO):
        inside = ((offset >= -reach_left) & (offset <= reach_right)).astype(jnp.float32)
        window_sum = window_sum + inside * padded[HALO + offset : HALO + offset + row_count]
    first_pos = jnp.maximum(positions[:, None] - reach_left[None, :], 0)
    last_pos = jnp.minimum(positions[:, None] + reach_right[None, :], seq_len - 1)
    counted = (last_pos - first_pos + 1).astype(jnp.float32)
    centre = padded[HALO : HALO + row_count]
    return (window_sum / counted - centre).astype(jnp.bfloat16)


def per_device(
    tokens,
    norm_gain,
    query_weight,
    key_weight,
    value_weight,
    outgate_weight,
    gate_weight,
    gate_bias,
    decay_extra,
    init_memory,
    init_normalizer,
    head_gain,
    pool_weight,
    mem_out_weight,
    pool_out_weight,
):
    block_len = tokens.shape[1]
    model_width = tokens.shape[2]
    head_count, head_width = head_gain.shape
    span = math.gcd(block_len, 256)
    flattened = tokens[0].astype(jnp.float32)
    normed = (
        flattened
        * lax.rsqrt(jnp.mean(flattened * flattened, axis=-1, keepdims=True) + norm_eps)
        * norm_gain
    ).astype(jnp.bfloat16)
    zero_start = tuple(
        (
            jnp.zeros((block_len, weight.shape[1]), jnp.float32)
            for weight in (query_weight, key_weight, value_weight, outgate_weight, pool_weight)
        )
    )
    zero_start = zero_start + (
        jnp.zeros((model_width, mem_out_weight.shape[1]), jnp.bfloat16),
        jnp.zeros((model_width, pool_out_weight.shape[1]), jnp.bfloat16),
    )
    line_query, line_key, line_value, line_outgate, line_pool, line_mem_out, line_pool_out = (
        lax.all_gather(query_weight, "fs", axis=0, tiled=True),
        lax.all_gather(key_weight, "fs", axis=0, tiled=True),
        lax.all_gather(value_weight, "fs", axis=0, tiled=True),
        lax.all_gather(outgate_weight, "fs", axis=0, tiled=True),
        lax.all_gather(pool_weight, "fs", axis=0, tiled=True),
        lax.all_gather(mem_out_weight, "fs", axis=0, tiled=True),
        lax.all_gather(pool_out_weight, "fs", axis=0, tiled=True),
    )
    pieces = (
        lax.all_gather(line_query, "sp", axis=0, tiled=True),
        lax.all_gather(line_key, "sp", axis=0, tiled=True),
        lax.all_gather(line_value, "sp", axis=0, tiled=True),
        lax.all_gather(line_outgate, "sp", axis=0, tiled=True),
        lax.all_gather(line_pool, "sp", axis=0, tiled=True),
        lax.all_gather(line_mem_out, "sp", axis=0, tiled=True),
        lax.all_gather(line_pool_out, "sp", axis=0, tiled=True),
    )
    partial_sums = tuple(
        (
            jnp.dot(normed, weight_rows, preferred_element_type=jnp.float32)
            for weight_rows in pieces[:5]
        )
    )
    collected = tuple((weight_rows for weight_rows in pieces[5:]))
    folded = partial_sums + collected
    query_proj, key_proj, value_proj, outgate, pool_input = tuple(
        (running.astype(jnp.bfloat16) for running in folded[:5])
    )
    mem_weight_all = folded[5]
    pool_weight_all = folded[6]
    gate_pre = lax.dot_general(
        normed,
        gate_weight.reshape(4 * head_count, model_width),
        (((1,), (1,)), ((), ())),
        preferred_element_type=jnp.float32,
    ) + gate_bias.reshape(4 * head_count)
    gate_pre = gate_pre.reshape(block_len, 4, head_count).transpose(1, 2, 0)
    query_heads = to_heads(query_proj, head_count)
    key_heads = to_heads(key_proj, head_count)
    value_heads = to_heads(value_proj, head_count)
    forward_forget = jax.nn.log_sigmoid(gate_pre[1]) + decay_extra[0, 0]
    backward_forget = jax.nn.log_sigmoid(gate_pre[3]) + decay_extra[0, 1]
    zero_rows = jnp.zeros((head_count,), jnp.float32)
    identity = (
        jnp.zeros((head_count, head_width, head_width), jnp.float32),
        jnp.zeros((head_count, head_width), jnp.float32),
        jnp.full((head_count,), -1e30, jnp.float32),
        zero_rows,
    )
    front_memory, front_norm, front_max, front_total = block_summary(
        key_heads, value_heads, gate_pre[0], forward_forget
    )
    prefix = carried_in(
        (front_memory, front_norm, front_max, front_total), "sp", combine, identity, False
    )
    incoming = combine((init_memory[0, 0], init_normalizer[0, 0], zero_rows, zero_rows), prefix)
    forward_out = span_sweep(
        query_heads,
        key_heads,
        value_heads,
        gate_pre[0],
        forward_forget,
        incoming[0],
        incoming[1],
        incoming[2],
        span,
    )
    back_query = reverse_time(query_heads)
    back_key = reverse_time(key_heads)
    back_value = reverse_time(value_heads)
    back_gate = reverse_time(gate_pre[2])
    back_forget = reverse_time(backward_forget)
    rear_memory, rear_norm, rear_max, rear_total = block_summary(
        back_key, back_value, back_gate, back_forget
    )
    suffix = carried_in(
        (rear_memory, rear_norm, rear_max, rear_total), "sp", combine, identity, True
    )
    back_incoming = combine(
        (init_memory[0, 1], init_normalizer[0, 1], zero_rows, zero_rows), suffix
    )
    backward_out = reverse_time(
        span_sweep(
            back_query,
            back_key,
            back_value,
            back_gate,
            back_forget,
            back_incoming[0],
            back_incoming[1],
            back_incoming[2],
            span,
        )
    )
    summed_dirs = (forward_out + backward_out).transpose(1, 0, 2)
    normed_heads = (
        summed_dirs
        * lax.rsqrt(jnp.mean(summed_dirs * summed_dirs, axis=-1, keepdims=True) + norm_eps)
        * head_gain
    )
    out_gate = jax.nn.sigmoid(
        outgate.astype(jnp.float32).reshape(block_len, head_count, head_width)
    )
    memory_out = (
        (normed_heads * out_gate).astype(jnp.bfloat16).reshape(block_len, head_count * head_width)
    )
    padded = padded_2(pool_input, (("sp", 0),), HALO).astype(jnp.float32)
    feature_count = pool_input.shape[1]
    positions = lax.axis_index("sp") * block_len + jnp.arange(block_len, dtype=jnp.int32)
    channels = lax.axis_index("tp") * feature_count + jnp.arange(feature_count, dtype=jnp.int32)
    pool_out = pool_window(
        padded, positions, channels, block_len * lax.axis_size("sp"), model_width // 4
    )
    own_rows = block_len // lax.axis_size("tp")
    result = lax.dot_general(
        memory_out, mem_weight_all, (((1,), (1,)), ((), ())), preferred_element_type=jnp.float32
    )
    mixed = lax.psum_scatter(
        (
            result
            + lax.dot_general(
                pool_out,
                pool_weight_all,
                (((1,), (1,)), ((), ())),
                preferred_element_type=jnp.float32,
            )
        ).astype(jnp.bfloat16),
        "tp",
        scatter_dimension=0,
        tiled=True,
    )
    return mixed.reshape(1, own_rows, model_width)


LOG2E = math.log2(math.e)


def scan_lanes(x, combine_, fill, reverse):
    length = x.shape[1]
    lane = lax.broadcasted_iota(jnp.int32, x.shape, 1)
    d = 1
    while d < length:
        if reverse:
            moved = jnp.where(lane < length - d, pltpu.roll(x, length - d, 1), fill)
        else:
            moved = jnp.where(lane >= d, pltpu.roll(x, d, 1), fill)
        x = combine_(x, moved)
        d *= 2
    return x


def transposed_dot(a, b):
    return lax.dot_general(a, b, (((1,), (1,)), ((), ())), preferred_element_type=jnp.float32)


def layer_kernel(
    n_sp,
    token_ref, gain_ref, qw, kw, vw, ow, gate_ref, bias_ref, decay_ref, mem_ref, nrm_ref,
    hgain_ref, pw, mw, fw,
    o_ref,
    x_all, normed, w_all, stage, transit, gmat, dec, init, nrm, proj_a, proj_b, pool_buf, act,
    flat, cols, level_rows, msg_out, msg_in, state_out, state_in, halo_out, halo_in,
    give, take, total, s1, l1, s2, l2,
    loc_w, loc_s, x_ss, x_rs, p_ss, p_rs, h_ss, h_rs, y_ss, y_rs,
    tz_ss, tz_rs, tx_ss, tx_rs, tw_ss, tw_rs, d_ss, d_rs, i_ss, i_rs, m_ss, m_rs,
    sw_ss, sw_rs, r1_ss, r1_rs, r2_ss, r2_rs,
):
    block, width = token_ref.shape
    rows = qw.shape[0]
    hw = hgain_ref.shape[1]
    feat = pw.shape[1] // 4
    half = block // 2
    span = 2 * block
    pieces_t = 2
    part = half // pieces_t
    z, fs, c = lax.axis_index("sp"), lax.axis_index("fs"), lax.axis_index("tp")
    y, x = fs // 2, lax.rem(fs, 2)
    h, p = z // 2, lax.rem(z, 2)
    zn = z + 1 - 2 * p
    zf = lax.rem(z + 2, n_sp)
    zfn = zf + 1 - 2 * p
    xn, yn = 2 * y + 1 - x, 2 * (1 - y) + x
    other = 1 - c
    low = h == 0
    quarter = 2 * p + x
    to_x, to_y, to_p, to_h, to_c = {"fs": xn}, {"fs": yn}, {"sp": zn}, {"sp": zf}, {"tp": other}

    def remote(src, dst, ss, rs, device):
        return pltpu.make_async_remote_copy(
            src_ref=src, dst_ref=dst, send_sem=ss, recv_sem=rs,
            device_id=device, device_id_type=MESH,
        )

    def at(start, size):
        return pl.ds(pl.multiple_of(start, size), size)

    barrier = pltpu.get_barrier_semaphore()
    for device in (to_x, to_y, to_p, to_h, to_c):
        pl.semaphore_signal(barrier, inc=1, device_id=device, device_id_type=MESH)

    groups = (((qw, hw), (kw, hw), (vw, hw)), ((ow, hw), (pw, feat)), ((mw, hw), (fw, feat)))
    quarters = (quarter, 2 * p + 1 - x, 2 * (1 - p) + 1 - x, 2 * (1 - p) + x)

    def row_block(zs, ys, xs):
        return at((zs * 4 + ys * 2 + xs) * rows, rows)

    def local_weights(g):
        copies = []
        for slot in (1, 2, 3, 0):
            start = 0
            for i, (ref, size) in enumerate(groups[g]):
                columns = pl.ds(start, size)
                if slot:
                    dst = stage.at[g, slot - 1, :, columns]
                else:
                    dst = w_all.at[g, row_block(z, y, x), columns]
                copies.append(
                    pltpu.make_async_copy(
                        ref.at[:, at(quarters[slot] * size, size)], dst, loc_w.at[g, slot, i]
                    )
                )
                start += size
        return copies

    locals_ = [local_weights(g) for g in range(3)]
    own_tokens = pltpu.make_async_copy(
        token_ref, x_all.at[at((2 * x + p) * block, block)], loc_s.at[0]
    )
    own_decay = pltpu.make_async_copy(decay_ref, dec.at[x, p], loc_s.at[1])
    own_init = pltpu.make_async_copy(mem_ref.at[h, quarter], init.at[x], loc_s.at[2])
    own_nrm = pltpu.make_async_copy(nrm_ref, nrm.at[x], loc_s.at[3])
    for copy in locals_[0]:
        copy.start()
    own_tokens.start()
    for copy in locals_[1] + locals_[2]:
        copy.start()
    for copy in (own_decay, own_init, own_nrm):
        copy.start()

    def x_copy(g, s, incoming=False):
        if s == 0:
            dst = w_all.at[g, row_block(z, y, 1 - x if incoming else x)]
        else:
            dst = transit.at[g]
        return remote(dst if incoming else stage.at[g, s], dst, x_ss.at[g, s], x_rs.at[g, s], to_x)

    def p_copy(g, s, incoming=False):
        dst = w_all.at[g, row_block(zn if incoming else z, y, 1 - x if s else x)]
        src = dst if incoming else (transit.at[g] if s else stage.at[g, 2])
        return remote(src, dst, p_ss.at[g, s], p_rs.at[g, s], to_p)

    def h_copy(g, k, s, incoming=False):
        source = (zf, zfn)[k] if incoming else (z, zn)[k]
        ref = w_all.at[g, row_block(source, y, 1 - x if s else x)]
        return remote(ref, ref, h_ss.at[g, k, s], h_rs.at[g, k, s], to_h)

    def y_copy(g, k, s, incoming=False):
        ref = w_all.at[
            g, row_block((z, zn, zf, zfn)[k], 1 - y if incoming else y, 1 - x if s else x)
        ]
        return remote(ref, ref, y_ss.at[g, k, s], y_rs.at[g, k, s], to_y)

    sent = []

    def go(copy):
        copy.start()
        sent.append(copy)

    def begin(g):
        for copy in locals_[g]:
            copy.wait()
        go(x_copy(g, 1))
        go(x_copy(g, 0))
        go(p_copy(g, 0))
        go(h_copy(g, 0, 0))
        go(y_copy(g, 0, 0))

    def after_x(g):
        x_copy(g, 1, True).wait_recv()
        go(p_copy(g, 1))
        x_copy(g, 0, True).wait_recv()
        go(h_copy(g, 0, 1))
        go(y_copy(g, 0, 1))

    def after_p(g):
        for s in range(2):
            p_copy(g, s, True).wait_recv()
            go(h_copy(g, 1, s))
            go(y_copy(g, 1, s))

    def after_h(g):
        for k in range(2):
            for s in range(2):
                h_copy(g, k, s, True).wait_recv()
                go(y_copy(g, 2 + k, s))

    def after_y(g):
        for k in range(4):
            for s in range(2):
                y_copy(g, k, s, True).wait_recv()

    def token_rows(j, b, side, i):
        return at((2 * j + b) * block + side * half + i * part, part)

    def token_p(i, incoming=False):
        b = 1 - p if incoming else p
        dst = x_all.at[token_rows(x, b, c, i)]
        src = dst if incoming else token_ref.at[at(c * half + i * part, part)]
        return remote(src, dst, tz_ss.at[i], tz_rs.at[i], to_p)

    def token_x(kind, i, incoming=False):
        b = 1 - p if kind else p
        dst = x_all.at[token_rows(1 - x if incoming else x, b, c, i)]
        src = dst if incoming or kind else token_ref.at[at(c * half + i * part, part)]
        return remote(src, dst, tx_ss.at[kind, i], tx_rs.at[kind, i], to_x)

    places = ((x, 1 - p), (1 - x, p), (1 - x, 1 - p))

    def token_swap(which, i, incoming=False):
        j, b = places[which]
        ref = x_all.at[token_rows(j, b, other if incoming else c, i)]
        return remote(ref, ref, tw_ss.at[which, i], tw_rs.at[which, i], to_c)

    def decay_p(incoming=False):
        dst = dec.at[x, 1 - p if incoming else p]
        return remote(dst if incoming else decay_ref, dst, d_ss.at[0], d_rs.at[0], to_p)

    def decay_x(kind, incoming=False):
        dst = dec.at[1 - x if incoming else x, 1 - p if kind else p]
        src = dst if incoming or kind else decay_ref
        return remote(src, dst, d_ss.at[1 + kind], d_rs.at[1 + kind], to_x)

    def init_x(which, incoming=False):
        dst = (init, nrm)[which].at[1 - x if incoming else x]
        src = (mem_ref.at[h, 2 * p + 1 - x], nrm_ref)[which]
        return remote(dst if incoming else src, dst, i_ss.at[which], i_rs.at[which], to_x)

    def normalise(j, b):
        step = 64

        def body(i, carry):
            here = at((2 * j + b) * block + i * step, step)
            wide = x_all[here, :].astype(jnp.float32)
            normed[here, :] = (
                wide
                * lax.rsqrt(jnp.mean(wide * wide, axis=-1, keepdims=True) + norm_eps)
                * gain_ref[...]
            ).astype(jnp.bfloat16)
            return carry

        lax.fori_loop(0, block // step, body, 0)

    pl.semaphore_wait(barrier, 5)
    begin(0)
    for i in range(pieces_t):
        go(token_p(i))
        go(token_x(0, i))
    own_decay.wait()
    go(decay_p())
    go(decay_x(0))
    gmat[...] = jnp.zeros_like(gmat)
    pick = lax.broadcasted_iota(jnp.int32, (4, width), 0) == quarter
    row16 = lax.broadcasted_iota(jnp.int32, (16, width), 0)
    gates16 = jnp.zeros((16, width), jnp.float32)
    for i in range(4):
        row = jnp.sum(
            jnp.where(pick, gate_ref[i].astype(jnp.float32), 0.0), axis=0, keepdims=True
        )
        gates16 = jnp.where((row16 == i) | (row16 == i + 4), row, gates16)
    gmat[0:16, :] = gates16.astype(jnp.bfloat16)
    own_tokens.wait()
    normalise(x, p)
    after_x(0)
    begin(1)
    go(init_x(0))
    go(init_x(1))
    for i in range(pieces_t):
        token_p(i, True).wait_recv()
        go(token_swap(0, i))
        go(token_x(1, i))
    decay_p(True).wait_recv()
    go(decay_x(1))
    after_p(0)
    for i in range(pieces_t):
        token_x(0, i, True).wait_recv()
        go(token_swap(1, i))
    for i in range(pieces_t):
        token_swap(0, i, True).wait_recv()
    normalise(x, 1 - p)
    after_x(1)
    begin(2)
    for i in range(pieces_t):
        token_swap(1, i, True).wait_recv()
    normalise(1 - x, p)
    after_h(0)
    for i in range(pieces_t):
        token_x(1, i, True).wait_recv()
        go(token_swap(2, i))
    after_p(1)
    for i in range(pieces_t):
        token_swap(2, i, True).wait_recv()
    normalise(1 - x, 1 - p)
    decay_x(0, True).wait_recv()
    decay_x(1, True).wait_recv()

    tall = []
    for j in range(2):
        pieces = []
        for b in range(2):
            pre = transposed_dot(normed[(2 * j + b) * block : (2 * j + b + 1) * block, :], gmat[...])
            pieces.append(pre.T[:8])
        tall.append(jnp.concatenate(pieces, axis=1))
    row8 = lax.broadcasted_iota(jnp.int32, (8, span), 0)
    gates = jnp.where(row8 < 4, tall[0], tall[1])
    extra = jnp.zeros((8, span), jnp.float32)
    for i in range(4):
        gates = gates + jnp.where((row8 == i) | (row8 == i + 4), bias_ref[i, quarter], 0.0)
    for j in range(2):
        for direction in range(2):
            value = jnp.concatenate(
                [dec[j, b, direction, pl.ds(quarter, 1), :] for b in range(2)], axis=1
            )
            extra = jnp.where(row8 == 4 * j + 1 + 2 * direction, value, extra)
    forget = jnp.minimum(gates, 0.0) - jnp.log1p(jnp.exp(-jnp.abs(gates))) + extra
    sum_f = pltpu.roll(scan_lanes(forget, jnp.add, 0.0, False), 7, 0)
    sum_b = pltpu.roll(scan_lanes(forget, jnp.add, 0.0, True), 7, 0)
    level_f = gates - sum_f
    level_b = gates - sum_b
    run_f = scan_lanes(level_f, jnp.maximum, -1e30, False)
    run_b = scan_lanes(level_b, jnp.maximum, -1e30, True)
    top_f = jnp.maximum(run_f[:, span - 1 : span], 0.0)
    top_b = jnp.maximum(run_b[:, 0:1], 0.0)
    end_f = sum_f[:, span - 1 : span] + top_f
    end_b = sum_b[:, 0:1] + top_b
    msg_out[...] = jnp.broadcast_to(jnp.where(low, end_f, end_b), msg_out.shape)

    def message(which, incoming=False):
        src = (msg_out, state_out, halo_out)[which]
        dst = (msg_in, state_in, halo_in)[which]
        return remote(dst if incoming else src, dst, m_ss.at[which], m_rs.at[which], to_h)

    go(message(0))

    after_y(0)

    def project(g, store):
        def body(i, carry):
            here = at(i * block, block)
            store(i, jnp.dot(
                normed[here, :], w_all[g], preferred_element_type=jnp.float32
            ).astype(jnp.bfloat16))
            return carry

        lax.fori_loop(0, 4, body, 0)

    def store_a(i, value):
        proj_a[at(i * block, block), :] = value

    project(0, store_a)
    after_h(1)

    message(0, True).wait_recv()
    arrived = msg_in[:, 0:1]
    enter_f = jnp.where(low, 0.0, arrived)
    enter_b = jnp.where(low, arrived, 0.0)
    scale_bits = -0.5 * math.log2(hw)
    lf2 = level_f * LOG2E + scale_bits
    lb2 = level_b * LOG2E + scale_bits
    peak_f = jnp.maximum(run_f, enter_f)
    peak_b = jnp.maximum(run_b, enter_b)
    level_rows[0:8, :] = lf2
    level_rows[8:16, :] = lb2
    flat[48:, :] = jnp.zeros_like(flat[48:, :])
    flat[0:8, :] = peak_f * LOG2E
    flat[8:16, :] = peak_b * LOG2E
    flat[16:24, :] = jnp.exp(enter_f - peak_f)
    flat[24:32, :] = jnp.exp(enter_b - peak_b)
    flat[32:40, :] = jnp.exp(-(sum_f + peak_f))
    flat[40:48, :] = jnp.exp(-(sum_b + peak_b))
    cols[...] = flat[...].T

    own_init.wait()
    own_nrm.wait()
    init_x(0, True).wait_recv()
    init_x(1, True).wait_recv()
    leave_f = jnp.exp2(lf2 - top_f * LOG2E)
    leave_b = jnp.exp2(lb2 - top_b * LOG2E)
    keep_f = jnp.exp(-top_f)
    keep_b = jnp.exp(-top_b)
    starts = []
    for j in range(2):
        here = slice(j * span, (j + 1) * span)
        own = jnp.where(low, leave_f[4 * j : 4 * j + 1], leave_b[4 * j + 2 : 4 * j + 3])
        kept = jnp.where(low, keep_f[4 * j : 4 * j + 1], keep_b[4 * j + 2 : 4 * j + 3])
        values = proj_a[here, 2 * hw : 3 * hw].astype(jnp.float32).T * own
        lhs = jnp.concatenate(
            [values, jnp.broadcast_to(own, (8, span))], axis=0
        ).astype(jnp.bfloat16)
        grown = jnp.dot(lhs, proj_a[here, hw : 2 * hw], preferred_element_type=jnp.float32)
        start = jnp.concatenate(
            [init[j], jnp.broadcast_to(nrm[j, h, pl.ds(quarter, 1), :], (8, hw))], axis=0
        )
        starts.append(start)
        state_out[j] = kept * start + grown
    go(message(1))

    after_y(1)

    def store_b(i, value):
        proj_b[at(i * block, block), :] = value[:, :hw]
        pool_buf[i // 2, pl.ds(pl.multiple_of(8 + lax.rem(i, 2) * block, 8), block), :] = value[
            :, hw:
        ].astype(jnp.float32)

    project(1, store_b)
    for j in range(2):
        halo_out[j] = jnp.where(low, pool_buf[j, span : span + 8, :], pool_buf[j, 8:16, :])
    go(message(2))
    after_x(2)
    after_p(2)

    message(1, True).wait_recv()
    for j in range(2):
        here = slice(j * span, (j + 1) * span)
        front_start = jnp.where(low, starts[j], state_in[j])
        rear_start = jnp.where(low, state_in[j], starts[j])
        carry_in = jnp.concatenate(
            [front_start[:hw], rear_start[:hw], front_start[hw:], rear_start[hw:]], axis=0
        )
        carry_in = jnp.concatenate(
            [carry_in, jnp.zeros((3 * hw - carry_in.shape[0], hw), jnp.float32)], axis=0
        )
        coarse = carry_in.astype(jnp.bfloat16)
        fine = (carry_in - coarse.astype(jnp.float32)).astype(jnp.bfloat16)
        for i in range(4):
            r0 = i * half
            mine = slice(j * span + r0, j * span + r0 + half)
            q = proj_a[mine, 0:hw]
            carry = transposed_dot(q, coarse) + transposed_dot(q, fine)
            score = transposed_dot(q, proj_a[here, hw : 2 * hw])
            col = cols[r0 : r0 + half, :]

            def direction(first, last, level, peak, decay, floor, got, den0, rear):
                weight = jnp.exp2(level[:, first:last] - peak) * score[:, first:last]
                t = r0 + lax.broadcasted_iota(jnp.int32, weight.shape, 0)
                s = first + lax.broadcasted_iota(jnp.int32, weight.shape, 1)
                weight = jnp.where(s >= t if rear else s <= t, weight, 0.0)
                num = decay * got + jnp.dot(
                    weight.astype(jnp.bfloat16),
                    proj_a[j * span + first : j * span + last, 2 * hw : 3 * hw],
                    preferred_element_type=jnp.float32,
                )
                den = decay * den0 + jnp.sum(weight, axis=1, keepdims=True)
                return num / jnp.maximum(jnp.abs(den), floor)

            f, b = 4 * j, 4 * j + 2
            summed = direction(
                0, r0 + half, level_rows[f : f + 1, :], col[:, f : f + 1],
                col[:, 16 + f : 17 + f], col[:, 32 + f : 33 + f],
                carry[:, :hw], carry[:, 2 * hw : 2 * hw + 1], False,
            ) + direction(
                r0, span, level_rows[8 + b : 9 + b, :], col[:, 8 + b : 9 + b],
                col[:, 24 + b : 25 + b], col[:, 40 + b : 41 + b],
                carry[:, hw : 2 * hw], carry[:, 2 * hw + 8 : 2 * hw + 9], True,
            )
            out = (
                summed
                * lax.rsqrt(jnp.mean(summed * summed, axis=-1, keepdims=True) + norm_eps)
                * hgain_ref[pl.ds(quarter, 1), :]
                * jax.nn.sigmoid(proj_b[mine, :].astype(jnp.float32))
            )
            place = (i % 2) * span + (2 * j + i // 2) * half
            act[place : place + half, 0:hw] = out.astype(jnp.bfloat16)
        if j == 0:
            after_h(2)

    message(2, True).wait_recv()
    for j in range(2):
        zero = jnp.zeros((8, feat), jnp.float32)
        pool_buf[j, 0:8, :] = jnp.where(low, zero, halo_in[j])
        pool_buf[j, span + 8 : span + 16, :] = jnp.where(low, halo_in[j], zero)
    group = (c * 4 + quarter) * feat * 4 // width
    for k in range(4):

        @pl.when(group == k)
        def _(k=k):
            reach = 2 ** k
            t = h * span + lax.broadcasted_iota(jnp.int32, (span, 1), 0)
            counted = jnp.minimum(t + reach - 1, n_sp * block - 1) - jnp.maximum(t - reach, 0) + 1
            counted = counted.astype(jnp.float32)
            length = span + 16
            for j in range(2):
                window = pool_buf[j]
                for e in range(k + 1):
                    window = window + pltpu.roll(window, length - 2 ** e, 0)
                if reach < 8:
                    window = pltpu.roll(window, length - (8 - reach), 0)
                value = window[:span] / counted - pool_buf[j, 8 : 8 + span, :]
                value = value.astype(jnp.bfloat16)
                for i in range(4):
                    place = (i % 2) * span + (2 * j + i // 2) * half
                    act[place : place + half, hw:] = value[i * half : (i + 1) * half]

    after_y(2)
    count = give.shape[0]
    tile = width // count

    def swap(n):
        return remote(give.at[n], take.at[n], sw_ss.at[n], sw_rs.at[n], to_c)

    def first_stage(n, slot, incoming=False):
        dst = l1.at[n, slot]
        return remote(
            dst if incoming else s1.at[n, slot], dst, r1_ss.at[n, slot], r1_rs.at[n, slot],
            to_p if n % 2 else to_x,
        )

    def second_stage(n, incoming=False):
        return remote(
            l2.at[n] if incoming else s2.at[n], l2.at[n], r2_ss.at[n], r2_rs.at[n],
            to_x if n % 2 else to_p,
        )

    def product(side, n):
        return transposed_dot(act[at(side * span, span), :], w_all[2, n * tile : (n + 1) * tile, :])

    for n in range(count):
        give[n] = product(other, n).astype(jnp.bfloat16).reshape(give.shape[1:])
        go(swap(n))
    home = 2 * x + p
    both = 2 * (1 - x) + 1 - p
    for n in range(count):
        part_sum = product(c, n)
        swap(n).wait_recv()
        total[n] = part_sum.reshape(total.shape[1:]) + take[n].astype(jnp.float32)
        near, middle = 2 * (1 - x) + p, 2 * x + 1 - p
        if n % 2:
            near, middle = middle, near
        s1[n, 1] = total[n, both].astype(jnp.bfloat16)
        go(first_stage(n, 1))
        s1[n, 0] = total[n, near].astype(jnp.bfloat16)
        go(first_stage(n, 0))
    for n in range(count):
        middle = 2 * (1 - x) + p if n % 2 else 2 * x + 1 - p
        first_stage(n, 1, True).wait_recv()
        s2[n] = (total[n, middle] + l1[n, 1].astype(jnp.float32)).astype(jnp.bfloat16)
        go(second_stage(n))
    for n in range(count):
        first_stage(n, 0, True).wait_recv()
        second_stage(n, True).wait_recv()
        o_ref[:, n * tile : (n + 1) * tile] = (
            total[n, home] + l1[n, 0].astype(jnp.float32) + l2[n].astype(jnp.float32)
        ).astype(jnp.bfloat16)
    for copy in sent:
        copy.wait_send()


def by_group(
    tokens, norm_gain, query_weight, key_weight, value_weight, outgate_weight, gate_weight,
    gate_bias, decay_extra, init_memory, init_normalizer, head_gain, pool_weight, mem_out_weight,
    pool_out_weight,
):
    n_sp = lax.axis_size("sp")
    block, width = tokens.shape[1:]
    rows = query_weight.shape[0]
    hw = head_gain.shape[1]
    feat = pool_weight.shape[1] // 4
    columns = 3 * hw
    half, span, everything = block // 2, 2 * block, 4 * block
    count = 4
    tile = width // count
    f32, bf16 = jnp.float32, jnp.bfloat16
    dma = pltpu.SemaphoreType.DMA
    vmem = pl.BlockSpec(memory_space=pltpu.VMEM)
    anywhere = pl.BlockSpec(memory_space=pl.ANY)
    smem = pl.BlockSpec(memory_space=pltpu.SMEM)
    mixed = pl.pallas_call(
        functools.partial(layer_kernel, n_sp),
        out_shape=jax.ShapeDtypeStruct((half, width), bf16),
        in_specs=[
            anywhere, vmem, anywhere, anywhere, anywhere, anywhere, vmem, smem, anywhere, anywhere,
            anywhere, vmem, anywhere, anywhere, anywhere,
        ],
        out_specs=vmem,
        scratch_shapes=[
            pltpu.VMEM((everything, width), bf16),
            pltpu.VMEM((everything, width), bf16),
            pltpu.VMEM((3, width, columns), bf16),
            pltpu.VMEM((3, 3, rows, columns), bf16),
            pltpu.VMEM((3, rows, columns), bf16),
            pltpu.VMEM((128, width), bf16),
            pltpu.VMEM((2, 2) + decay_extra.shape[1:], f32),
            pltpu.VMEM((2, hw, hw), f32),
            pltpu.VMEM((2,) + init_normalizer.shape[1:], f32),
            pltpu.VMEM((everything, columns), bf16),
            pltpu.VMEM((everything, hw), bf16),
            pltpu.VMEM((2, span + 16, feat), f32),
            pltpu.VMEM((everything, columns), bf16),
            pltpu.VMEM((128, span), f32),
            pltpu.VMEM((span, 128), f32),
            pltpu.VMEM((16, span), f32),
            pltpu.VMEM((8, 128), f32),
            pltpu.VMEM((8, 128), f32),
            pltpu.VMEM((2, hw + 8, hw), f32),
            pltpu.VMEM((2, hw + 8, hw), f32),
            pltpu.VMEM((2, 8, feat), f32),
            pltpu.VMEM((2, 8, feat), f32),
            pltpu.VMEM((count, 4, half, tile), bf16),
            pltpu.VMEM((count, 4, half, tile), bf16),
            pltpu.VMEM((count, 4, half, tile), f32),
            pltpu.VMEM((count, 2, half, tile), bf16),
            pltpu.VMEM((count, 2, half, tile), bf16),
            pltpu.VMEM((count, half, tile), bf16),
            pltpu.VMEM((count, half, tile), bf16),
            dma((3, 4, 3)),
            dma((4,)),
            dma((3, 2)), dma((3, 2)),
            dma((3, 2)), dma((3, 2)),
            dma((3, 2, 2)), dma((3, 2, 2)),
            dma((3, 4, 2)), dma((3, 4, 2)),
            dma((2,)), dma((2,)),
            dma((2, 2)), dma((2, 2)),
            dma((3, 2)), dma((3, 2)),
            dma((3,)), dma((3,)),
            dma((2,)), dma((2,)),
            dma((3,)), dma((3,)),
            dma((count,)), dma((count,)),
            dma((count, 2)), dma((count, 2)),
            dma((count,)), dma((count,)),
        ],
        compiler_params=pltpu.CompilerParams(
            collective_id=0, has_side_effects=True, vmem_limit_bytes=60 * 2**20
        ),
        name="layer",
    )(
        tokens[0], norm_gain[None], query_weight, key_weight, value_weight, outgate_weight,
        gate_weight, gate_bias, decay_extra[0], init_memory[0], init_normalizer[0], head_gain,
        pool_weight, mem_out_weight, pool_out_weight,
    )
    return mixed[None]


def solution(mesh):
    placed = (
        P("fs", "sp", None),
        P(),
        P(("sp", "fs"), "tp"),
        P(("sp", "fs"), "tp"),
        P(("sp", "fs"), "tp"),
        P(("sp", "fs"), "tp"),
        P(None, "tp", None),
        P(None, "tp"),
        P("fs", None, "tp", "sp"),
        P("fs", None, "tp", None, None),
        P("fs", None, "tp", None),
        P("tp", None),
        P(("sp", "fs"), "tp"),
        P(("sp", "fs"), "tp"),
        P(("sp", "fs"), "tp"),
    )

    def body(*args):
        heads, width = args[11].shape
        features = args[12].shape[1]
        block, model_width = args[0].shape[1:]
        fits = (
            lax.axis_size("tp") == 2
            and lax.axis_size("fs") == 4
            and lax.axis_size("sp") == 4
            and heads == 4
            and width == 128
            and features == 8 * width
            and model_width == 2 * features
            and block == 2 * width
        )
        return (by_group if fits else per_device)(*args)

    return jax.shard_map(
        body,
        mesh=mesh,
        in_specs=placed,
        out_specs=P("fs", ("sp", "tp"), None),
        check_vma=False,
    )
```

```python
import functools
import math

import jax
import jax.numpy as jnp
from jax import lax
from jax.experimental import pallas as pl
from jax.experimental.pallas import tpu as pltpu
from jax.sharding import PartitionSpec as P

MESH = pl.DeviceIdType.MESH

HALO = 8


norm_eps = 1e-06
exact_mode = lax.Precision.HIGHEST


def carried_in(x, axis, combine, identity, reverse):
    length, position = (lax.axis_size(axis), lax.axis_index(axis))
    everything = jax.tree.map(lambda part: lax.all_gather(part, axis), x)
    start = jax.tree.map(
        lambda part, zero: jnp.broadcast_to(jnp.asarray(zero, part.dtype), part.shape), x, identity
    )

    def lap(k, before):
        at = length - 1 - k if reverse else k
        reached = at > position if reverse else at < position
        new = combine(before, jax.tree.map(lambda part: part[at], everything))
        return jax.tree.map(lambda a, b: jnp.where(reached, a, b), new, before)

    return lax.fori_loop(0, length, lap, start)


def padded_2(block, sides, width):
    for axis, dim in sides:
        count = lax.axis_size(axis)
        forward = [(i, i + 1) for i in range(count - 1)]
        backward = [(target, source) for source, target in forward]
        low = lax.ppermute(
            lax.slice_in_dim(block, block.shape[dim] - width, None, axis=dim), axis, forward
        )
        high = lax.ppermute(lax.slice_in_dim(block, 0, width, axis=dim), axis, backward)
        block = jnp.concatenate([low, block, high], axis=dim)
    return block


def block_output(
    query_rows, key_rows, value_rows, input_gate, log_forget, memory, normalizer, stabilizer
):
    block_len = query_rows.shape[1]
    key_scale = key_rows.shape[-1] ** (-0.5)
    lower_mask = jnp.tril(jnp.ones((block_len, block_len), dtype=bool))
    summed = jnp.cumsum(log_forget, axis=-1)
    log_decay = jnp.where(
        lower_mask, summed[:, :, None] - summed[:, None, :] + input_gate[:, None, :], -jnp.inf
    )
    log_carry = stabilizer[:, None] + summed
    running_max = jnp.maximum(log_carry, jnp.max(log_decay, axis=-1))
    scores = (
        jnp.einsum("btd,bsd->bts", query_rows, key_rows, preferred_element_type=jnp.float32)
        * key_scale
    )
    inner_weight = jnp.exp(log_decay - running_max[:, :, None]) * scores
    weight_rounded = inner_weight.astype(jnp.bfloat16)
    carry_weight = jnp.exp(log_carry - running_max)
    query_wide = query_rows.astype(jnp.float32)
    numerator = carry_weight[:, :, None] * jnp.einsum(
        "bed,btd->bte", memory, query_wide, precision=exact_mode
    )
    numerator = numerator + jnp.einsum(
        "bts,bse->bte", weight_rounded, value_rows, preferred_element_type=jnp.float32
    )
    denominator = carry_weight * jnp.einsum(
        "bd,btd->bt", normalizer, query_wide, precision=exact_mode
    )
    denominator = denominator + jnp.sum(inner_weight, axis=-1)
    return numerator / jnp.maximum(jnp.abs(denominator), jnp.exp(-running_max))[:, :, None]


def block_summary(key_rows, value_rows, input_gate, log_forget):
    key_wide = key_rows.astype(jnp.float32) * key_rows.shape[-1] ** (-0.5)
    summed = jnp.cumsum(log_forget, axis=-1)
    forget_total = summed[:, -1]
    log_weight = forget_total[:, None] - summed + input_gate
    running_max = jnp.max(log_weight, axis=-1)
    weights = jnp.exp(log_weight - running_max[:, None])
    memory = jnp.einsum(
        "bse,bsd->bed",
        weights[:, :, None] * value_rows.astype(jnp.float32),
        key_wide,
        precision=exact_mode,
    )
    normalizer = jnp.einsum("bs,bsd->bd", weights, key_wide, precision=exact_mode)
    return (memory, normalizer, running_max, forget_total)


def combine(earlier, latter):
    early_memory, early_norm, early_max, early_total = earlier
    late_memory, late_norm, late_max, late_total = latter
    joint_max = jnp.maximum(early_max + late_total, late_max)
    early_scale = jnp.exp(early_max + late_total - joint_max)
    late_scale = jnp.exp(late_max - joint_max)
    memory = early_scale[:, None, None] * early_memory + late_scale[:, None, None] * late_memory
    normalizer = early_scale[:, None] * early_norm + late_scale[:, None] * late_norm
    return (memory, normalizer, joint_max, early_total + late_total)


def span_sweep(
    query_rows, key_rows, value_rows, input_gate, log_forget, memory, normalizer, stabilizer, span
):
    block_count = query_rows.shape[1] // span

    def to_blocks(array):
        shaped = array.reshape((array.shape[0], block_count, span) + array.shape[2:])
        return jnp.moveaxis(shaped, 1, 0)

    def advance(carried, pieces):
        query_blk, key_blk, value_blk, gate_blk, forget_blk = pieces
        result = block_output(
            query_blk, key_blk, value_blk, gate_blk, forget_blk, carried[0], carried[1], carried[2]
        )
        return (combine(carried, block_summary(key_blk, value_blk, gate_blk, forget_blk)), result)

    initial = (memory, normalizer, stabilizer, jnp.zeros_like(stabilizer))
    ignored, outputs = lax.scan(
        advance,
        initial,
        tuple(
            (
                to_blocks(array)
                for array in (query_rows, key_rows, value_rows, input_gate, log_forget)
            )
        ),
    )
    return jnp.moveaxis(outputs, 0, 1).reshape(query_rows.shape[:2] + (value_rows.shape[2],))


def reverse_time(array):
    return jnp.flip(array, axis=1)


def to_heads(matrix, head_count):
    shaped = matrix.reshape(matrix.shape[0], head_count, matrix.shape[1] // head_count)
    return shaped.transpose(1, 0, 2)


def pool_window(padded, positions, channels, seq_len, group_size):
    row_count = positions.shape[0]
    group_index = channels // group_size
    reach_left = jnp.left_shift(jnp.ones_like(group_index), group_index)
    reach_right = reach_left - 1
    window_sum = jnp.zeros((row_count, channels.shape[0]), jnp.float32)
    for offset in range(-HALO, HALO):
        inside = ((offset >= -reach_left) & (offset <= reach_right)).astype(jnp.float32)
        window_sum = window_sum + inside * padded[HALO + offset : HALO + offset + row_count]
    first_pos = jnp.maximum(positions[:, None] - reach_left[None, :], 0)
    last_pos = jnp.minimum(positions[:, None] + reach_right[None, :], seq_len - 1)
    counted = (last_pos - first_pos + 1).astype(jnp.float32)
    centre = padded[HALO : HALO + row_count]
    return (window_sum / counted - centre).astype(jnp.bfloat16)


def per_device(
    tokens,
    norm_gain,
    query_weight,
    key_weight,
    value_weight,
    outgate_weight,
    gate_weight,
    gate_bias,
    decay_extra,
    init_memory,
    init_normalizer,
    head_gain,
    pool_weight,
    mem_out_weight,
    pool_out_weight,
):
    block_len = tokens.shape[1]
    model_width = tokens.shape[2]
    head_count, head_width = head_gain.shape
    span = math.gcd(block_len, 256)
    flattened = tokens[0].astype(jnp.float32)
    normed = (
        flattened
        * lax.rsqrt(jnp.mean(flattened * flattened, axis=-1, keepdims=True) + norm_eps)
        * norm_gain
    ).astype(jnp.bfloat16)
    zero_start = tuple(
        (
            jnp.zeros((block_len, weight.shape[1]), jnp.float32)
            for weight in (query_weight, key_weight, value_weight, outgate_weight, pool_weight)
        )
    )
    zero_start = zero_start + (
        jnp.zeros((model_width, mem_out_weight.shape[1]), jnp.bfloat16),
        jnp.zeros((model_width, pool_out_weight.shape[1]), jnp.bfloat16),
    )
    line_query, line_key, line_value, line_outgate, line_pool, line_mem_out, line_pool_out = (
        lax.all_gather(query_weight, "fs", axis=0, tiled=True),
        lax.all_gather(key_weight, "fs", axis=0, tiled=True),
        lax.all_gather(value_weight, "fs", axis=0, tiled=True),
        lax.all_gather(outgate_weight, "fs", axis=0, tiled=True),
        lax.all_gather(pool_weight, "fs", axis=0, tiled=True),
        lax.all_gather(mem_out_weight, "fs", axis=0, tiled=True),
        lax.all_gather(pool_out_weight, "fs", axis=0, tiled=True),
    )
    pieces = (
        lax.all_gather(line_query, "sp", axis=0, tiled=True),
        lax.all_gather(line_key, "sp", axis=0, tiled=True),
        lax.all_gather(line_value, "sp", axis=0, tiled=True),
        lax.all_gather(line_outgate, "sp", axis=0, tiled=True),
        lax.all_gather(line_pool, "sp", axis=0, tiled=True),
        lax.all_gather(line_mem_out, "sp", axis=0, tiled=True),
        lax.all_gather(line_pool_out, "sp", axis=0, tiled=True),
    )
    partial_sums = tuple(
        (
            jnp.dot(normed, weight_rows, preferred_element_type=jnp.float32)
            for weight_rows in pieces[:5]
        )
    )
    collected = tuple((weight_rows for weight_rows in pieces[5:]))
    folded = partial_sums + collected
    query_proj, key_proj, value_proj, outgate, pool_input = tuple(
        (running.astype(jnp.bfloat16) for running in folded[:5])
    )
    mem_weight_all = folded[5]
    pool_weight_all = folded[6]
    gate_pre = lax.dot_general(
        normed,
        gate_weight.reshape(4 * head_count, model_width),
        (((1,), (1,)), ((), ())),
        preferred_element_type=jnp.float32,
    ) + gate_bias.reshape(4 * head_count)
    gate_pre = gate_pre.reshape(block_len, 4, head_count).transpose(1, 2, 0)
    query_heads = to_heads(query_proj, head_count)
    key_heads = to_heads(key_proj, head_count)
    value_heads = to_heads(value_proj, head_count)
    forward_forget = jax.nn.log_sigmoid(gate_pre[1]) + decay_extra[0, 0]
    backward_forget = jax.nn.log_sigmoid(gate_pre[3]) + decay_extra[0, 1]
    zero_rows = jnp.zeros((head_count,), jnp.float32)
    identity = (
        jnp.zeros((head_count, head_width, head_width), jnp.float32),
        jnp.zeros((head_count, head_width), jnp.float32),
        jnp.full((head_count,), -1e30, jnp.float32),
        zero_rows,
    )
    front_memory, front_norm, front_max, front_total = block_summary(
        key_heads, value_heads, gate_pre[0], forward_forget
    )
    prefix = carried_in(
        (front_memory, front_norm, front_max, front_total), "sp", combine, identity, False
    )
    incoming = combine((init_memory[0, 0], init_normalizer[0, 0], zero_rows, zero_rows), prefix)
    forward_out = span_sweep(
        query_heads,
        key_heads,
        value_heads,
        gate_pre[0],
        forward_forget,
        incoming[0],
        incoming[1],
        incoming[2],
        span,
    )
    back_query = reverse_time(query_heads)
    back_key = reverse_time(key_heads)
    back_value = reverse_time(value_heads)
    back_gate = reverse_time(gate_pre[2])
    back_forget = reverse_time(backward_forget)
    rear_memory, rear_norm, rear_max, rear_total = block_summary(
        back_key, back_value, back_gate, back_forget
    )
    suffix = carried_in(
        (rear_memory, rear_norm, rear_max, rear_total), "sp", combine, identity, True
    )
    back_incoming = combine(
        (init_memory[0, 1], init_normalizer[0, 1], zero_rows, zero_rows), suffix
    )
    backward_out = reverse_time(
        span_sweep(
            back_query,
            back_key,
            back_value,
            back_gate,
            back_forget,
            back_incoming[0],
            back_incoming[1],
            back_incoming[2],
            span,
        )
    )
    summed_dirs = (forward_out + backward_out).transpose(1, 0, 2)
    normed_heads = (
        summed_dirs
        * lax.rsqrt(jnp.mean(summed_dirs * summed_dirs, axis=-1, keepdims=True) + norm_eps)
        * head_gain
    )
    out_gate = jax.nn.sigmoid(
        outgate.astype(jnp.float32).reshape(block_len, head_count, head_width)
    )
    memory_out = (
        (normed_heads * out_gate).astype(jnp.bfloat16).reshape(block_len, head_count * head_width)
    )
    padded = padded_2(pool_input, (("sp", 0),), HALO).astype(jnp.float32)
    feature_count = pool_input.shape[1]
    positions = lax.axis_index("sp") * block_len + jnp.arange(block_len, dtype=jnp.int32)
    channels = lax.axis_index("tp") * feature_count + jnp.arange(feature_count, dtype=jnp.int32)
    pool_out = pool_window(
        padded, positions, channels, block_len * lax.axis_size("sp"), model_width // 4
    )
    own_rows = block_len // lax.axis_size("tp")
    result = lax.dot_general(
        memory_out, mem_weight_all, (((1,), (1,)), ((), ())), preferred_element_type=jnp.float32
    )
    mixed = lax.psum_scatter(
        (
            result
            + lax.dot_general(
                pool_out,
                pool_weight_all,
                (((1,), (1,)), ((), ())),
                preferred_element_type=jnp.float32,
            )
        ).astype(jnp.bfloat16),
        "tp",
        scatter_dimension=0,
        tiled=True,
    )
    return mixed.reshape(1, own_rows, model_width)


LOG2E = math.log2(math.e)


def scan_lanes(x, combine_, fill, reverse):
    length = x.shape[1]
    lane = lax.broadcasted_iota(jnp.int32, x.shape, 1)
    d = 1
    while d < length:
        if reverse:
            moved = jnp.where(lane < length - d, pltpu.roll(x, length - d, 1), fill)
        else:
            moved = jnp.where(lane >= d, pltpu.roll(x, d, 1), fill)
        x = combine_(x, moved)
        d *= 2
    return x


def transposed_dot(a, b):
    return lax.dot_general(a, b, (((1,), (1,)), ((), ())), preferred_element_type=jnp.float32)


def layer_kernel(
    n_sp,
    token_ref, gain_ref, qw, kw, vw, ow, gate_ref, bias_ref, decay_ref, mem_ref, nrm_ref,
    hgain_ref, pw, mw, fw,
    o_ref,
    x_all, normed, w_all, stage, transit, gmat, dec, init, nrm, proj_a, proj_b, pool_buf, act,
    within, dens, values_t, pre_rows, flat, cols, run_rows, aux_out, aux_in, state_out, state_in, halo_tok,
    give, take, total, s1, l1, s2, l2,
    loc_w, loc_s, x_ss, x_rs, p_ss, p_rs, h_ss, h_rs, y_ss, y_rs,
    token_p_ss, token_p_rs, tx_ss, tx_rs, tw_ss, tw_rs, d_ss, d_rs, i_ss, i_rs, m_ss, m_rs, e_ss, e_rs,
    sw_ss, sw_rs, r1_ss, r1_rs, r2_ss, r2_rs,
):
    block, width = token_ref.shape
    rows = qw.shape[0]
    hw = hgain_ref.shape[1]
    feat = pw.shape[1] // 4
    half = block // 2
    span = 2 * block
    pieces_t = token_p_ss.shape[0]
    part = half // pieces_t
    z, fs, c = lax.axis_index("sp"), lax.axis_index("fs"), lax.axis_index("tp")
    y, x = fs // 2, lax.rem(fs, 2)
    h, p = z // 2, lax.rem(z, 2)
    zn = z + 1 - 2 * p
    zf = lax.rem(z + 2, n_sp)
    zfn = zf + 1 - 2 * p
    xn, yn = 2 * y + 1 - x, 2 * (1 - y) + x
    other = 1 - c
    low = h == 0
    quarter = 2 * p + x
    to_x, to_y, to_p, to_h, to_c = {"fs": xn}, {"fs": yn}, {"sp": zn}, {"sp": zf}, {"tp": other}

    def remote(src, dst, ss, rs, device):
        return pltpu.make_async_remote_copy(
            src_ref=src, dst_ref=dst, send_sem=ss, recv_sem=rs,
            device_id=device, device_id_type=MESH,
        )

    def at(start, size):
        return pl.ds(pl.multiple_of(start, size), size)

    inner = p != h
    to_m = {"sp": n_sp - 1 - z}
    barrier = pltpu.get_barrier_semaphore()
    for device in (to_x, to_y, to_p, to_h, to_c):
        pl.semaphore_signal(barrier, inc=1, device_id=device, device_id_type=MESH)

    @pl.when(inner)
    def _():
        pl.semaphore_signal(barrier, inc=1, device_id=to_m, device_id_type=MESH)

    groups = (((qw, hw), (kw, hw), (vw, hw)), ((ow, hw), (pw, feat)), ((mw, hw), (fw, feat)))
    quarters = (quarter, 2 * p + 1 - x, 2 * (1 - p) + 1 - x, 2 * (1 - p) + x)

    def row_block(zs, ys, xs):
        return at((zs * 4 + ys * 2 + xs) * rows, rows)

    def local_weights(g):
        copies = []
        for slot in (1, 2, 3, 0):
            start = 0
            for i, (ref, size) in enumerate(groups[g]):
                columns = pl.ds(start, size)
                if slot:
                    dst = stage.at[g, slot - 1, :, columns]
                else:
                    dst = w_all.at[g, row_block(z, y, x), columns]
                copies.append(
                    pltpu.make_async_copy(
                        ref.at[:, at(quarters[slot] * size, size)], dst, loc_w.at[g, slot, i]
                    )
                )
                start += size
        return copies

    locals_ = [local_weights(g) for g in range(3)]
    own_tokens = pltpu.make_async_copy(
        token_ref, x_all.at[at((2 * x + p) * block, block)], loc_s.at[0]
    )
    own_decay = pltpu.make_async_copy(decay_ref, dec.at[x, p], loc_s.at[1])
    own_init = pltpu.make_async_copy(mem_ref.at[h, quarter], init.at[x], loc_s.at[2])
    own_nrm = pltpu.make_async_copy(nrm_ref, nrm.at[x], loc_s.at[3])
    for copy in locals_[0]:
        copy.start()
    own_tokens.start()
    for copy in locals_[1] + locals_[2]:
        copy.start()
    for copy in (own_decay, own_init, own_nrm):
        copy.start()

    def x_copy(g, s, incoming=False):
        if s == 0:
            dst = w_all.at[g, row_block(z, y, 1 - x if incoming else x)]
        else:
            dst = transit.at[g]
        return remote(dst if incoming else stage.at[g, s], dst, x_ss.at[g, s], x_rs.at[g, s], to_x)

    def p_copy(g, s, incoming=False):
        dst = w_all.at[g, row_block(zn if incoming else z, y, 1 - x if s else x)]
        src = dst if incoming else (transit.at[g] if s else stage.at[g, 2])
        return remote(src, dst, p_ss.at[g, s], p_rs.at[g, s], to_p)

    def h_copy(g, k, s, incoming=False):
        source = (zf, zfn)[k] if incoming else (z, zn)[k]
        ref = w_all.at[g, row_block(source, y, 1 - x if s else x)]
        return remote(ref, ref, h_ss.at[g, k, s], h_rs.at[g, k, s], to_h)

    def y_copy(g, plane, s, incoming=False):
        ref = w_all.at[g, row_block(plane, 1 - y if incoming else y, 1 - x if s else x)]
        return remote(ref, ref, y_ss.at[g, plane, s], y_rs.at[g, plane, s], to_y)

    sent = []

    def go(copy):
        copy.start()
        sent.append(copy)

    def ready(g, slots):
        size = len(groups[g])
        for place, slot in enumerate((1, 2, 3, 0)):
            if slot in slots:
                for copy in locals_[g][place * size : (place + 1) * size]:
                    copy.wait()

    def begin_x(g):
        ready(g, (1, 2))
        go(x_copy(g, 1))
        go(x_copy(g, 0))

    def begin_p(g):
        ready(g, (3,))
        go(p_copy(g, 0))

    def begin_h(g):
        go(h_copy(g, 0, 0))

    def begin_z(g):
        begin_p(g)
        if g == 0:
            ready(g, (0,))
        begin_h(g)

    def begin_y(g):
        if g:
            ready(g, (0,))
        go(y_copy(g, z, 0))

    def after_x(g):
        x_copy(g, 1, True).wait_recv()
        go(p_copy(g, 1))
        x_copy(g, 0, True).wait_recv()
        go(h_copy(g, 0, 1))
        go(y_copy(g, z, 1))

    def after_p(g):
        for s in range(2):
            p_copy(g, s, True).wait_recv()
            go(h_copy(g, 1, s))
            go(y_copy(g, zn, s))

    def after_h(g, k):
        for s in range(2):
            h_copy(g, k, s, True).wait_recv()
            go(y_copy(g, (zf, zfn)[k], s))

    def after_y(g, plane):
        for s in range(2):
            y_copy(g, plane, s, True).wait_recv()

    def all_y(g):
        for plane in (z, zn, zf, zfn):
            after_y(g, plane)

    def token_rows(j, b, side, i):
        return at((2 * j + b) * block + side * half + i * part, part)

    def token_p(i, incoming=False):
        b = 1 - p if incoming else p
        dst = x_all.at[token_rows(x, b, c, i)]
        src = dst if incoming else token_ref.at[at(c * half + i * part, part)]
        return remote(src, dst, token_p_ss.at[i], token_p_rs.at[i], to_p)

    def token_x(kind, i, incoming=False):
        b = 1 - p if kind else p
        dst = x_all.at[token_rows(1 - x if incoming else x, b, c, i)]
        src = dst if incoming or kind else token_ref.at[at(c * half + i * part, part)]
        return remote(src, dst, tx_ss.at[kind, i], tx_rs.at[kind, i], to_x)

    places = ((x, 1 - p), (1 - x, p), (1 - x, 1 - p))

    def token_swap(which, i, incoming=False):
        j, b = places[which]
        ref = x_all.at[token_rows(j, b, other if incoming else c, i)]
        return remote(ref, ref, tw_ss.at[which, i], tw_rs.at[which, i], to_c)

    edge_rows = halo_tok.shape[1]

    def edge_copy(which):
        return remote(
            token_ref.at[at((1 - h) * (block - edge_rows), edge_rows)], halo_tok.at[x],
            e_ss.at[which], e_rs.at[0], (to_h, to_m)[which],
        )

    def edges(action):
        @pl.when(inner)
        def _():
            for which in range(2):
                action(edge_copy(which))

    def edge_x(incoming=False):
        ref = halo_tok.at[1 - x if incoming else x]
        return remote(ref, ref, e_ss.at[2], e_rs.at[1], to_x)

    def normalise_edges():
        wide = halo_tok[...].reshape(2 * edge_rows, width).astype(jnp.float32)
        normed[4 * block :, :] = (
            wide
            * lax.rsqrt(jnp.mean(wide * wide, axis=-1, keepdims=True) + norm_eps)
            * gain_ref[...]
        ).astype(jnp.bfloat16)

    def decay_p(incoming=False):
        dst = dec.at[x, 1 - p if incoming else p]
        return remote(dst if incoming else decay_ref, dst, d_ss.at[0], d_rs.at[0], to_p)

    def decay_x(kind, incoming=False):
        dst = dec.at[1 - x if incoming else x, 1 - p if kind else p]
        src = dst if incoming or kind else decay_ref
        return remote(src, dst, d_ss.at[1 + kind], d_rs.at[1 + kind], to_x)

    def init_x(which, incoming=False):
        dst = (init, nrm)[which].at[1 - x if incoming else x]
        src = (mem_ref.at[h, 2 * p + 1 - x], nrm_ref)[which]
        return remote(dst if incoming else src, dst, i_ss.at[which], i_rs.at[which], to_x)

    def normalise(j, b):
        step = 64

        def body(i, carry):
            here = at((2 * j + b) * block + i * step, step)
            wide = x_all[here, :].astype(jnp.float32)
            normed[here, :] = (
                wide
                * lax.rsqrt(jnp.mean(wide * wide, axis=-1, keepdims=True) + norm_eps)
                * gain_ref[...]
            ).astype(jnp.bfloat16)
            return carry

        lax.fori_loop(0, block // step, body, 0)
        here = at((2 * j + b) * block, block)
        pre_rows[2 * j + b] = transposed_dot(normed[here, :], gmat[...]).T[:8]

    def scoped(name, function, *args):
        with jax.named_scope(name):
            return function(*args)

    def token_arrivals_p(these):
        for i in these:
            token_p(i, True).wait_recv()
            go(token_swap(0, i))
            go(token_x(1, i))

    def token_arrivals_x(kind, these):
        for i in these:
            token_x(kind, i, True).wait_recv()
            go(token_swap(1 + kind, i))

    def swapped(which):
        for i in range(pieces_t):
            token_swap(which, i, True).wait_recv()
        normalise(*places[which])

    def pick_gates():
        gmat[...] = jnp.zeros_like(gmat)
        pick = lax.broadcasted_iota(jnp.int32, (4, width), 0) == quarter
        row16 = lax.broadcasted_iota(jnp.int32, (16, width), 0)
        gates16 = jnp.zeros((16, width), jnp.float32)
        for i in range(4):
            row = jnp.sum(
                jnp.where(pick, gate_ref[i].astype(jnp.float32), 0.0), axis=0, keepdims=True
            )
            gates16 = jnp.where((row16 == i) | (row16 == i + 4), row, gates16)
        gmat[0:16, :] = gates16.astype(jnp.bfloat16)

    scoped("barrier", pl.semaphore_wait, barrier, 5 + inner.astype(jnp.int32))
    begin_x(0)
    begin_z(0)
    begin_y(0)
    edges(lambda copy: copy.start())
    own_decay.wait()
    go(decay_p())
    go(decay_x(0))
    go(token_p(0))
    begin_x(1)
    for i in range(pieces_t):
        go(token_x(0, i))
    begin_y(1)
    scoped("pick", pick_gates)
    scoped("tok_own", own_tokens.wait)
    scoped("norm_own", normalise, x, p)
    scoped("after_x_0", after_x, 0)
    remote(halo_tok.at[x], halo_tok.at[x], e_ss.at[0], e_rs.at[0], to_h).wait_recv()
    go(edge_x())
    scoped("after_p_0", after_p, 0)
    for i in range(1, pieces_t):
        go(token_p(i))
    begin_z(1)
    scoped("after_x_1", after_x, 1)
    scoped("after_h_0", after_h, 0, 0)
    scoped("tok_p", token_arrivals_p, (0,))
    scoped("tok_x0", token_arrivals_x, 0, (0, 1))
    scoped("after_h_0", after_h, 0, 1)
    scoped("tok_p", token_arrivals_p, (1,))
    scoped("tok_x0", token_arrivals_x, 0, (2, 3))
    scoped("norm_x", swapped, 1)
    edge_x(True).wait_recv()
    normalise_edges()
    scoped("tok_p", token_arrivals_p, (2, 3))
    decay_p(True).wait_recv()
    go(decay_x(1))
    go(init_x(0))
    go(init_x(1))
    begin_x(2)
    begin_y(2)
    scoped("norm_p", swapped, 0)
    scoped("after_y_0", all_y, 0)

    def project(g, place, store):
        i = 2 * place[0] + place[1]
        store(i, jnp.dot(
            normed[at(i * block, block), :], w_all[g], preferred_element_type=jnp.float32
        ).astype(jnp.bfloat16))

    def store_a(i, value):
        proj_a[at(i * block, block), :] = value

    for place in ((x, p), places[0], places[1]):
        scoped("project_0", project, 0, place, store_a)
    scoped("tok_x1", token_arrivals_x, 1, (0, 1))
    scoped("after_p_1", after_p, 1)
    scoped("tok_x1", token_arrivals_x, 1, (2, 3))
    scoped("after_h_1", after_h, 1, 0)
    scoped("norm_px", swapped, 2)
    decay_x(0, True).wait_recv()
    decay_x(1, True).wait_recv()

    with jax.named_scope("gates"):
        tall = []
        for j in range(2):
            tall.append(jnp.concatenate([pre_rows[2 * j], pre_rows[2 * j + 1]], axis=1))
        row8 = lax.broadcasted_iota(jnp.int32, (8, span), 0)
        gates = jnp.where(row8 < 4, tall[0], tall[1])
        extra = jnp.zeros((8, span), jnp.float32)
        for i in range(4):
            gates = gates + jnp.where((row8 == i) | (row8 == i + 4), bias_ref[i, quarter], 0.0)
        for j in range(2):
            for direction in range(2):
                value = jnp.concatenate(
                    [dec[j, b, direction, pl.ds(quarter, 1), :] for b in range(2)], axis=1
                )
                extra = jnp.where(row8 == 4 * j + 1 + 2 * direction, value, extra)
        forget = jnp.minimum(gates, 0.0) - jnp.log1p(jnp.exp(-jnp.abs(gates))) + extra
        sum_f = pltpu.roll(scan_lanes(forget, jnp.add, 0.0, False), 7, 0)
        sum_b = pltpu.roll(scan_lanes(forget, jnp.add, 0.0, True), 7, 0)
        level_f = gates - sum_f
        level_b = gates - sum_b
        run_f = scan_lanes(level_f, jnp.maximum, -1e30, False)
        run_b = scan_lanes(level_b, jnp.maximum, -1e30, True)
        top_f = jnp.maximum(run_f[:, span - 1 : span], 0.0)
        top_b = jnp.maximum(run_b[:, 0:1], 0.0)
        end_f = sum_f[:, span - 1 : span] + top_f
        end_b = sum_b[:, 0:1] + top_b
        aux_out[2] = jnp.broadcast_to(jnp.where(low, end_f, end_b), (8, hw))

    def message(which, incoming=False):
        src = (aux_out, state_out)[which]
        dst = (aux_in, state_in)[which]
        return remote(dst if incoming else src, dst, m_ss.at[which], m_rs.at[which], to_h)

    scoped("project_0", project, 0, places[2], store_a)

    with jax.named_scope("state"):
        scale_bits = -0.5 * math.log2(hw)
        lf2 = level_f * LOG2E + scale_bits
        lb2 = level_b * LOG2E + scale_bits
        own_init.wait()
        own_nrm.wait()
        init_x(0, True).wait_recv()
        init_x(1, True).wait_recv()
        leave_f = jnp.exp2(lf2 - top_f * LOG2E)
        leave_b = jnp.exp2(lb2 - top_b * LOG2E)
        keep_f = jnp.exp(-top_f)
        keep_b = jnp.exp(-top_b)
        for j in range(2):
            here = slice(j * span, (j + 1) * span)
            own = jnp.where(low, leave_f[4 * j : 4 * j + 1], leave_b[4 * j + 2 : 4 * j + 3])
            kept = jnp.where(low, keep_f[4 * j : 4 * j + 1], keep_b[4 * j + 2 : 4 * j + 3])
            values = proj_a[here, 2 * hw : 3 * hw].astype(jnp.float32).T
            values_t[j] = values.astype(jnp.bfloat16)
            values = values * own
            lhs = jnp.concatenate(
                [values, jnp.broadcast_to(own, (8, span))], axis=0
            ).astype(jnp.bfloat16)
            grown = jnp.dot(lhs, proj_a[here, hw : 2 * hw], preferred_element_type=jnp.float32)
            state_out[j] = (kept * init[j] + grown[:hw]).astype(jnp.bfloat16)
            aux_out[j] = kept * nrm[j, h, pl.ds(quarter, 1), :] + grown[hw:]
    go(message(0))
    go(message(1))
    begin_p(2)
    begin_h(2)

    with jax.named_scope("levels"):
        flat[16:, :] = jnp.zeros_like(flat[16:, :])
        flat[0:8, :] = lf2
        flat[8:16, :] = lb2
        cols[...] = flat[...].T
        run_rows[0] = run_f * LOG2E
        run_rows[1] = run_b * LOG2E

    def attend(j):
        here = slice(j * span, (j + 1) * span)
        f, b = 4 * j, 4 * j + 2
        levels = [jnp.broadcast_to(cols[:, k : k + 1], (span, half)) for k in (f, 8 + b)]
        for i in range(4):
            r0 = i * half
            mine = slice(j * span + r0, j * span + r0 + half)
            score = transposed_dot(proj_a[here, hw : 2 * hw], proj_a[mine, 0:hw])
            for which, first, last in ((0, 0, r0 + half), (1, r0, span)):
                row = (f, b)[which]
                peak = run_rows[which, row : row + 1, r0 : r0 + half]
                weight = jnp.exp2(levels[which][first:last] - peak) * score[first:last]
                s = first + lax.broadcasted_iota(jnp.int32, weight.shape, 0)
                t = r0 + lax.broadcasted_iota(jnp.int32, weight.shape, 1)
                weight = jnp.where(s >= t if which else s <= t, weight, 0.0)
                within[which, j, :, r0 : r0 + half] = jnp.dot(
                    values_t[j, :, first:last], weight.astype(jnp.bfloat16),
                    preferred_element_type=jnp.float32,
                )
                dens[which, j : j + 1, r0 : r0 + half] = jnp.sum(weight, axis=0, keepdims=True)

    scoped("attend_0", attend, 0)
    scoped("attend_1", attend, 1)
    scoped("after_x_2", after_x, 2)
    scoped("after_h_1", after_h, 1, 1)
    scoped("after_p_2", after_p, 2)
    scoped("after_y_1", all_y, 1)

    def project_b():
        for i in range(4):
            last_rows = 2 * edge_rows if i == 3 else 0
            value = jnp.dot(
                normed[i * block : (i + 1) * block + last_rows, :], w_all[1],
                preferred_element_type=jnp.float32,
            ).astype(jnp.bfloat16)
            proj_b[i * block : (i + 1) * block, :] = value[:block, :hw]
            start = 8 + (i % 2) * block
            pool_buf[i // 2, start : start + block, :] = value[:block, hw:].astype(jnp.float32)
        beyond = value[block:, hw:].astype(jnp.float32)
        zero = jnp.zeros((8, feat), jnp.float32)
        for j in range(2):
            mine = beyond[j * edge_rows : (j + 1) * edge_rows]
            pool_buf[j, 0:8, :] = jnp.where(low, zero, mine[edge_rows - 8 :])
            pool_buf[j, span + 8 : span + 16, :] = jnp.where(low, mine[:8], zero)

    scoped("project_1", project_b)
    scoped("state_in", message(1, True).wait_recv)
    scoped("aux_in", message(0, True).wait_recv)

    with jax.named_scope("enter"):
        arrived = aux_in[2, :, 0:1]
        enter_f = jnp.where(low, 0.0, arrived)
        enter_b = jnp.where(low, arrived, 0.0)
        factors = []
        for run, enter, summed in ((run_f, enter_f, sum_f), (run_b, enter_b, sum_b)):
            peak = jnp.maximum(run, enter)
            factors.append(
                (jnp.exp(run - peak), jnp.exp(enter - peak), jnp.exp(-(summed + peak)))
            )

    def finish(j):
        own_n = jnp.broadcast_to(nrm[j, h, pl.ds(quarter, 1), :], (8, hw))
        there = state_in[j].astype(jnp.float32)
        carry_in = jnp.concatenate(
            [
                jnp.where(low, init[j], there),
                jnp.where(low, there, init[j]),
                jnp.where(low, own_n, aux_in[j]),
                jnp.where(low, aux_in[j], own_n),
            ],
            axis=0,
        )
        coarse = carry_in.astype(jnp.bfloat16)
        fine = (carry_in - coarse.astype(jnp.float32)).astype(jnp.bfloat16)
        q = proj_a[j * span : (j + 1) * span, 0:hw]
        carry = transposed_dot(
            jnp.concatenate([coarse, fine], axis=1), jnp.concatenate([q, q], axis=1)
        )
        both = []
        for which in range(2):
            row = 4 * j + 2 * which
            grow, decay, floor = (part[row : row + 1] for part in factors[which])
            den0 = carry[2 * hw + 8 * which : 2 * hw + 8 * which + 1]
            den = grow * dens[which, j : j + 1, :] + decay * den0
            share = 1.0 / jnp.maximum(jnp.abs(den), floor)
            both.append(
                (grow * share) * within[which, j]
                + (decay * share) * carry[which * hw : (which + 1) * hw]
            )
        summed = both[0] + both[1]
        summed = summed * lax.rsqrt(jnp.mean(summed * summed, axis=0, keepdims=True) + norm_eps)
        out = (
            summed.T
            * hgain_ref[pl.ds(quarter, 1), :]
            * jax.nn.sigmoid(proj_b[j * span : (j + 1) * span, :].astype(jnp.float32))
        ).astype(jnp.bfloat16)
        for i in range(4):
            place = (i % 2) * span + (2 * j + i // 2) * half
            act[place : place + half, 0:hw] = out[i * half : (i + 1) * half]

    scoped("finish", finish, 0)
    scoped("finish", finish, 1)

    with jax.named_scope("pooling"):
        group = (c * 4 + quarter) * feat * 4 // width
        for k in range(4):

            @pl.when(group == k)
            def _(k=k):
                reach = 2 ** k
                t = h * span + lax.broadcasted_iota(jnp.int32, (span, 1), 0)
                counted = jnp.minimum(t + reach - 1, n_sp * block - 1) - jnp.maximum(t - reach, 0) + 1
                counted = counted.astype(jnp.float32)
                length = span + 16
                for j in range(2):
                    window = pool_buf[j]
                    for e in range(k + 1):
                        window = window + pltpu.roll(window, length - 2 ** e, 0)
                    if reach < 8:
                        window = pltpu.roll(window, length - (8 - reach), 0)
                    value = window[:span] / counted - pool_buf[j, 8 : 8 + span, :]
                    value = value.astype(jnp.bfloat16)
                    for i in range(4):
                        place = (i % 2) * span + (2 * j + i // 2) * half
                        act[place : place + half, hw:] = value[i * half : (i + 1) * half]

    count = give.shape[0]
    tile = width // count
    each = count // 4
    planes = (2 * h, 2 * h + 1, 2 * (1 - h), 2 * (1 - h) + 1)

    def columns_of(n):
        return at(planes[n // each] * (width // 4) + (n % each) * tile, tile)

    def mixed(n):
        return n % 2 == 1

    def swap(n):
        return remote(give.at[n], take.at[n], sw_ss.at[n], sw_rs.at[n], to_c)

    def first_stage(n, slot, incoming=False):
        dst = l1.at[n, slot]
        return remote(
            dst if incoming else s1.at[n, slot], dst, r1_ss.at[n, slot], r1_rs.at[n, slot],
            to_p if mixed(n) else to_x,
        )

    def second_stage(n, incoming=False):
        return remote(
            l2.at[n] if incoming else s2.at[n], l2.at[n], r2_ss.at[n], r2_rs.at[n],
            to_x if mixed(n) else to_p,
        )

    def product(side, n):
        return transposed_dot(act[at(side * span, span), :], w_all[2, columns_of(n), :])

    home = 2 * x + p
    both = 2 * (1 - x) + 1 - p

    def first(n):
        part_sum = product(c, n)
        swap(n).wait_recv()
        total[n] = part_sum.reshape(total.shape[1:]) + take[n].astype(jnp.float32)
        near, middle = 2 * (1 - x) + p, 2 * x + 1 - p
        if mixed(n):
            near, middle = middle, near
        s1[n, 1] = total[n, both].astype(jnp.bfloat16)
        go(first_stage(n, 1))
        s1[n, 0] = total[n, near].astype(jnp.bfloat16)
        go(first_stage(n, 0))

    def second(n):
        middle = 2 * (1 - x) + p if mixed(n) else 2 * x + 1 - p
        first_stage(n, 1, True).wait_recv()
        s2[n] = (total[n, middle] + l1[n, 1].astype(jnp.float32)).astype(jnp.bfloat16)
        go(second_stage(n))

    def last(n):
        first_stage(n, 0, True).wait_recv()
        second_stage(n, True).wait_recv()
        o_ref[:, columns_of(n)] = (
            total[n, home] + l1[n, 0].astype(jnp.float32) + l2[n].astype(jnp.float32)
        ).astype(jnp.bfloat16)

    for q in range(4):
        mine = range(q * each, (q + 1) * each)
        scoped("plane#q=%d" % q, after_y, 2, planes[q])
        with jax.named_scope("give#q=%d" % q):
            for n in mine:
                give[n] = product(other, n).astype(jnp.bfloat16).reshape(give.shape[1:])
                go(swap(n))
        with jax.named_scope("first#q=%d" % q):
            for n in mine:
                first(n)
        if q == 0:
            scoped("after_h_2", after_h, 2, 0)
        if q == 1:
            scoped("after_h_2", after_h, 2, 1)
        if q:
            with jax.named_scope("second#q=%d" % (q - 1)):
                for n in mine:
                    second(n - each)
    with jax.named_scope("last#q=0"):
        for n in range(2 * each):
            last(n)
    with jax.named_scope("second#q=3"):
        for n in range(3 * each, count):
            second(n)
    with jax.named_scope("last#q=1"):
        for n in range(2 * each, count):
            last(n)

    with jax.named_scope("drain"):
        for copy in sent:
            copy.wait_send()
        edges(lambda copy: copy.wait_send())


def by_group(
    tokens, norm_gain, query_weight, key_weight, value_weight, outgate_weight, gate_weight,
    gate_bias, decay_extra, init_memory, init_normalizer, head_gain, pool_weight, mem_out_weight,
    pool_out_weight,
):
    n_sp = lax.axis_size("sp")
    block, width = tokens.shape[1:]
    rows = query_weight.shape[0]
    hw = head_gain.shape[1]
    feat = pool_weight.shape[1] // 4
    columns = 3 * hw
    half, span, everything = block // 2, 2 * block, 4 * block
    count, pieces = 8, 4
    tile = width // count
    f32, bf16 = jnp.float32, jnp.bfloat16
    dma = pltpu.SemaphoreType.DMA
    vmem = pl.BlockSpec(memory_space=pltpu.VMEM)
    anywhere = pl.BlockSpec(memory_space=pl.ANY)
    smem = pl.BlockSpec(memory_space=pltpu.SMEM)
    mixed = pl.pallas_call(
        functools.partial(layer_kernel, n_sp),
        out_shape=jax.ShapeDtypeStruct((half, width), bf16),
        in_specs=[
            anywhere, vmem, anywhere, anywhere, anywhere, anywhere, vmem, smem, anywhere, anywhere,
            anywhere, vmem, anywhere, anywhere, anywhere,
        ],
        out_specs=vmem,
        scratch_shapes=[
            pltpu.VMEM((everything, width), bf16),
            pltpu.VMEM((everything + 16, width), bf16),
            pltpu.VMEM((3, width, columns), bf16),
            pltpu.VMEM((3, 3, rows, columns), bf16),
            pltpu.VMEM((3, rows, columns), bf16),
            pltpu.VMEM((128, width), bf16),
            pltpu.VMEM((2, 2) + decay_extra.shape[1:], f32),
            pltpu.VMEM((2, hw, hw), f32),
            pltpu.VMEM((2,) + init_normalizer.shape[1:], f32),
            pltpu.VMEM((everything, columns), bf16),
            pltpu.VMEM((everything, hw), bf16),
            pltpu.VMEM((2, span + 16, feat), f32),
            pltpu.VMEM((everything, columns), bf16),
            pltpu.VMEM((2, 2, hw, span), f32),
            pltpu.VMEM((2, 8, span), f32),
            pltpu.VMEM((2, hw, span), bf16),
            pltpu.VMEM((4, 8, block), f32),
            pltpu.VMEM((128, span), f32),
            pltpu.VMEM((span, 128), f32),
            pltpu.VMEM((2, 8, span), f32),
            pltpu.VMEM((3, 8, hw), f32),
            pltpu.VMEM((3, 8, hw), f32),
            pltpu.VMEM((2, hw, hw), bf16),
            pltpu.VMEM((2, hw, hw), bf16),
            pltpu.VMEM((2, 8, width), bf16),
            pltpu.VMEM((count, 4, half, tile), bf16),
            pltpu.VMEM((count, 4, half, tile), bf16),
            pltpu.VMEM((count, 4, half, tile), f32),
            pltpu.VMEM((count, 2, half, tile), bf16),
            pltpu.VMEM((count, 2, half, tile), bf16),
            pltpu.VMEM((count, half, tile), bf16),
            pltpu.VMEM((count, half, tile), bf16),
            dma((3, 4, 3)),
            dma((4,)),
            dma((3, 2)), dma((3, 2)),
            dma((3, 2)), dma((3, 2)),
            dma((3, 2, 2)), dma((3, 2, 2)),
            dma((3, 4, 2)), dma((3, 4, 2)),
            dma((pieces,)), dma((pieces,)),
            dma((2, pieces)), dma((2, pieces)),
            dma((3, pieces)), dma((3, pieces)),
            dma((3,)), dma((3,)),
            dma((2,)), dma((2,)),
            dma((2,)), dma((2,)),
            dma((3,)), dma((2,)),
            dma((count,)), dma((count,)),
            dma((count, 2)), dma((count, 2)),
            dma((count,)), dma((count,)),
        ],
        compiler_params=pltpu.CompilerParams(
            collective_id=0, has_side_effects=True, vmem_limit_bytes=60 * 2**20
        ),
        name="layer",
    )(
        tokens[0], norm_gain[None], query_weight, key_weight, value_weight, outgate_weight,
        gate_weight, gate_bias, decay_extra[0], init_memory[0], init_normalizer[0], head_gain,
        pool_weight, mem_out_weight, pool_out_weight,
    )
    return mixed[None]


def solution(mesh):
    placed = (
        P("fs", "sp", None),
        P(),
        P(("sp", "fs"), "tp"),
        P(("sp", "fs"), "tp"),
        P(("sp", "fs"), "tp"),
        P(("sp", "fs"), "tp"),
        P(None, "tp", None),
        P(None, "tp"),
        P("fs", None, "tp", "sp"),
        P("fs", None, "tp", None, None),
        P("fs", None, "tp", None),
        P("tp", None),
        P(("sp", "fs"), "tp"),
        P(("sp", "fs"), "tp"),
        P(("sp", "fs"), "tp"),
    )

    def body(*args):
        heads, width = args[11].shape
        features = args[12].shape[1]
        block, model_width = args[0].shape[1:]
        fits = (
            lax.axis_size("tp") == 2
            and lax.axis_size("fs") == 4
            and lax.axis_size("sp") == 4
            and heads == 4
            and width == 128
            and features == 8 * width
            and model_width == 2 * features
            and block == 2 * width
        )
        return (by_group if fits else per_device)(*args)

    return jax.shard_map(
        body,
        mesh=mesh,
        in_specs=placed,
        out_specs=P("fs", ("sp", "tp"), None),
        check_vma=False,
    )
```

```python
import functools
import math

import jax
import jax.numpy as jnp
from jax import lax
from jax.experimental import pallas as pl
from jax.experimental.pallas import tpu as pltpu
from jax.sharding import PartitionSpec as P

MESH = pl.DeviceIdType.MESH

HALO = 8


norm_eps = 1e-06
exact_mode = lax.Precision.HIGHEST


def carried_in(x, axis, combine, identity, reverse):
    length, position = (lax.axis_size(axis), lax.axis_index(axis))
    everything = jax.tree.map(lambda part: lax.all_gather(part, axis), x)
    start = jax.tree.map(
        lambda part, zero: jnp.broadcast_to(jnp.asarray(zero, part.dtype), part.shape), x, identity
    )

    def lap(k, before):
        at = length - 1 - k if reverse else k
        reached = at > position if reverse else at < position
        new = combine(before, jax.tree.map(lambda part: part[at], everything))
        return jax.tree.map(lambda a, b: jnp.where(reached, a, b), new, before)

    return lax.fori_loop(0, length, lap, start)


def padded_2(block, sides, width):
    for axis, dim in sides:
        count = lax.axis_size(axis)
        forward = [(i, i + 1) for i in range(count - 1)]
        backward = [(target, source) for source, target in forward]
        low = lax.ppermute(
            lax.slice_in_dim(block, block.shape[dim] - width, None, axis=dim), axis, forward
        )
        high = lax.ppermute(lax.slice_in_dim(block, 0, width, axis=dim), axis, backward)
        block = jnp.concatenate([low, block, high], axis=dim)
    return block


def block_output(
    query_rows, key_rows, value_rows, input_gate, log_forget, memory, normalizer, stabilizer
):
    block_len = query_rows.shape[1]
    key_scale = key_rows.shape[-1] ** (-0.5)
    lower_mask = jnp.tril(jnp.ones((block_len, block_len), dtype=bool))
    summed = jnp.cumsum(log_forget, axis=-1)
    log_decay = jnp.where(
        lower_mask, summed[:, :, None] - summed[:, None, :] + input_gate[:, None, :], -jnp.inf
    )
    log_carry = stabilizer[:, None] + summed
    running_max = jnp.maximum(log_carry, jnp.max(log_decay, axis=-1))
    scores = (
        jnp.einsum("btd,bsd->bts", query_rows, key_rows, preferred_element_type=jnp.float32)
        * key_scale
    )
    inner_weight = jnp.exp(log_decay - running_max[:, :, None]) * scores
    weight_rounded = inner_weight.astype(jnp.bfloat16)
    carry_weight = jnp.exp(log_carry - running_max)
    query_wide = query_rows.astype(jnp.float32)
    numerator = carry_weight[:, :, None] * jnp.einsum(
        "bed,btd->bte", memory, query_wide, precision=exact_mode
    )
    numerator = numerator + jnp.einsum(
        "bts,bse->bte", weight_rounded, value_rows, preferred_element_type=jnp.float32
    )
    denominator = carry_weight * jnp.einsum(
        "bd,btd->bt", normalizer, query_wide, precision=exact_mode
    )
    denominator = denominator + jnp.sum(inner_weight, axis=-1)
    return numerator / jnp.maximum(jnp.abs(denominator), jnp.exp(-running_max))[:, :, None]


def block_summary(key_rows, value_rows, input_gate, log_forget):
    key_wide = key_rows.astype(jnp.float32) * key_rows.shape[-1] ** (-0.5)
    summed = jnp.cumsum(log_forget, axis=-1)
    forget_total = summed[:, -1]
    log_weight = forget_total[:, None] - summed + input_gate
    running_max = jnp.max(log_weight, axis=-1)
    weights = jnp.exp(log_weight - running_max[:, None])
    memory = jnp.einsum(
        "bse,bsd->bed",
        weights[:, :, None] * value_rows.astype(jnp.float32),
        key_wide,
        precision=exact_mode,
    )
    normalizer = jnp.einsum("bs,bsd->bd", weights, key_wide, precision=exact_mode)
    return (memory, normalizer, running_max, forget_total)


def combine(earlier, latter):
    early_memory, early_norm, early_max, early_total = earlier
    late_memory, late_norm, late_max, late_total = latter
    joint_max = jnp.maximum(early_max + late_total, late_max)
    early_scale = jnp.exp(early_max + late_total - joint_max)
    late_scale = jnp.exp(late_max - joint_max)
    memory = early_scale[:, None, None] * early_memory + late_scale[:, None, None] * late_memory
    normalizer = early_scale[:, None] * early_norm + late_scale[:, None] * late_norm
    return (memory, normalizer, joint_max, early_total + late_total)


def span_sweep(
    query_rows, key_rows, value_rows, input_gate, log_forget, memory, normalizer, stabilizer, span
):
    block_count = query_rows.shape[1] // span

    def to_blocks(array):
        shaped = array.reshape((array.shape[0], block_count, span) + array.shape[2:])
        return jnp.moveaxis(shaped, 1, 0)

    def advance(carried, pieces):
        query_blk, key_blk, value_blk, gate_blk, forget_blk = pieces
        result = block_output(
            query_blk, key_blk, value_blk, gate_blk, forget_blk, carried[0], carried[1], carried[2]
        )
        return (combine(carried, block_summary(key_blk, value_blk, gate_blk, forget_blk)), result)

    initial = (memory, normalizer, stabilizer, jnp.zeros_like(stabilizer))
    ignored, outputs = lax.scan(
        advance,
        initial,
        tuple(
            (
                to_blocks(array)
                for array in (query_rows, key_rows, value_rows, input_gate, log_forget)
            )
        ),
    )
    return jnp.moveaxis(outputs, 0, 1).reshape(query_rows.shape[:2] + (value_rows.shape[2],))


def reverse_time(array):
    return jnp.flip(array, axis=1)


def to_heads(matrix, head_count):
    shaped = matrix.reshape(matrix.shape[0], head_count, matrix.shape[1] // head_count)
    return shaped.transpose(1, 0, 2)


def pool_window(padded, positions, channels, seq_len, group_size):
    row_count = positions.shape[0]
    group_index = channels // group_size
    reach_left = jnp.left_shift(jnp.ones_like(group_index), group_index)
    reach_right = reach_left - 1
    window_sum = jnp.zeros((row_count, channels.shape[0]), jnp.float32)
    for offset in range(-HALO, HALO):
        inside = ((offset >= -reach_left) & (offset <= reach_right)).astype(jnp.float32)
        window_sum = window_sum + inside * padded[HALO + offset : HALO + offset + row_count]
    first_pos = jnp.maximum(positions[:, None] - reach_left[None, :], 0)
    last_pos = jnp.minimum(positions[:, None] + reach_right[None, :], seq_len - 1)
    counted = (last_pos - first_pos + 1).astype(jnp.float32)
    centre = padded[HALO : HALO + row_count]
    return (window_sum / counted - centre).astype(jnp.bfloat16)


def per_device(
    tokens,
    norm_gain,
    query_weight,
    key_weight,
    value_weight,
    outgate_weight,
    gate_weight,
    gate_bias,
    decay_extra,
    init_memory,
    init_normalizer,
    head_gain,
    pool_weight,
    mem_out_weight,
    pool_out_weight,
):
    block_len = tokens.shape[1]
    model_width = tokens.shape[2]
    head_count, head_width = head_gain.shape
    span = math.gcd(block_len, 256)
    flattened = tokens[0].astype(jnp.float32)
    normed = (
        flattened
        * lax.rsqrt(jnp.mean(flattened * flattened, axis=-1, keepdims=True) + norm_eps)
        * norm_gain
    ).astype(jnp.bfloat16)
    zero_start = tuple(
        (
            jnp.zeros((block_len, weight.shape[1]), jnp.float32)
            for weight in (query_weight, key_weight, value_weight, outgate_weight, pool_weight)
        )
    )
    zero_start = zero_start + (
        jnp.zeros((model_width, mem_out_weight.shape[1]), jnp.bfloat16),
        jnp.zeros((model_width, pool_out_weight.shape[1]), jnp.bfloat16),
    )
    line_query, line_key, line_value, line_outgate, line_pool, line_mem_out, line_pool_out = (
        lax.all_gather(query_weight, "fs", axis=0, tiled=True),
        lax.all_gather(key_weight, "fs", axis=0, tiled=True),
        lax.all_gather(value_weight, "fs", axis=0, tiled=True),
        lax.all_gather(outgate_weight, "fs", axis=0, tiled=True),
        lax.all_gather(pool_weight, "fs", axis=0, tiled=True),
        lax.all_gather(mem_out_weight, "fs", axis=0, tiled=True),
        lax.all_gather(pool_out_weight, "fs", axis=0, tiled=True),
    )
    pieces = (
        lax.all_gather(line_query, "sp", axis=0, tiled=True),
        lax.all_gather(line_key, "sp", axis=0, tiled=True),
        lax.all_gather(line_value, "sp", axis=0, tiled=True),
        lax.all_gather(line_outgate, "sp", axis=0, tiled=True),
        lax.all_gather(line_pool, "sp", axis=0, tiled=True),
        lax.all_gather(line_mem_out, "sp", axis=0, tiled=True),
        lax.all_gather(line_pool_out, "sp", axis=0, tiled=True),
    )
    partial_sums = tuple(
        (
            jnp.dot(normed, weight_rows, preferred_element_type=jnp.float32)
            for weight_rows in pieces[:5]
        )
    )
    collected = tuple((weight_rows for weight_rows in pieces[5:]))
    folded = partial_sums + collected
    query_proj, key_proj, value_proj, outgate, pool_input = tuple(
        (running.astype(jnp.bfloat16) for running in folded[:5])
    )
    mem_weight_all = folded[5]
    pool_weight_all = folded[6]
    gate_pre = lax.dot_general(
        normed,
        gate_weight.reshape(4 * head_count, model_width),
        (((1,), (1,)), ((), ())),
        preferred_element_type=jnp.float32,
    ) + gate_bias.reshape(4 * head_count)
    gate_pre = gate_pre.reshape(block_len, 4, head_count).transpose(1, 2, 0)
    query_heads = to_heads(query_proj, head_count)
    key_heads = to_heads(key_proj, head_count)
    value_heads = to_heads(value_proj, head_count)
    forward_forget = jax.nn.log_sigmoid(gate_pre[1]) + decay_extra[0, 0]
    backward_forget = jax.nn.log_sigmoid(gate_pre[3]) + decay_extra[0, 1]
    zero_rows = jnp.zeros((head_count,), jnp.float32)
    identity = (
        jnp.zeros((head_count, head_width, head_width), jnp.float32),
        jnp.zeros((head_count, head_width), jnp.float32),
        jnp.full((head_count,), -1e30, jnp.float32),
        zero_rows,
    )
    front_memory, front_norm, front_max, front_total = block_summary(
        key_heads, value_heads, gate_pre[0], forward_forget
    )
    prefix = carried_in(
        (front_memory, front_norm, front_max, front_total), "sp", combine, identity, False
    )
    incoming = combine((init_memory[0, 0], init_normalizer[0, 0], zero_rows, zero_rows), prefix)
    forward_out = span_sweep(
        query_heads,
        key_heads,
        value_heads,
        gate_pre[0],
        forward_forget,
        incoming[0],
        incoming[1],
        incoming[2],
        span,
    )
    back_query = reverse_time(query_heads)
    back_key = reverse_time(key_heads)
    back_value = reverse_time(value_heads)
    back_gate = reverse_time(gate_pre[2])
    back_forget = reverse_time(backward_forget)
    rear_memory, rear_norm, rear_max, rear_total = block_summary(
        back_key, back_value, back_gate, back_forget
    )
    suffix = carried_in(
        (rear_memory, rear_norm, rear_max, rear_total), "sp", combine, identity, True
    )
    back_incoming = combine(
        (init_memory[0, 1], init_normalizer[0, 1], zero_rows, zero_rows), suffix
    )
    backward_out = reverse_time(
        span_sweep(
            back_query,
            back_key,
            back_value,
            back_gate,
            back_forget,
            back_incoming[0],
            back_incoming[1],
            back_incoming[2],
            span,
        )
    )
    summed_dirs = (forward_out + backward_out).transpose(1, 0, 2)
    normed_heads = (
        summed_dirs
        * lax.rsqrt(jnp.mean(summed_dirs * summed_dirs, axis=-1, keepdims=True) + norm_eps)
        * head_gain
    )
    out_gate = jax.nn.sigmoid(
        outgate.astype(jnp.float32).reshape(block_len, head_count, head_width)
    )
    memory_out = (
        (normed_heads * out_gate).astype(jnp.bfloat16).reshape(block_len, head_count * head_width)
    )
    padded = padded_2(pool_input, (("sp", 0),), HALO).astype(jnp.float32)
    feature_count = pool_input.shape[1]
    positions = lax.axis_index("sp") * block_len + jnp.arange(block_len, dtype=jnp.int32)
    channels = lax.axis_index("tp") * feature_count + jnp.arange(feature_count, dtype=jnp.int32)
    pool_out = pool_window(
        padded, positions, channels, block_len * lax.axis_size("sp"), model_width // 4
    )
    own_rows = block_len // lax.axis_size("tp")
    result = lax.dot_general(
        memory_out, mem_weight_all, (((1,), (1,)), ((), ())), preferred_element_type=jnp.float32
    )
    mixed = lax.psum_scatter(
        (
            result
            + lax.dot_general(
                pool_out,
                pool_weight_all,
                (((1,), (1,)), ((), ())),
                preferred_element_type=jnp.float32,
            )
        ).astype(jnp.bfloat16),
        "tp",
        scatter_dimension=0,
        tiled=True,
    )
    return mixed.reshape(1, own_rows, model_width)


LOG2E = math.log2(math.e)


def scan_lanes(x, combine_, fill, reverse):
    length = x.shape[1]
    lane = lax.broadcasted_iota(jnp.int32, x.shape, 1)
    d = 1
    while d < length:
        if reverse:
            moved = jnp.where(lane < length - d, pltpu.roll(x, length - d, 1), fill)
        else:
            moved = jnp.where(lane >= d, pltpu.roll(x, d, 1), fill)
        x = combine_(x, moved)
        d *= 2
    return x


def transposed_dot(a, b):
    return lax.dot_general(a, b, (((1,), (1,)), ((), ())), preferred_element_type=jnp.float32)


def layer_kernel(
    n_sp,
    token_ref, gain_ref, qw, kw, vw, ow, gate_ref, bias_ref, decay_ref, mem_ref, nrm_ref,
    hgain_ref, pw, mw, fw,
    out_ref,
    o_ref, x_all, normed, w_all, stage, transit, gmat, dec, init, nrm, proj_a, ungated, pool_buf, act,
    within, dens, values_t, pre_rows, flat, cols, run_rows, aux_out, aux_in, state_out, state_in, halo_tok,
    give, take, total, s1, l1, s2, l2,
    loc_w, loc_s, out_sem, x_ss, x_rs, p_ss, p_rs, h_ss, h_rs, y_ss, y_rs,
    token_p_ss, token_p_rs, tx_ss, tx_rs, tw_ss, tw_rs, d_ss, d_rs, i_ss, i_rs, m_ss, m_rs, e_ss, e_rs,
    sw_ss, sw_rs, r1_ss, r1_rs, r2_ss, r2_rs,
):
    block, width = token_ref.shape
    rows = qw.shape[0]
    hw = hgain_ref.shape[1]
    feat = pw.shape[1] // 4
    half = block // 2
    span = 2 * block
    pieces_t = token_p_rs.shape[0]
    part = half // pieces_t
    z, fs, c = lax.axis_index("sp"), lax.axis_index("fs"), lax.axis_index("tp")
    y, x = fs // 2, lax.rem(fs, 2)
    h, p = z // 2, lax.rem(z, 2)
    zn = z + 1 - 2 * p
    zf = lax.rem(z + 2, n_sp)
    zfn = zf + 1 - 2 * p
    xn, yn = 2 * y + 1 - x, 2 * (1 - y) + x
    other = 1 - c
    low = h == 0
    quarter = 2 * p + x
    to_x, to_y, to_p, to_h, to_c = {"fs": xn}, {"fs": yn}, {"sp": zn}, {"sp": zf}, {"tp": other}

    def remote(src, dst, ss, rs, device):
        return pltpu.make_async_remote_copy(
            src_ref=src, dst_ref=dst, send_sem=ss, recv_sem=rs,
            device_id=device, device_id_type=MESH,
        )

    def at(start, size):
        return pl.ds(pl.multiple_of(start, size), size)

    inner, outer = p != h, p == h
    to_m = {"sp": n_sp - 1 - z}
    barrier = pltpu.get_barrier_semaphore()
    for device in (to_x, to_y, to_p, to_h, to_c):
        pl.semaphore_signal(barrier, inc=1, device_id=device, device_id_type=MESH)

    @pl.when(inner)
    def _():
        pl.semaphore_signal(barrier, inc=1, device_id=to_m, device_id_type=MESH)

    groups = (((qw, hw), (kw, hw), (vw, hw)), ((ow, hw), (pw, feat)), ((mw, hw), (fw, feat)))
    quarters = (quarter, 2 * p + 1 - x, 2 * (1 - p) + 1 - x, 2 * (1 - p) + x)

    def row_block(zs, ys, xs):
        return at((zs * 4 + ys * 2 + xs) * rows, rows)

    def local_weights(g):
        copies = []
        for slot in (1, 2, 3, 0):
            start = 0
            for i, (ref, size) in enumerate(groups[g]):
                columns = pl.ds(start, size)
                if slot:
                    dst = stage.at[g, slot - 1, :, columns]
                else:
                    dst = w_all.at[g, row_block(z, y, x), columns]
                copies.append(
                    pltpu.make_async_copy(
                        ref.at[:, at(quarters[slot] * size, size)], dst, loc_w.at[g, slot]
                    )
                )
                start += size
        return copies

    locals_ = [local_weights(g) for g in range(3)]
    own_tokens = pltpu.make_async_copy(
        token_ref, x_all.at[at((2 * x + p) * block, block)], loc_s.at[0]
    )
    own_decay = pltpu.make_async_copy(decay_ref, dec.at[x, p], loc_s.at[1])
    own_init = pltpu.make_async_copy(mem_ref.at[h, quarter], init.at[x], loc_s.at[2])
    own_nrm = pltpu.make_async_copy(nrm_ref, nrm.at[x], loc_s.at[3])
    for copy in locals_[0]:
        copy.start()
    own_tokens.start()
    for copy in locals_[1] + locals_[2]:
        copy.start()
    for copy in (own_decay, own_init, own_nrm):
        copy.start()

    def x_copy(g, s, incoming=False):
        if s == 0:
            dst = w_all.at[g, row_block(z, y, 1 - x if incoming else x)]
        else:
            dst = transit.at[g]
        return remote(dst if incoming else stage.at[g, s], dst, x_ss, x_rs.at[g, s], to_x)

    def p_copy(g, s, incoming=False):
        dst = w_all.at[g, row_block(zn if incoming else z, y, 1 - x if s else x)]
        src = dst if incoming else (transit.at[g] if s else stage.at[g, 2])
        return remote(src, dst, p_ss, p_rs.at[g, s], to_p)

    def h_plane(g, e, s, incoming=False):
        source = 2 * (1 - h if incoming else h) + e
        ref = w_all.at[g, row_block(source, y, 1 - x if s else x)]
        return remote(ref, ref, h_ss, h_rs.at[g, e, s], to_h)

    def h_copy(g, k, s, incoming=False):
        return h_plane(g, 1 - p if k else p, s, incoming)

    def y_copy(g, plane, s, incoming=False):
        ref = w_all.at[g, row_block(plane, 1 - y if incoming else y, 1 - x if s else x)]
        return remote(ref, ref, y_ss, y_rs.at[2 + plane if g == 2 else g], to_y)

    def go(copy):
        copy.start()

    def ready(g, slots):
        for slot in slots:
            ref = stage.at[g, slot - 1] if slot else w_all.at[g, row_block(z, y, x)]
            pltpu.make_async_copy(ref, ref, loc_w.at[g, slot]).wait()

    def go_if(here, copy):
        @pl.when(here)
        def _():
            copy.start()

    def begin_x(g):
        ready(g, (1, 2))
        go(x_copy(g, 1))
        go(x_copy(g, 0))

    def begin_p(g):
        ready(g, (3,))
        go(p_copy(g, 0))

    def begin_y(g):
        ready(g, (0,))
        go(y_copy(g, z, 0))

    def after_x(g):
        x_copy(g, 1, True).wait_recv()
        go(p_copy(g, 1))
        x_copy(g, 0, True).wait_recv()
        go(y_copy(g, z, 1))

    def after_p_y(g):
        for s in range(2):
            p_copy(g, s, True).wait_recv()
            go(y_copy(g, zn, s))

    def all_far_if(here, g):
        @pl.when(here)
        def _():
            for e in range(2):
                for s in range(2):
                    h_plane(g, e, s).start()

    def far_if(here, g):
        @pl.when(here)
        def _():
            for s in range(2):
                h_copy(g, 0, s).start()

    def after_p(g):
        for s in range(2):
            p_copy(g, s, True).wait_recv()
            go(h_copy(g, 1, s))
            go(y_copy(g, zn, s))

    def after_h(g, k):
        for s in range(2):
            h_copy(g, k, s, True).wait_recv()
            go(y_copy(g, (zf, zfn)[k], s))

    def after_plane(g, e):
        for s in range(2):
            h_plane(g, e, s, True).wait_recv()
            go(y_copy(g, 2 * (1 - h) + e, s))

    def arrived_y(ref, sem):
        remote(ref, ref, y_ss, sem, to_y).wait_recv()

    def after_y(g, plane):
        start = pl.multiple_of((plane * 4 + 2 * (1 - y)) * rows, rows)
        arrived_y(w_all.at[g, pl.ds(start, 2 * rows)], y_rs.at[2 + plane])

    def all_y(g):
        arrived_y(w_all.at[g, pl.ds(0, 8 * rows)], y_rs.at[g])

    def token_rows(j, b, side, i):
        return at((2 * j + b) * block + side * half + i * part, part)

    def token_p(i, incoming=False):
        b = 1 - p if incoming else p
        dst = x_all.at[token_rows(x, b, c, i)]
        src = dst if incoming else token_ref.at[at(c * half + i * part, part)]
        return remote(src, dst, token_p_ss, token_p_rs.at[i], to_p)

    def token_x(kind, i, incoming=False):
        b = 1 - p if kind else p
        dst = x_all.at[token_rows(1 - x if incoming else x, b, c, i)]
        src = dst if incoming or kind else token_ref.at[at(c * half + i * part, part)]
        return remote(src, dst, tx_ss, tx_rs.at[kind, i], to_x)

    places = ((x, 1 - p), (1 - x, p), (1 - x, 1 - p))

    def token_swap(which, i, incoming=False):
        j, b = places[which]
        ref = x_all.at[token_rows(j, b, other if incoming else c, i)]
        return remote(ref, ref, tw_ss, tw_rs.at[which], to_c)

    edge_rows = halo_tok.shape[1]

    def edge_copy(which):
        return remote(
            token_ref.at[at((1 - h) * (block - edge_rows), edge_rows)], halo_tok.at[x],
            e_ss.at[which], e_rs.at[0], (to_h, to_m)[which],
        )

    def edges(action):
        @pl.when(inner)
        def _():
            for which in range(2):
                action(edge_copy(which))

    def edge_x(incoming=False):
        ref = halo_tok.at[1 - x if incoming else x]
        return remote(ref, ref, e_ss.at[2], e_rs.at[1], to_x)

    def normalise_edges():
        wide = halo_tok[...].reshape(2 * edge_rows, width).astype(jnp.float32)
        normed[4 * block :, :] = (
            wide
            * lax.rsqrt(jnp.mean(wide * wide, axis=-1, keepdims=True) + norm_eps)
            * gain_ref[...]
        ).astype(jnp.bfloat16)

    def decay_p(incoming=False):
        dst = dec.at[x, 1 - p if incoming else p]
        return remote(dst if incoming else decay_ref, dst, d_ss.at[0], d_rs.at[0], to_p)

    def decay_x(kind, incoming=False):
        dst = dec.at[1 - x if incoming else x, 1 - p if kind else p]
        src = dst if incoming or kind else decay_ref
        return remote(src, dst, d_ss.at[1 + kind], d_rs.at[1 + kind], to_x)

    def init_x(which, incoming=False):
        dst = (init, nrm)[which].at[1 - x if incoming else x]
        src = (mem_ref.at[h, 2 * p + 1 - x], nrm_ref)[which]
        return remote(dst if incoming else src, dst, i_ss.at[which], i_rs.at[which], to_x)

    def normalise(j, b):
        step = 64

        def body(i, carry):
            here = at((2 * j + b) * block + i * step, step)
            wide = x_all[here, :].astype(jnp.float32)
            normed[here, :] = (
                wide
                * lax.rsqrt(jnp.mean(wide * wide, axis=-1, keepdims=True) + norm_eps)
                * gain_ref[...]
            ).astype(jnp.bfloat16)
            return carry

        lax.fori_loop(0, block // step, body, 0)
        here = at((2 * j + b) * block, block)
        pre_rows[2 * j + b] = transposed_dot(normed[here, :], gmat[...]).T[:8]

    def scoped(name, function, *args):
        with jax.named_scope(name):
            return function(*args)

    def token_arrivals_p(these):
        for i in these:
            token_p(i, True).wait_recv()
            go(token_swap(0, i))
            go(token_x(1, i))

    def token_arrivals_x(kind, these):
        for i in these:
            token_x(kind, i, True).wait_recv()
            go(token_swap(1 + kind, i))

    def swapped(which):
        j, b = places[which]
        ref = x_all.at[at((2 * j + b) * block + other * half, half)]
        remote(ref, ref, tw_ss, tw_rs.at[which], to_c).wait_recv()
        normalise(j, b)

    def pick_gates():
        gmat[...] = jnp.zeros_like(gmat)
        pick = lax.broadcasted_iota(jnp.int32, (4, width), 0) == quarter
        row16 = lax.broadcasted_iota(jnp.int32, (16, width), 0)
        gates16 = jnp.zeros((16, width), jnp.float32)
        for i in range(4):
            row = jnp.sum(
                jnp.where(pick, gate_ref[i].astype(jnp.float32), 0.0), axis=0, keepdims=True
            )
            gates16 = jnp.where((row16 == i) | (row16 == i + 4), row, gates16)
        gmat[0:16, :] = gates16.astype(jnp.bfloat16)

    scoped("barrier", pl.semaphore_wait, barrier, 5 + inner.astype(jnp.int32))
    begin_x(0)
    begin_p(0)
    begin_y(0)
    go(h_copy(0, 0, 0))
    edges(lambda copy: copy.start())
    own_decay.wait()
    go(decay_p())
    go(decay_x(0))
    go(token_p(0))
    begin_x(1)
    for i in range(pieces_t):
        go(token_x(0, i))
    begin_y(1)
    scoped("pick", pick_gates)
    scoped("tok_own", own_tokens.wait)
    scoped("norm_own", normalise, x, p)
    scoped("after_x_0", after_x, 0)
    go(h_copy(0, 0, 1))
    early = 2
    for i in range(1, early):
        go_if(outer, token_p(i))
    remote(halo_tok.at[x], halo_tok.at[x], e_ss.at[0], e_rs.at[0], to_h).wait_recv()
    go(edge_x())
    scoped("after_p_0", after_p, 0)
    for i in range(1, early):
        go_if(inner, token_p(i))
    for i in range(early, pieces_t):
        go(token_p(i))
    begin_p(1)
    scoped("after_x_1", after_x, 1)
    far_if(outer, 1)
    scoped("after_h_0", after_h, 0, 0)
    scoped("tok_p", token_arrivals_p, (0,))
    scoped("tok_x0", token_arrivals_x, 0, (0, 1))
    scoped("after_h_0", after_h, 0, 1)
    scoped("tok_p", token_arrivals_p, (1,))
    scoped("tok_x0", token_arrivals_x, 0, (2, 3))
    scoped("norm_x", swapped, 1)
    far_if(inner, 1)
    edge_x(True).wait_recv()
    normalise_edges()
    scoped("tok_p", token_arrivals_p, (2, 3))
    decay_p(True).wait_recv()
    go(decay_x(1))
    go(init_x(0))
    go(init_x(1))
    begin_x(2)
    begin_y(2)

    scoped("norm_p", swapped, 0)

    @pl.when(outer)
    def _():
        scoped("after_p_1", after_p, 1)

    scoped("after_y_0", all_y, 0)

    def project(g, place, store):
        i = 2 * place[0] + place[1]
        store(i, jnp.dot(
            normed[at(i * block, block), :], w_all[g], preferred_element_type=jnp.float32
        ).astype(jnp.bfloat16))

    def store_a(i, value):
        proj_a[at(i * block, block), :] = value

    for place in ((x, p), places[0], places[1]):
        scoped("project_0", project, 0, place, store_a)
    scoped("tok_x1", token_arrivals_x, 1, (0, 1))

    @pl.when(inner)
    def _():
        scoped("after_p_1i", after_p, 1)

    begin_p(2)

    scoped("tok_x1", token_arrivals_x, 1, (2, 3))
    scoped("after_h_1", after_h, 1, 0)
    scoped("norm_px", swapped, 2)
    decay_x(0, True).wait_recv()
    decay_x(1, True).wait_recv()

    scoped("after_x_2", after_x, 2)

    with jax.named_scope("gates"):
        tall = []
        for j in range(2):
            tall.append(jnp.concatenate([pre_rows[2 * j], pre_rows[2 * j + 1]], axis=1))
        row8 = lax.broadcasted_iota(jnp.int32, (8, span), 0)
        gates = jnp.where(row8 < 4, tall[0], tall[1])
        extra = jnp.zeros((8, span), jnp.float32)
        for i in range(4):
            gates = gates + jnp.where((row8 == i) | (row8 == i + 4), bias_ref[i, quarter], 0.0)
        for j in range(2):
            for direction in range(2):
                value = jnp.concatenate(
                    [dec[j, b, direction, pl.ds(quarter, 1), :] for b in range(2)], axis=1
                )
                extra = jnp.where(row8 == 4 * j + 1 + 2 * direction, value, extra)
        forget = jnp.minimum(gates, 0.0) - jnp.log1p(jnp.exp(-jnp.abs(gates))) + extra
        sum_f = pltpu.roll(scan_lanes(forget, jnp.add, 0.0, False), 7, 0)
        sum_b = pltpu.roll(scan_lanes(forget, jnp.add, 0.0, True), 7, 0)
        level_f = gates - sum_f
        level_b = gates - sum_b
        run_f = scan_lanes(level_f, jnp.maximum, -1e30, False)
        run_b = scan_lanes(level_b, jnp.maximum, -1e30, True)
        top_f = jnp.maximum(run_f[:, span - 1 : span], 0.0)
        top_b = jnp.maximum(run_b[:, 0:1], 0.0)
        end_f = sum_f[:, span - 1 : span] + top_f
        end_b = sum_b[:, 0:1] + top_b
        aux_out[2] = jnp.broadcast_to(jnp.where(low, end_f, end_b), (8, hw))

    def message(which, incoming=False):
        src = (aux_out, state_out)[which]
        dst = (aux_in, state_in)[which]
        return remote(dst if incoming else src, dst, m_ss.at[which], m_rs.at[which], to_h)

    scoped("project_0", project, 0, places[2], store_a)

    with jax.named_scope("state"):
        scale_bits = -0.5 * math.log2(hw)
        lf2 = level_f * LOG2E + scale_bits
        lb2 = level_b * LOG2E + scale_bits
        own_init.wait()
        own_nrm.wait()
        init_x(0, True).wait_recv()
        init_x(1, True).wait_recv()
        leave_f = jnp.exp2(lf2 - top_f * LOG2E)
        leave_b = jnp.exp2(lb2 - top_b * LOG2E)
        keep_f = jnp.exp(-top_f)
        keep_b = jnp.exp(-top_b)
        for j in range(2):
            here = slice(j * span, (j + 1) * span)
            own = jnp.where(low, leave_f[4 * j : 4 * j + 1], leave_b[4 * j + 2 : 4 * j + 3])
            kept = jnp.where(low, keep_f[4 * j : 4 * j + 1], keep_b[4 * j + 2 : 4 * j + 3])
            values = proj_a[here, 2 * hw : 3 * hw].astype(jnp.float32).T
            values_t[j] = values.astype(jnp.bfloat16)
            values = values * own
            lhs = jnp.concatenate(
                [values, jnp.broadcast_to(own, (8, span))], axis=0
            ).astype(jnp.bfloat16)
            grown = jnp.dot(lhs, proj_a[here, hw : 2 * hw], preferred_element_type=jnp.float32)
            state_out[j] = (kept * init[j] + grown[:hw]).astype(jnp.bfloat16)
            aux_out[j] = kept * nrm[j, h, pl.ds(quarter, 1), :] + grown[hw:]
    go(message(0))
    go(message(1))

    with jax.named_scope("levels"):
        flat[16:, :] = jnp.zeros_like(flat[16:, :])
        flat[0:8, :] = lf2
        flat[8:16, :] = lb2
        cols[...] = flat[...].T
        run_rows[0] = run_f * LOG2E
        run_rows[1] = run_b * LOG2E

    def attend(j):
        here = slice(j * span, (j + 1) * span)
        f, b = 4 * j, 4 * j + 2
        levels = [jnp.broadcast_to(cols[:, k : k + 1], (span, half)) for k in (f, 8 + b)]
        for i in range(4):
            r0 = i * half
            mine = slice(j * span + r0, j * span + r0 + half)
            score = transposed_dot(proj_a[here, hw : 2 * hw], proj_a[mine, 0:hw])
            for which, first, last in ((0, 0, r0 + half), (1, r0, span)):
                row = (f, b)[which]
                peak = run_rows[which, row : row + 1, r0 : r0 + half]
                weight = jnp.exp2(levels[which][first:last] - peak) * score[first:last]
                s = first + lax.broadcasted_iota(jnp.int32, weight.shape, 0)
                t = r0 + lax.broadcasted_iota(jnp.int32, weight.shape, 1)
                weight = jnp.where(s >= t if which else s <= t, weight, 0.0)
                within[which, j, :, r0 : r0 + half] = jnp.dot(
                    values_t[j, :, first:last], weight.astype(jnp.bfloat16),
                    preferred_element_type=jnp.float32,
                )
                dens[which, j : j + 1, r0 : r0 + half] = jnp.sum(weight, axis=0, keepdims=True)

    scoped("attend_0", attend, 0)
    scoped("attend_1", attend, 1)
    scoped("after_h_1", after_h, 1, 1)
    scoped("after_p_2y", after_p_y, 2)
    all_far_if(inner, 2)
    scoped("state_in", message(1, True).wait_recv)
    scoped("aux_in", message(0, True).wait_recv)
    all_far_if(outer, 2)

    with jax.named_scope("enter"):
        arrived = aux_in[2, :, 0:1]
        enter_f = jnp.where(low, 0.0, arrived)
        enter_b = jnp.where(low, arrived, 0.0)
        factors = []
        for run, enter, summed in ((run_f, enter_f, sum_f), (run_b, enter_b, sum_b)):
            peak = jnp.maximum(run, enter)
            factors.append(
                (jnp.exp(run - peak), jnp.exp(enter - peak), jnp.exp(-(summed + peak)))
            )

    def finish(j):
        own_n = jnp.broadcast_to(nrm[j, h, pl.ds(quarter, 1), :], (8, hw))
        there = state_in[j].astype(jnp.float32)
        carry_in = jnp.concatenate(
            [
                jnp.where(low, init[j], there),
                jnp.where(low, there, init[j]),
                jnp.where(low, own_n, aux_in[j]),
                jnp.where(low, aux_in[j], own_n),
            ],
            axis=0,
        )
        coarse = carry_in.astype(jnp.bfloat16)
        fine = (carry_in - coarse.astype(jnp.float32)).astype(jnp.bfloat16)
        q = proj_a[j * span : (j + 1) * span, 0:hw]
        carry = transposed_dot(
            jnp.concatenate([coarse, fine], axis=1), jnp.concatenate([q, q], axis=1)
        )
        both = []
        for which in range(2):
            row = 4 * j + 2 * which
            grow, decay, floor = (part[row : row + 1] for part in factors[which])
            den0 = carry[2 * hw + 8 * which : 2 * hw + 8 * which + 1]
            den = grow * dens[which, j : j + 1, :] + decay * den0
            share = 1.0 / jnp.maximum(jnp.abs(den), floor)
            both.append(
                (grow * share) * within[which, j]
                + (decay * share) * carry[which * hw : (which + 1) * hw]
            )
        summed = both[0] + both[1]
        summed = summed * lax.rsqrt(jnp.mean(summed * summed, axis=0, keepdims=True) + norm_eps)
        ungated[j * span : (j + 1) * span, :] = summed.T * hgain_ref[pl.ds(quarter, 1), :]

    scoped("finish", finish, 0)
    scoped("finish", finish, 1)

    scoped("after_y_1", all_y, 1)

    def project_b():
        for i in range(4):
            last_rows = 2 * edge_rows if i == 3 else 0
            value = jnp.dot(
                normed[i * block : (i + 1) * block + last_rows, :], w_all[1],
                preferred_element_type=jnp.float32,
            ).astype(jnp.bfloat16)
            gate = jax.nn.sigmoid(value[:block, :hw].astype(jnp.float32))
            out = (ungated[i * block : (i + 1) * block, :] * gate).astype(jnp.bfloat16)
            for e in range(2):
                act[e * span + i * half : e * span + (i + 1) * half, 0:hw] = out[
                    e * half : (e + 1) * half
                ]
            start = 8 + (i % 2) * block
            pool_buf[i // 2, start : start + block, :] = value[:block, hw:].astype(jnp.float32)
        beyond = value[block:, hw:].astype(jnp.float32)
        zero = jnp.zeros((8, feat), jnp.float32)
        for j in range(2):
            mine = beyond[j * edge_rows : (j + 1) * edge_rows]
            pool_buf[j, 0:8, :] = jnp.where(low, zero, mine[edge_rows - 8 :])
            pool_buf[j, span + 8 : span + 16, :] = jnp.where(low, mine[:8], zero)

    scoped("project_1", project_b)
    with jax.named_scope("pooling"):
        group = (c * 4 + quarter) * feat * 4 // width
        for k in range(4):

            @pl.when(group == k)
            def _(k=k):
                reach = 2 ** k
                t = h * span + lax.broadcasted_iota(jnp.int32, (span, 1), 0)
                counted = jnp.minimum(t + reach - 1, n_sp * block - 1) - jnp.maximum(t - reach, 0) + 1
                counted = counted.astype(jnp.float32)
                length = span + 16
                for j in range(2):
                    window = pool_buf[j]
                    for e in range(k + 1):
                        window = window + pltpu.roll(window, length - 2 ** e, 0)
                    if reach < 8:
                        window = pltpu.roll(window, length - (8 - reach), 0)
                    value = window[:span] / counted - pool_buf[j, 8 : 8 + span, :]
                    value = value.astype(jnp.bfloat16)
                    for i in range(4):
                        place = (i % 2) * span + (2 * j + i // 2) * half
                        act[place : place + half, hw:] = value[i * half : (i + 1) * half]

    count = give.shape[0]
    tile = width // count
    each = count // 4
    planes = (2 * h, 2 * h + 1, 2 * (1 - h), 2 * (1 - h) + 1)

    def columns_of(n):
        return at(planes[n // each] * (width // 4) + (n % each) * tile, tile)

    def mixed(n):
        return n in (3, 5, 7)

    def swap(n):
        return remote(give.at[n], take.at[n], sw_ss, sw_rs.at[n], to_c)

    def first_stage(n, slot, incoming=False):
        dst = l1.at[n, slot]
        return remote(
            dst if incoming else s1.at[n, slot], dst, r1_ss, r1_rs.at[n, slot],
            to_p if mixed(n) else to_x,
        )

    def second_stage(n, incoming=False):
        return remote(
            l2.at[n] if incoming else s2.at[n], l2.at[n], r2_ss, r2_rs.at[n],
            to_x if mixed(n) else to_p,
        )

    def product(side, n):
        return transposed_dot(act[at(side * span, span), :], w_all[2, columns_of(n), :])

    home = 2 * x + p
    both = 2 * (1 - x) + 1 - p

    def first(n):
        part_sum = product(c, n)
        swap(n).wait_recv()
        total[n] = part_sum.reshape(total.shape[1:]) + take[n].astype(jnp.float32)
        near, middle = 2 * (1 - x) + p, 2 * x + 1 - p
        if mixed(n):
            near, middle = middle, near
        s1[n, 1] = total[n, both].astype(jnp.bfloat16)
        go(first_stage(n, 1))
        s1[n, 0] = total[n, near].astype(jnp.bfloat16)
        go(first_stage(n, 0))

    def second(n):
        middle = 2 * (1 - x) + p if mixed(n) else 2 * x + 1 - p
        first_stage(n, 1, True).wait_recv()
        s2[n] = (total[n, middle] + l1[n, 1].astype(jnp.float32)).astype(jnp.bfloat16)
        go(second_stage(n))

    def out_copy(n):
        return pltpu.make_async_copy(
            o_ref.at[:, columns_of(n)], out_ref.at[:, columns_of(n)], out_sem
        )

    def last(n):
        first_stage(n, 0, True).wait_recv()
        second_stage(n, True).wait_recv()
        o_ref[:, columns_of(n)] = (
            total[n, home] + l1[n, 0].astype(jnp.float32) + l2[n].astype(jnp.float32)
        ).astype(jnp.bfloat16)
        out_copy(n).start()

    for q in range(4):
        mine = range(q * each, (q + 1) * each)
        if q == 2:
            with jax.named_scope("second#q=1"):
                for n in range(each, 2 * each):
                    second(n)
        scoped("plane#q=%d" % q, after_y, 2, planes[q])
        with jax.named_scope("give#q=%d" % q):
            for n in mine:
                give[n] = product(other, n).astype(jnp.bfloat16).reshape(give.shape[1:])
                go(swap(n))
        with jax.named_scope("first#q=%d" % q):
            for n in mine:
                first(n)
        if q == 1:
            scoped("after_h_2", after_plane, 2, 0)
            with jax.named_scope("second#q=0"):
                for n in range(each):
                    second(n)
            scoped("after_h_2", after_plane, 2, 1)
        if q > 2:
            with jax.named_scope("second#q=%d" % (q - 1)):
                for n in mine:
                    second(n - each)
    with jax.named_scope("last#q=0"):
        for n in range(2 * each):
            last(n)
    with jax.named_scope("second#q=3"):
        for n in range(3 * each, count):
            second(n)
    with jax.named_scope("last#q=1"):
        for n in range(2 * each, count):
            last(n)

    with jax.named_scope("drain"):
        sends = (
            (w_all.at[:, 0 : 2 * rows], x_ss),
            (w_all.at[:, 0 : 2 * rows], p_ss),
            (w_all.at[:, 0 : 4 * rows], h_ss),
            (w_all.at[:, 0 : 8 * rows], y_ss),
            (x_all.at[0:half], token_p_ss),
            (x_all.at[0 : 2 * half], tx_ss),
            (x_all.at[0 : 3 * half], tw_ss),
            (give, sw_ss),
            (s1, r1_ss),
            (s2, r2_ss),
        )
        for ref, sem in sends:
            remote(ref, ref, sem, e_rs.at[0], to_x).wait_send()
        for copy in (
            decay_p(), decay_x(0), decay_x(1), init_x(0), init_x(1), message(0), message(1), edge_x()
        ):
            copy.wait_send()
        edges(lambda copy: copy.wait_send())
        pltpu.make_async_copy(o_ref, out_ref, out_sem).wait()


def by_group(
    tokens, norm_gain, query_weight, key_weight, value_weight, outgate_weight, gate_weight,
    gate_bias, decay_extra, init_memory, init_normalizer, head_gain, pool_weight, mem_out_weight,
    pool_out_weight,
):
    n_sp = lax.axis_size("sp")
    block, width = tokens.shape[1:]
    rows = query_weight.shape[0]
    hw = head_gain.shape[1]
    feat = pool_weight.shape[1] // 4
    columns = 3 * hw
    half, span, everything = block // 2, 2 * block, 4 * block
    count, pieces = 8, 4
    tile = width // count
    f32, bf16 = jnp.float32, jnp.bfloat16
    dma = pltpu.SemaphoreType.DMA
    vmem = pl.BlockSpec(memory_space=pltpu.VMEM)
    anywhere = pl.BlockSpec(memory_space=pl.ANY)
    smem = pl.BlockSpec(memory_space=pltpu.SMEM)
    mixed = pl.pallas_call(
        functools.partial(layer_kernel, n_sp),
        out_shape=jax.ShapeDtypeStruct((half, width), bf16),
        in_specs=[
            anywhere, vmem, anywhere, anywhere, anywhere, anywhere, vmem, smem, anywhere, anywhere,
            anywhere, vmem, anywhere, anywhere, anywhere,
        ],
        out_specs=anywhere,
        scratch_shapes=[
            pltpu.VMEM((half, width), bf16),
            pltpu.VMEM((everything, width), bf16),
            pltpu.VMEM((everything + 16, width), bf16),
            pltpu.VMEM((3, width, columns), bf16),
            pltpu.VMEM((3, 3, rows, columns), bf16),
            pltpu.VMEM((3, rows, columns), bf16),
            pltpu.VMEM((128, width), bf16),
            pltpu.VMEM((2, 2) + decay_extra.shape[1:], f32),
            pltpu.VMEM((2, hw, hw), f32),
            pltpu.VMEM((2,) + init_normalizer.shape[1:], f32),
            pltpu.VMEM((everything, columns), bf16),
            pltpu.VMEM((everything, hw), f32),
            pltpu.VMEM((2, span + 16, feat), f32),
            pltpu.VMEM((everything, columns), bf16),
            pltpu.VMEM((2, 2, hw, span), f32),
            pltpu.VMEM((2, 8, span), f32),
            pltpu.VMEM((2, hw, span), bf16),
            pltpu.VMEM((4, 8, block), f32),
            pltpu.VMEM((128, span), f32),
            pltpu.VMEM((span, 128), f32),
            pltpu.VMEM((2, 8, span), f32),
            pltpu.VMEM((3, 8, hw), f32),
            pltpu.VMEM((3, 8, hw), f32),
            pltpu.VMEM((2, hw, hw), bf16),
            pltpu.VMEM((2, hw, hw), bf16),
            pltpu.VMEM((2, 8, width), bf16),
            pltpu.VMEM((count, 4, half, tile), bf16),
            pltpu.VMEM((count, 4, half, tile), bf16),
            pltpu.VMEM((count, 4, half, tile), f32),
            pltpu.VMEM((count, 2, half, tile), bf16),
            pltpu.VMEM((count, 2, half, tile), bf16),
            pltpu.VMEM((count, half, tile), bf16),
            pltpu.VMEM((count, half, tile), bf16),
            dma((3, 4)),
            dma((4,)),
            dma(()),
            dma(()), dma((3, 2)),
            dma(()), dma((3, 2)),
            dma(()), dma((3, 2, 2)),
            dma(()), dma((6,)),
            dma(()), dma((pieces,)),
            dma(()), dma((2, pieces)),
            dma(()), dma((3,)),
            dma((3,)), dma((3,)),
            dma((2,)), dma((2,)),
            dma((2,)), dma((2,)),
            dma((3,)), dma((2,)),
            dma(()), dma((count,)),
            dma(()), dma((count, 2)),
            dma(()), dma((count,)),
        ],
        compiler_params=pltpu.CompilerParams(
            collective_id=0, has_side_effects=True, vmem_limit_bytes=60 * 2**20
        ),
        name="layer",
    )(
        tokens[0], norm_gain[None], query_weight, key_weight, value_weight, outgate_weight,
        gate_weight, gate_bias, decay_extra[0], init_memory[0], init_normalizer[0], head_gain,
        pool_weight, mem_out_weight, pool_out_weight,
    )
    return mixed[None]


def solution(mesh):
    placed = (
        P("fs", "sp", None),
        P(),
        P(("sp", "fs"), "tp"),
        P(("sp", "fs"), "tp"),
        P(("sp", "fs"), "tp"),
        P(("sp", "fs"), "tp"),
        P(None, "tp", None),
        P(None, "tp"),
        P("fs", None, "tp", "sp"),
        P("fs", None, "tp", None, None),
        P("fs", None, "tp", None),
        P("tp", None),
        P(("sp", "fs"), "tp"),
        P(("sp", "fs"), "tp"),
        P(("sp", "fs"), "tp"),
    )

    def body(*args):
        heads, width = args[11].shape
        features = args[12].shape[1]
        block, model_width = args[0].shape[1:]
        fits = (
            lax.axis_size("tp") == 2
            and lax.axis_size("fs") == 4
            and lax.axis_size("sp") == 4
            and heads == 4
            and width == 128
            and features == 8 * width
            and model_width == 2 * features
            and block == 2 * width
        )
        return (by_group if fits else per_device)(*args)

    return jax.shard_map(
        body,
        mesh=mesh,
        in_specs=placed,
        out_specs=P("fs", ("sp", "tp"), None),
        check_vma=False,
    )
```

```python
import functools
import math

import jax
import jax.numpy as jnp
from jax import lax
from jax.experimental import pallas as pl
from jax.experimental.pallas import tpu as pltpu
from jax.sharding import PartitionSpec as P

MESH = pl.DeviceIdType.MESH

HALO = 8


norm_eps = 1e-06
exact_mode = lax.Precision.HIGHEST


def carried_in(x, axis, combine, identity, reverse):
    length, position = (lax.axis_size(axis), lax.axis_index(axis))
    everything = jax.tree.map(lambda part: lax.all_gather(part, axis), x)
    start = jax.tree.map(
        lambda part, zero: jnp.broadcast_to(jnp.asarray(zero, part.dtype), part.shape), x, identity
    )

    def lap(k, before):
        at = length - 1 - k if reverse else k
        reached = at > position if reverse else at < position
        new = combine(before, jax.tree.map(lambda part: part[at], everything))
        return jax.tree.map(lambda a, b: jnp.where(reached, a, b), new, before)

    return lax.fori_loop(0, length, lap, start)


def padded_2(block, sides, width):
    for axis, dim in sides:
        count = lax.axis_size(axis)
        forward = [(i, i + 1) for i in range(count - 1)]
        backward = [(target, source) for source, target in forward]
        low = lax.ppermute(
            lax.slice_in_dim(block, block.shape[dim] - width, None, axis=dim), axis, forward
        )
        high = lax.ppermute(lax.slice_in_dim(block, 0, width, axis=dim), axis, backward)
        block = jnp.concatenate([low, block, high], axis=dim)
    return block


def block_output(
    query_rows, key_rows, value_rows, input_gate, log_forget, memory, normalizer, stabilizer
):
    block_len = query_rows.shape[1]
    key_scale = key_rows.shape[-1] ** (-0.5)
    lower_mask = jnp.tril(jnp.ones((block_len, block_len), dtype=bool))
    summed = jnp.cumsum(log_forget, axis=-1)
    log_decay = jnp.where(
        lower_mask, summed[:, :, None] - summed[:, None, :] + input_gate[:, None, :], -jnp.inf
    )
    log_carry = stabilizer[:, None] + summed
    running_max = jnp.maximum(log_carry, jnp.max(log_decay, axis=-1))
    scores = (
        jnp.einsum("btd,bsd->bts", query_rows, key_rows, preferred_element_type=jnp.float32)
        * key_scale
    )
    inner_weight = jnp.exp(log_decay - running_max[:, :, None]) * scores
    weight_rounded = inner_weight.astype(jnp.bfloat16)
    carry_weight = jnp.exp(log_carry - running_max)
    query_wide = query_rows.astype(jnp.float32)
    numerator = carry_weight[:, :, None] * jnp.einsum(
        "bed,btd->bte", memory, query_wide, precision=exact_mode
    )
    numerator = numerator + jnp.einsum(
        "bts,bse->bte", weight_rounded, value_rows, preferred_element_type=jnp.float32
    )
    denominator = carry_weight * jnp.einsum(
        "bd,btd->bt", normalizer, query_wide, precision=exact_mode
    )
    denominator = denominator + jnp.sum(inner_weight, axis=-1)
    return numerator / jnp.maximum(jnp.abs(denominator), jnp.exp(-running_max))[:, :, None]


def block_summary(key_rows, value_rows, input_gate, log_forget):
    key_wide = key_rows.astype(jnp.float32) * key_rows.shape[-1] ** (-0.5)
    summed = jnp.cumsum(log_forget, axis=-1)
    forget_total = summed[:, -1]
    log_weight = forget_total[:, None] - summed + input_gate
    running_max = jnp.max(log_weight, axis=-1)
    weights = jnp.exp(log_weight - running_max[:, None])
    memory = jnp.einsum(
        "bse,bsd->bed",
        weights[:, :, None] * value_rows.astype(jnp.float32),
        key_wide,
        precision=exact_mode,
    )
    normalizer = jnp.einsum("bs,bsd->bd", weights, key_wide, precision=exact_mode)
    return (memory, normalizer, running_max, forget_total)


def combine(earlier, latter):
    early_memory, early_norm, early_max, early_total = earlier
    late_memory, late_norm, late_max, late_total = latter
    joint_max = jnp.maximum(early_max + late_total, late_max)
    early_scale = jnp.exp(early_max + late_total - joint_max)
    late_scale = jnp.exp(late_max - joint_max)
    memory = early_scale[:, None, None] * early_memory + late_scale[:, None, None] * late_memory
    normalizer = early_scale[:, None] * early_norm + late_scale[:, None] * late_norm
    return (memory, normalizer, joint_max, early_total + late_total)


def span_sweep(
    query_rows, key_rows, value_rows, input_gate, log_forget, memory, normalizer, stabilizer, span
):
    block_count = query_rows.shape[1] // span

    def to_blocks(array):
        shaped = array.reshape((array.shape[0], block_count, span) + array.shape[2:])
        return jnp.moveaxis(shaped, 1, 0)

    def advance(carried, pieces):
        query_blk, key_blk, value_blk, gate_blk, forget_blk = pieces
        result = block_output(
            query_blk, key_blk, value_blk, gate_blk, forget_blk, carried[0], carried[1], carried[2]
        )
        return (combine(carried, block_summary(key_blk, value_blk, gate_blk, forget_blk)), result)

    initial = (memory, normalizer, stabilizer, jnp.zeros_like(stabilizer))
    ignored, outputs = lax.scan(
        advance,
        initial,
        tuple(
            (
                to_blocks(array)
                for array in (query_rows, key_rows, value_rows, input_gate, log_forget)
            )
        ),
    )
    return jnp.moveaxis(outputs, 0, 1).reshape(query_rows.shape[:2] + (value_rows.shape[2],))


def reverse_time(array):
    return jnp.flip(array, axis=1)


def to_heads(matrix, head_count):
    shaped = matrix.reshape(matrix.shape[0], head_count, matrix.shape[1] // head_count)
    return shaped.transpose(1, 0, 2)


def pool_window(padded, positions, channels, seq_len, group_size):
    row_count = positions.shape[0]
    group_index = channels // group_size
    reach_left = jnp.left_shift(jnp.ones_like(group_index), group_index)
    reach_right = reach_left - 1
    window_sum = jnp.zeros((row_count, channels.shape[0]), jnp.float32)
    for offset in range(-HALO, HALO):
        inside = ((offset >= -reach_left) & (offset <= reach_right)).astype(jnp.float32)
        window_sum = window_sum + inside * padded[HALO + offset : HALO + offset + row_count]
    first_pos = jnp.maximum(positions[:, None] - reach_left[None, :], 0)
    last_pos = jnp.minimum(positions[:, None] + reach_right[None, :], seq_len - 1)
    counted = (last_pos - first_pos + 1).astype(jnp.float32)
    centre = padded[HALO : HALO + row_count]
    return (window_sum / counted - centre).astype(jnp.bfloat16)


def per_device(
    tokens,
    norm_gain,
    query_weight,
    key_weight,
    value_weight,
    outgate_weight,
    gate_weight,
    gate_bias,
    decay_extra,
    init_memory,
    init_normalizer,
    head_gain,
    pool_weight,
    mem_out_weight,
    pool_out_weight,
):
    block_len = tokens.shape[1]
    model_width = tokens.shape[2]
    head_count, head_width = head_gain.shape
    span = math.gcd(block_len, 256)
    flattened = tokens[0].astype(jnp.float32)
    normed = (
        flattened
        * lax.rsqrt(jnp.mean(flattened * flattened, axis=-1, keepdims=True) + norm_eps)
        * norm_gain
    ).astype(jnp.bfloat16)
    zero_start = tuple(
        (
            jnp.zeros((block_len, weight.shape[1]), jnp.float32)
            for weight in (query_weight, key_weight, value_weight, outgate_weight, pool_weight)
        )
    )
    zero_start = zero_start + (
        jnp.zeros((model_width, mem_out_weight.shape[1]), jnp.bfloat16),
        jnp.zeros((model_width, pool_out_weight.shape[1]), jnp.bfloat16),
    )
    line_query, line_key, line_value, line_outgate, line_pool, line_mem_out, line_pool_out = (
        lax.all_gather(query_weight, "fs", axis=0, tiled=True),
        lax.all_gather(key_weight, "fs", axis=0, tiled=True),
        lax.all_gather(value_weight, "fs", axis=0, tiled=True),
        lax.all_gather(outgate_weight, "fs", axis=0, tiled=True),
        lax.all_gather(pool_weight, "fs", axis=0, tiled=True),
        lax.all_gather(mem_out_weight, "fs", axis=0, tiled=True),
        lax.all_gather(pool_out_weight, "fs", axis=0, tiled=True),
    )
    pieces = (
        lax.all_gather(line_query, "sp", axis=0, tiled=True),
        lax.all_gather(line_key, "sp", axis=0, tiled=True),
        lax.all_gather(line_value, "sp", axis=0, tiled=True),
        lax.all_gather(line_outgate, "sp", axis=0, tiled=True),
        lax.all_gather(line_pool, "sp", axis=0, tiled=True),
        lax.all_gather(line_mem_out, "sp", axis=0, tiled=True),
        lax.all_gather(line_pool_out, "sp", axis=0, tiled=True),
    )
    partial_sums = tuple(
        (
            jnp.dot(normed, weight_rows, preferred_element_type=jnp.float32)
            for weight_rows in pieces[:5]
        )
    )
    collected = tuple((weight_rows for weight_rows in pieces[5:]))
    folded = partial_sums + collected
    query_proj, key_proj, value_proj, outgate, pool_input = tuple(
        (running.astype(jnp.bfloat16) for running in folded[:5])
    )
    mem_weight_all = folded[5]
    pool_weight_all = folded[6]
    gate_pre = lax.dot_general(
        normed,
        gate_weight.reshape(4 * head_count, model_width),
        (((1,), (1,)), ((), ())),
        preferred_element_type=jnp.float32,
    ) + gate_bias.reshape(4 * head_count)
    gate_pre = gate_pre.reshape(block_len, 4, head_count).transpose(1, 2, 0)
    query_heads = to_heads(query_proj, head_count)
    key_heads = to_heads(key_proj, head_count)
    value_heads = to_heads(value_proj, head_count)
    forward_forget = jax.nn.log_sigmoid(gate_pre[1]) + decay_extra[0, 0]
    backward_forget = jax.nn.log_sigmoid(gate_pre[3]) + decay_extra[0, 1]
    zero_rows = jnp.zeros((head_count,), jnp.float32)
    identity = (
        jnp.zeros((head_count, head_width, head_width), jnp.float32),
        jnp.zeros((head_count, head_width), jnp.float32),
        jnp.full((head_count,), -1e30, jnp.float32),
        zero_rows,
    )
    front_memory, front_norm, front_max, front_total = block_summary(
        key_heads, value_heads, gate_pre[0], forward_forget
    )
    prefix = carried_in(
        (front_memory, front_norm, front_max, front_total), "sp", combine, identity, False
    )
    incoming = combine((init_memory[0, 0], init_normalizer[0, 0], zero_rows, zero_rows), prefix)
    forward_out = span_sweep(
        query_heads,
        key_heads,
        value_heads,
        gate_pre[0],
        forward_forget,
        incoming[0],
        incoming[1],
        incoming[2],
        span,
    )
    back_query = reverse_time(query_heads)
    back_key = reverse_time(key_heads)
    back_value = reverse_time(value_heads)
    back_gate = reverse_time(gate_pre[2])
    back_forget = reverse_time(backward_forget)
    rear_memory, rear_norm, rear_max, rear_total = block_summary(
        back_key, back_value, back_gate, back_forget
    )
    suffix = carried_in(
        (rear_memory, rear_norm, rear_max, rear_total), "sp", combine, identity, True
    )
    back_incoming = combine(
        (init_memory[0, 1], init_normalizer[0, 1], zero_rows, zero_rows), suffix
    )
    backward_out = reverse_time(
        span_sweep(
            back_query,
            back_key,
            back_value,
            back_gate,
            back_forget,
            back_incoming[0],
            back_incoming[1],
            back_incoming[2],
            span,
        )
    )
    summed_dirs = (forward_out + backward_out).transpose(1, 0, 2)
    normed_heads = (
        summed_dirs
        * lax.rsqrt(jnp.mean(summed_dirs * summed_dirs, axis=-1, keepdims=True) + norm_eps)
        * head_gain
    )
    out_gate = jax.nn.sigmoid(
        outgate.astype(jnp.float32).reshape(block_len, head_count, head_width)
    )
    memory_out = (
        (normed_heads * out_gate).astype(jnp.bfloat16).reshape(block_len, head_count * head_width)
    )
    padded = padded_2(pool_input, (("sp", 0),), HALO).astype(jnp.float32)
    feature_count = pool_input.shape[1]
    positions = lax.axis_index("sp") * block_len + jnp.arange(block_len, dtype=jnp.int32)
    channels = lax.axis_index("tp") * feature_count + jnp.arange(feature_count, dtype=jnp.int32)
    pool_out = pool_window(
        padded, positions, channels, block_len * lax.axis_size("sp"), model_width // 4
    )
    own_rows = block_len // lax.axis_size("tp")
    result = lax.dot_general(
        memory_out, mem_weight_all, (((1,), (1,)), ((), ())), preferred_element_type=jnp.float32
    )
    mixed = lax.psum_scatter(
        (
            result
            + lax.dot_general(
                pool_out,
                pool_weight_all,
                (((1,), (1,)), ((), ())),
                preferred_element_type=jnp.float32,
            )
        ).astype(jnp.bfloat16),
        "tp",
        scatter_dimension=0,
        tiled=True,
    )
    return mixed.reshape(1, own_rows, model_width)


LOG2E = math.log2(math.e)


def scan_lanes(x, combine_, fill, reverse):
    length = x.shape[1]
    lane = lax.broadcasted_iota(jnp.int32, x.shape, 1)
    d = 1
    while d < length:
        if reverse:
            moved = jnp.where(lane < length - d, pltpu.roll(x, length - d, 1), fill)
        else:
            moved = jnp.where(lane >= d, pltpu.roll(x, d, 1), fill)
        x = combine_(x, moved)
        d *= 2
    return x


def transposed_dot(a, b):
    return lax.dot_general(a, b, (((1,), (1,)), ((), ())), preferred_element_type=jnp.float32)


def layer_kernel(
    n_sp,
    token_ref, gain_hbm, qw, kw, vw, ow, gate_hbm, bias_hbm, decay_ref, mem_ref, nrm_ref,
    hgain_hbm, pw, mw, fw,
    o_ref,
    gain_ref, gate_ref, bias_ref, hgain_ref, x_all, normed, w_all, stage, transit, gmat, dec, init, nrm, proj_a, ungated, pool_buf, act,
    within, dens, values_t, pre_rows, flat, cols, run_rows, aux_out, aux_in, state_out, state_in, halo_tok,
    give, take, total, s1, l1, s2, l2,
    loc_w, loc_s, small_sem, x_ss, x_rs, p_ss, p_rs, h_ss, h_rs, y_ss, y_rs,
    token_p_ss, token_p_rs, tx_ss, tx_rs, tw_ss, tw_rs, d_ss, d_rs, i_ss, i_rs, m_ss, m_rs, e_ss, e_rs,
    sw_ss, sw_rs, r1_ss, r1_rs, r2_ss, r2_rs,
):
    block, width = token_ref.shape
    rows = qw.shape[0]
    hw = hgain_hbm.shape[1]
    feat = pw.shape[1] // 4
    half = block // 2
    span = 2 * block
    pieces_t = token_p_rs.shape[0]
    part = half // pieces_t
    z, fs, c = lax.axis_index("sp"), lax.axis_index("fs"), lax.axis_index("tp")
    y, x = fs // 2, lax.rem(fs, 2)
    h, p = z // 2, lax.rem(z, 2)
    zn = z + 1 - 2 * p
    zf = lax.rem(z + 2, n_sp)
    zfn = zf + 1 - 2 * p
    xn, yn = 2 * y + 1 - x, 2 * (1 - y) + x
    other = 1 - c
    low = h == 0
    quarter = 2 * p + x
    to_x, to_y, to_p, to_h, to_c = {"fs": xn}, {"fs": yn}, {"sp": zn}, {"sp": zf}, {"tp": other}

    def remote(src, dst, ss, rs, device):
        return pltpu.make_async_remote_copy(
            src_ref=src, dst_ref=dst, send_sem=ss, recv_sem=rs,
            device_id=device, device_id_type=MESH,
        )

    def at(start, size):
        return pl.ds(pl.multiple_of(start, size), size)

    inner, outer = p != h, p == h
    to_m = {"sp": n_sp - 1 - z}
    barrier = pltpu.get_barrier_semaphore()
    for device in (to_x, to_y, to_p, to_h, to_c):
        pl.semaphore_signal(barrier, inc=1, device_id=device, device_id_type=MESH)

    @pl.when(inner)
    def _():
        pl.semaphore_signal(barrier, inc=1, device_id=to_m, device_id_type=MESH)

    groups = (((qw, hw), (kw, hw), (vw, hw)), ((ow, hw), (pw, feat)), ((mw, hw), (fw, feat)))
    quarters = (quarter, 2 * p + 1 - x, 2 * (1 - p) + 1 - x, 2 * (1 - p) + x)

    def row_block(zs, ys, xs):
        return at((zs * 4 + ys * 2 + xs) * rows, rows)

    def local_weights(g):
        copies = []
        for slot in (1, 2, 3, 0):
            start = 0
            for i, (ref, size) in enumerate(groups[g]):
                columns = pl.ds(start, size)
                if slot:
                    dst = stage.at[g, slot - 1, :, columns]
                else:
                    dst = w_all.at[g, row_block(z, y, x), columns]
                copies.append(
                    pltpu.make_async_copy(
                        ref.at[:, at(quarters[slot] * size, size)], dst, loc_w.at[g, slot]
                    )
                )
                start += size
        return copies

    small = [
        pltpu.make_async_copy(src, dst, small_sem.at[i])
        for i, (src, dst) in enumerate(
            (
                (gain_hbm, gain_ref), (gate_hbm, gate_ref), (bias_hbm, bias_ref),
                (hgain_hbm, hgain_ref),
            )
        )
    ]
    locals_ = [local_weights(g) for g in range(3)]
    own_tokens = pltpu.make_async_copy(
        token_ref, x_all.at[at((2 * x + p) * block, block)], loc_s.at[0]
    )
    own_decay = pltpu.make_async_copy(decay_ref, dec.at[x, p], loc_s.at[1])
    own_init = pltpu.make_async_copy(mem_ref.at[h, quarter], init.at[x], loc_s.at[2])
    own_nrm = pltpu.make_async_copy(nrm_ref, nrm.at[x], loc_s.at[3])
    for copy in locals_[0]:
        copy.start()
    own_tokens.start()
    for copy in locals_[1] + locals_[2]:
        copy.start()
    for copy in small + [own_decay, own_init, own_nrm]:
        copy.start()

    def x_copy(g, s, incoming=False):
        if s == 0:
            dst = w_all.at[g, row_block(z, y, 1 - x if incoming else x)]
        else:
            dst = transit.at[g]
        return remote(dst if incoming else stage.at[g, s], dst, x_ss, x_rs.at[g, s], to_x)

    def p_copy(g, s, incoming=False):
        dst = w_all.at[g, row_block(zn if incoming else z, y, 1 - x if s else x)]
        src = dst if incoming else (transit.at[g] if s else stage.at[g, 2])
        return remote(src, dst, p_ss, p_rs.at[g, s], to_p)

    def h_plane(g, e, s, incoming=False):
        source = 2 * (1 - h if incoming else h) + e
        ref = w_all.at[g, row_block(source, y, 1 - x if s else x)]
        return remote(ref, ref, h_ss, h_rs.at[g, e, s], to_h)

    def h_copy(g, k, s, incoming=False):
        return h_plane(g, 1 - p if k else p, s, incoming)

    def y_copy(g, plane, s, incoming=False):
        ref = w_all.at[g, row_block(plane, 1 - y if incoming else y, 1 - x if s else x)]
        return remote(ref, ref, y_ss, y_rs.at[2 + plane if g == 2 else g], to_y)

    def go(copy):
        copy.start()

    def ready(g, slots):
        for slot in slots:
            ref = stage.at[g, slot - 1] if slot else w_all.at[g, row_block(z, y, x)]
            pltpu.make_async_copy(ref, ref, loc_w.at[g, slot]).wait()

    def go_if(here, copy):
        @pl.when(here)
        def _():
            copy.start()

    def begin_x(g):
        ready(g, (1, 2))
        go(x_copy(g, 1))
        go(x_copy(g, 0))

    def begin_p(g):
        ready(g, (3,))
        go(p_copy(g, 0))

    def begin_y(g):
        ready(g, (0,))
        go(y_copy(g, z, 0))

    def after_x(g):
        x_copy(g, 1, True).wait_recv()
        go(p_copy(g, 1))
        x_copy(g, 0, True).wait_recv()
        go(y_copy(g, z, 1))

    def after_p_y(g):
        for s in range(2):
            p_copy(g, s, True).wait_recv()
            go(y_copy(g, zn, s))

    def all_far_if(here, g):
        @pl.when(here)
        def _():
            for e in range(2):
                for s in range(2):
                    h_plane(g, e, s).start()

    def far_if(here, g):
        @pl.when(here)
        def _():
            for s in range(2):
                h_copy(g, 0, s).start()

    def after_p(g):
        for s in range(2):
            p_copy(g, s, True).wait_recv()
            go(h_copy(g, 1, s))
            go(y_copy(g, zn, s))

    def after_h(g, k):
        for s in range(2):
            h_copy(g, k, s, True).wait_recv()
            go(y_copy(g, (zf, zfn)[k], s))

    def after_plane(g, e):
        for s in range(2):
            h_plane(g, e, s, True).wait_recv()
            go(y_copy(g, 2 * (1 - h) + e, s))

    def arrived_y(ref, sem):
        remote(ref, ref, y_ss, sem, to_y).wait_recv()

    def after_y(g, plane):
        start = pl.multiple_of((plane * 4 + 2 * (1 - y)) * rows, rows)
        arrived_y(w_all.at[g, pl.ds(start, 2 * rows)], y_rs.at[2 + plane])

    def all_y(g):
        arrived_y(w_all.at[g, pl.ds(0, 8 * rows)], y_rs.at[g])

    def token_rows(j, b, side, i):
        return at((2 * j + b) * block + side * half + i * part, part)

    def token_p(i, incoming=False):
        b = 1 - p if incoming else p
        dst = x_all.at[token_rows(x, b, c, i)]
        src = dst if incoming else token_ref.at[at(c * half + i * part, part)]
        return remote(src, dst, token_p_ss, token_p_rs.at[i], to_p)

    def token_x(kind, i, incoming=False):
        b = 1 - p if kind else p
        dst = x_all.at[token_rows(1 - x if incoming else x, b, c, i)]
        src = dst if incoming or kind else token_ref.at[at(c * half + i * part, part)]
        return remote(src, dst, tx_ss, tx_rs.at[kind, i], to_x)

    places = ((x, 1 - p), (1 - x, p), (1 - x, 1 - p))

    def token_swap(which, i, incoming=False):
        j, b = places[which]
        ref = x_all.at[token_rows(j, b, other if incoming else c, i)]
        return remote(ref, ref, tw_ss, tw_rs.at[which], to_c)

    edge_rows = halo_tok.shape[1]

    def edge_copy(which):
        return remote(
            token_ref.at[at((1 - h) * (block - edge_rows), edge_rows)], halo_tok.at[x],
            e_ss.at[which], e_rs.at[0], (to_h, to_m)[which],
        )

    def edges(action):
        @pl.when(inner)
        def _():
            for which in range(2):
                action(edge_copy(which))

    def edge_x(incoming=False):
        ref = halo_tok.at[1 - x if incoming else x]
        return remote(ref, ref, e_ss.at[2], e_rs.at[1], to_x)

    def normalise_edges():
        wide = halo_tok[...].reshape(2 * edge_rows, width).astype(jnp.float32)
        normed[4 * block :, :] = (
            wide
            * lax.rsqrt(jnp.mean(wide * wide, axis=-1, keepdims=True) + norm_eps)
            * gain_ref[...]
        ).astype(jnp.bfloat16)

    def decay_p(incoming=False):
        dst = dec.at[x, 1 - p if incoming else p]
        return remote(dst if incoming else decay_ref, dst, d_ss.at[0], d_rs.at[0], to_p)

    def decay_x(kind, incoming=False):
        dst = dec.at[1 - x if incoming else x, 1 - p if kind else p]
        src = dst if incoming or kind else decay_ref
        return remote(src, dst, d_ss.at[1 + kind], d_rs.at[1 + kind], to_x)

    def init_x(which, incoming=False):
        dst = (init, nrm)[which].at[1 - x if incoming else x]
        src = (mem_ref.at[h, 2 * p + 1 - x], nrm_ref)[which]
        return remote(dst if incoming else src, dst, i_ss.at[which], i_rs.at[which], to_x)

    def normalise(j, b):
        step = 64

        def body(i, carry):
            here = at((2 * j + b) * block + i * step, step)
            wide = x_all[here, :].astype(jnp.float32)
            normed[here, :] = (
                wide
                * lax.rsqrt(jnp.mean(wide * wide, axis=-1, keepdims=True) + norm_eps)
                * gain_ref[...]
            ).astype(jnp.bfloat16)
            return carry

        lax.fori_loop(0, block // step, body, 0)
        here = at((2 * j + b) * block, block)
        pre_rows[2 * j + b] = transposed_dot(normed[here, :], gmat[...]).T[:8]

    def scoped(name, function, *args):
        with jax.named_scope(name):
            return function(*args)

    def token_arrivals_p(these):
        for i in these:
            token_p(i, True).wait_recv()
            go(token_swap(0, i))
            go(token_x(1, i))

    def token_arrivals_x(kind, these):
        for i in these:
            token_x(kind, i, True).wait_recv()
            go(token_swap(1 + kind, i))

    def swapped(which):
        j, b = places[which]
        ref = x_all.at[at((2 * j + b) * block + other * half, half)]
        remote(ref, ref, tw_ss, tw_rs.at[which], to_c).wait_recv()
        normalise(j, b)

    def pick_gates():
        gmat[...] = jnp.zeros_like(gmat)
        pick = lax.broadcasted_iota(jnp.int32, (4, width), 0) == quarter
        row16 = lax.broadcasted_iota(jnp.int32, (16, width), 0)
        gates16 = jnp.zeros((16, width), jnp.float32)
        for i in range(4):
            row = jnp.sum(
                jnp.where(pick, gate_ref[i].astype(jnp.float32), 0.0), axis=0, keepdims=True
            )
            gates16 = jnp.where((row16 == i) | (row16 == i + 4), row, gates16)
        gmat[0:16, :] = gates16.astype(jnp.bfloat16)

    scoped("barrier", pl.semaphore_wait, barrier, 5 + inner.astype(jnp.int32))
    begin_x(0)
    begin_p(0)
    begin_y(0)
    go(h_copy(0, 0, 0))
    edges(lambda copy: copy.start())
    own_decay.wait()
    go(decay_p())
    go(decay_x(0))
    go(token_p(0))
    begin_x(1)
    for i in range(pieces_t):
        go(token_x(0, i))
    begin_y(1)
    for copy in small:
        copy.wait()
    scoped("pick", pick_gates)
    scoped("tok_own", own_tokens.wait)
    scoped("norm_own", normalise, x, p)
    scoped("after_x_0", after_x, 0)
    go(h_copy(0, 0, 1))
    early = 2
    for i in range(1, early):
        go_if(outer, token_p(i))
    remote(halo_tok.at[x], halo_tok.at[x], e_ss.at[0], e_rs.at[0], to_h).wait_recv()
    go(edge_x())
    scoped("after_p_0", after_p, 0)
    for i in range(1, early):
        go_if(inner, token_p(i))
    for i in range(early, pieces_t):
        go(token_p(i))
    begin_p(1)
    scoped("after_x_1", after_x, 1)
    far_if(outer, 1)
    scoped("after_h_0", after_h, 0, 0)
    scoped("tok_p", token_arrivals_p, (0,))
    scoped("tok_x0", token_arrivals_x, 0, (0, 1))
    scoped("after_h_0", after_h, 0, 1)
    scoped("tok_p", token_arrivals_p, (1,))
    scoped("tok_x0", token_arrivals_x, 0, (2, 3))
    scoped("norm_x", swapped, 1)
    far_if(inner, 1)
    edge_x(True).wait_recv()
    normalise_edges()
    scoped("tok_p", token_arrivals_p, (2, 3))
    decay_p(True).wait_recv()
    go(decay_x(1))
    go(init_x(0))
    go(init_x(1))
    begin_x(2)
    begin_y(2)

    scoped("norm_p", swapped, 0)

    @pl.when(outer)
    def _():
        scoped("after_p_1", after_p, 1)

    scoped("after_y_0", all_y, 0)

    def project(g, place, store):
        i = 2 * place[0] + place[1]
        store(i, jnp.dot(
            normed[at(i * block, block), :], w_all[g], preferred_element_type=jnp.float32
        ).astype(jnp.bfloat16))

    def store_a(i, value):
        proj_a[at(i * block, block), :] = value

    for place in ((x, p), places[0], places[1]):
        scoped("project_0", project, 0, place, store_a)
    scoped("tok_x1", token_arrivals_x, 1, (0, 1))

    @pl.when(inner)
    def _():
        scoped("after_p_1i", after_p, 1)

    begin_p(2)

    scoped("tok_x1", token_arrivals_x, 1, (2, 3))

    @pl.when(inner)
    def _():
        scoped("after_h_1i", after_h, 1, 0)

    scoped("norm_px", swapped, 2)
    decay_x(0, True).wait_recv()
    decay_x(1, True).wait_recv()

    scoped("after_x_2", after_x, 2)

    with jax.named_scope("gates"):
        tall = []
        for j in range(2):
            tall.append(jnp.concatenate([pre_rows[2 * j], pre_rows[2 * j + 1]], axis=1))
        row8 = lax.broadcasted_iota(jnp.int32, (8, span), 0)
        gates = jnp.where(row8 < 4, tall[0], tall[1])
        extra = jnp.zeros((8, span), jnp.float32)
        for i in range(4):
            gates = gates + jnp.where((row8 == i) | (row8 == i + 4), bias_ref[i, quarter], 0.0)
        for j in range(2):
            for direction in range(2):
                value = jnp.concatenate(
                    [dec[j, b, direction, pl.ds(quarter, 1), :] for b in range(2)], axis=1
                )
                extra = jnp.where(row8 == 4 * j + 1 + 2 * direction, value, extra)
        forget = jnp.minimum(gates, 0.0) - jnp.log1p(jnp.exp(-jnp.abs(gates))) + extra
        sum_f = pltpu.roll(scan_lanes(forget, jnp.add, 0.0, False), 7, 0)
        sum_b = pltpu.roll(scan_lanes(forget, jnp.add, 0.0, True), 7, 0)
        level_f = gates - sum_f
        level_b = gates - sum_b
        run_f = scan_lanes(level_f, jnp.maximum, -1e30, False)
        run_b = scan_lanes(level_b, jnp.maximum, -1e30, True)
        top_f = jnp.maximum(run_f[:, span - 1 : span], 0.0)
        top_b = jnp.maximum(run_b[:, 0:1], 0.0)
        end_f = sum_f[:, span - 1 : span] + top_f
        end_b = sum_b[:, 0:1] + top_b
        aux_out[2] = jnp.broadcast_to(jnp.where(low, end_f, end_b), (8, hw))

    def message(which, incoming=False):
        src = (aux_out, state_out)[which]
        dst = (aux_in, state_in)[which]
        return remote(dst if incoming else src, dst, m_ss.at[which], m_rs.at[which], to_h)

    @pl.when(outer)
    def _():
        scoped("after_h_1", after_h, 1, 0)

    scoped("project_0", project, 0, places[2], store_a)

    with jax.named_scope("state"):
        scale_bits = -0.5 * math.log2(hw)
        lf2 = level_f * LOG2E + scale_bits
        lb2 = level_b * LOG2E + scale_bits
        own_init.wait()
        own_nrm.wait()
        init_x(0, True).wait_recv()
        init_x(1, True).wait_recv()
        leave_f = jnp.exp2(lf2 - top_f * LOG2E)
        leave_b = jnp.exp2(lb2 - top_b * LOG2E)
        keep_f = jnp.exp(-top_f)
        keep_b = jnp.exp(-top_b)
        for j in range(2):
            here = slice(j * span, (j + 1) * span)
            own = jnp.where(low, leave_f[4 * j : 4 * j + 1], leave_b[4 * j + 2 : 4 * j + 3])
            kept = jnp.where(low, keep_f[4 * j : 4 * j + 1], keep_b[4 * j + 2 : 4 * j + 3])
            values = proj_a[here, 2 * hw : 3 * hw].astype(jnp.float32).T
            values_t[j] = values.astype(jnp.bfloat16)
            values = values * own
            lhs = jnp.concatenate(
                [values, jnp.broadcast_to(own, (8, span))], axis=0
            ).astype(jnp.bfloat16)
            grown = jnp.dot(lhs, proj_a[here, hw : 2 * hw], preferred_element_type=jnp.float32)
            state_out[j] = (kept * init[j] + grown[:hw]).astype(jnp.bfloat16)
            aux_out[j] = kept * nrm[j, h, pl.ds(quarter, 1), :] + grown[hw:]
    go(message(0))
    go(message(1))

    with jax.named_scope("levels"):
        flat[16:, :] = jnp.zeros_like(flat[16:, :])
        flat[0:8, :] = lf2
        flat[8:16, :] = lb2
        cols[...] = flat[...].T
        run_rows[0] = run_f * LOG2E
        run_rows[1] = run_b * LOG2E

    def attend(j):
        here = slice(j * span, (j + 1) * span)
        f, b = 4 * j, 4 * j + 2
        levels = [jnp.broadcast_to(cols[:, k : k + 1], (span, half)) for k in (f, 8 + b)]
        for i in range(4):
            r0 = i * half
            mine = slice(j * span + r0, j * span + r0 + half)
            score = transposed_dot(proj_a[here, hw : 2 * hw], proj_a[mine, 0:hw])
            for which, first, last in ((0, 0, r0 + half), (1, r0, span)):
                row = (f, b)[which]
                peak = run_rows[which, row : row + 1, r0 : r0 + half]
                weight = jnp.exp2(levels[which][first:last] - peak) * score[first:last]
                s = first + lax.broadcasted_iota(jnp.int32, weight.shape, 0)
                t = r0 + lax.broadcasted_iota(jnp.int32, weight.shape, 1)
                weight = jnp.where(s >= t if which else s <= t, weight, 0.0)
                within[which, j, :, r0 : r0 + half] = jnp.dot(
                    values_t[j, :, first:last], weight.astype(jnp.bfloat16),
                    preferred_element_type=jnp.float32,
                )
                dens[which, j : j + 1, r0 : r0 + half] = jnp.sum(weight, axis=0, keepdims=True)

    scoped("attend_0", attend, 0)
    scoped("attend_1", attend, 1)
    scoped("after_h_1", after_h, 1, 1)
    scoped("after_p_2y", after_p_y, 2)
    all_far_if(inner, 2)
    scoped("state_in", message(1, True).wait_recv)
    scoped("aux_in", message(0, True).wait_recv)
    all_far_if(outer, 2)

    with jax.named_scope("enter"):
        arrived = aux_in[2, :, 0:1]
        enter_f = jnp.where(low, 0.0, arrived)
        enter_b = jnp.where(low, arrived, 0.0)
        factors = []
        for run, enter, summed in ((run_f, enter_f, sum_f), (run_b, enter_b, sum_b)):
            peak = jnp.maximum(run, enter)
            factors.append(
                (jnp.exp(run - peak), jnp.exp(enter - peak), jnp.exp(-(summed + peak)))
            )

    def finish(j):
        own_n = jnp.broadcast_to(nrm[j, h, pl.ds(quarter, 1), :], (8, hw))
        there = state_in[j].astype(jnp.float32)
        carry_in = jnp.concatenate(
            [
                jnp.where(low, init[j], there),
                jnp.where(low, there, init[j]),
                jnp.where(low, own_n, aux_in[j]),
                jnp.where(low, aux_in[j], own_n),
            ],
            axis=0,
        )
        coarse = carry_in.astype(jnp.bfloat16)
        fine = (carry_in - coarse.astype(jnp.float32)).astype(jnp.bfloat16)
        q = proj_a[j * span : (j + 1) * span, 0:hw]
        carry = transposed_dot(
            jnp.concatenate([coarse, fine], axis=1), jnp.concatenate([q, q], axis=1)
        )
        both = []
        for which in range(2):
            row = 4 * j + 2 * which
            grow, decay, floor = (part[row : row + 1] for part in factors[which])
            den0 = carry[2 * hw + 8 * which : 2 * hw + 8 * which + 1]
            den = grow * dens[which, j : j + 1, :] + decay * den0
            share = 1.0 / jnp.maximum(jnp.abs(den), floor)
            both.append(
                (grow * share) * within[which, j]
                + (decay * share) * carry[which * hw : (which + 1) * hw]
            )
        summed = both[0] + both[1]
        summed = summed * lax.rsqrt(jnp.mean(summed * summed, axis=0, keepdims=True) + norm_eps)
        ungated[j * span : (j + 1) * span, :] = summed.T * hgain_ref[pl.ds(quarter, 1), :]

    scoped("finish", finish, 0)
    scoped("finish", finish, 1)

    scoped("after_y_1", all_y, 1)

    def project_b():
        for i in range(4):
            last_rows = 2 * edge_rows if i == 3 else 0
            value = jnp.dot(
                normed[i * block : (i + 1) * block + last_rows, :], w_all[1],
                preferred_element_type=jnp.float32,
            ).astype(jnp.bfloat16)
            gate = jax.nn.sigmoid(value[:block, :hw].astype(jnp.float32))
            out = (ungated[i * block : (i + 1) * block, :] * gate).astype(jnp.bfloat16)
            for e in range(2):
                act[e * span + i * half : e * span + (i + 1) * half, 0:hw] = out[
                    e * half : (e + 1) * half
                ]
            start = 8 + (i % 2) * block
            pool_buf[i // 2, start : start + block, :] = value[:block, hw:].astype(jnp.float32)
        beyond = value[block:, hw:].astype(jnp.float32)
        zero = jnp.zeros((8, feat), jnp.float32)
        for j in range(2):
            mine = beyond[j * edge_rows : (j + 1) * edge_rows]
            pool_buf[j, 0:8, :] = jnp.where(low, zero, mine[edge_rows - 8 :])
            pool_buf[j, span + 8 : span + 16, :] = jnp.where(low, mine[:8], zero)

    scoped("project_1", project_b)
    with jax.named_scope("pooling"):
        group = (c * 4 + quarter) * feat * 4 // width
        for k in range(4):

            @pl.when(group == k)
            def _(k=k):
                reach = 2 ** k
                t = h * span + lax.broadcasted_iota(jnp.int32, (span, 1), 0)
                counted = jnp.minimum(t + reach - 1, n_sp * block - 1) - jnp.maximum(t - reach, 0) + 1
                counted = counted.astype(jnp.float32)
                length = span + 16
                for j in range(2):
                    window = pool_buf[j]
                    for e in range(k + 1):
                        window = window + pltpu.roll(window, length - 2 ** e, 0)
                    if reach < 8:
                        window = pltpu.roll(window, length - (8 - reach), 0)
                    value = window[:span] / counted - pool_buf[j, 8 : 8 + span, :]
                    value = value.astype(jnp.bfloat16)
                    for i in range(4):
                        place = (i % 2) * span + (2 * j + i // 2) * half
                        act[place : place + half, hw:] = value[i * half : (i + 1) * half]

    count = give.shape[0]
    tile = width // count
    each = count // 4
    planes = (2 * h, 2 * h + 1, 2 * (1 - h), 2 * (1 - h) + 1)

    def columns_of(n):
        return at(planes[n // each] * (width // 4) + (n % each) * tile, tile)

    def mixed(n):
        return n in (3, 5, 7)

    def swap(n):
        return remote(give.at[n], take.at[n], sw_ss, sw_rs.at[n], to_c)

    def first_stage(n, slot, incoming=False):
        dst = l1.at[n, slot]
        return remote(
            dst if incoming else s1.at[n, slot], dst, r1_ss, r1_rs.at[n, slot],
            to_p if mixed(n) else to_x,
        )

    def second_stage(n, incoming=False):
        return remote(
            l2.at[n] if incoming else s2.at[n], l2.at[n], r2_ss, r2_rs.at[n],
            to_x if mixed(n) else to_p,
        )

    def product(side, n):
        return transposed_dot(act[at(side * span, span), :], w_all[2, columns_of(n), :])

    home = 2 * x + p
    both = 2 * (1 - x) + 1 - p

    def first(n):
        part_sum = product(c, n)
        swap(n).wait_recv()
        total[n] = part_sum.reshape(total.shape[1:]) + take[n].astype(jnp.float32)
        near, middle = 2 * (1 - x) + p, 2 * x + 1 - p
        if mixed(n):
            near, middle = middle, near
        s1[n, 1] = total[n, both].astype(jnp.bfloat16)
        go(first_stage(n, 1))
        s1[n, 0] = total[n, near].astype(jnp.bfloat16)
        go(first_stage(n, 0))

    def second(n):
        middle = 2 * (1 - x) + p if mixed(n) else 2 * x + 1 - p
        first_stage(n, 1, True).wait_recv()
        s2[n] = (total[n, middle] + l1[n, 1].astype(jnp.float32)).astype(jnp.bfloat16)
        go(second_stage(n))

    def last(n):
        first_stage(n, 0, True).wait_recv()
        second_stage(n, True).wait_recv()
        o_ref[:, columns_of(n)] = (
            total[n, home] + l1[n, 0].astype(jnp.float32) + l2[n].astype(jnp.float32)
        ).astype(jnp.bfloat16)

    for q in range(4):
        mine = range(q * each, (q + 1) * each)
        if q == 2:
            with jax.named_scope("second#q=1"):
                for n in range(each, 2 * each):
                    second(n)
        scoped("plane#q=%d" % q, after_y, 2, planes[q])
        with jax.named_scope("give#q=%d" % q):
            for n in mine:
                give[n] = product(other, n).astype(jnp.bfloat16).reshape(give.shape[1:])
                go(swap(n))
        with jax.named_scope("first#q=%d" % q):
            for n in mine:
                first(n)
        if q == 1:
            scoped("after_h_2", after_plane, 2, 0)
            with jax.named_scope("second#q=0"):
                for n in range(each):
                    second(n)
            scoped("after_h_2", after_plane, 2, 1)
        if q > 2:
            with jax.named_scope("second#q=%d" % (q - 1)):
                for n in mine:
                    second(n - each)
    with jax.named_scope("second#q=3"):
        for n in range(3 * each, count):
            second(n)
    with jax.named_scope("last#q=0"):
        for n in range(2 * each):
            last(n)
    with jax.named_scope("last#q=1"):
        for n in range(2 * each, count):
            last(n)

    with jax.named_scope("drain"):
        sends = (
            (w_all.at[:, 0 : 2 * rows], x_ss),
            (w_all.at[:, 0 : 2 * rows], p_ss),
            (w_all.at[:, 0 : 4 * rows], h_ss),
            (w_all.at[:, 0 : 8 * rows], y_ss),
            (x_all.at[0:half], token_p_ss),
            (x_all.at[0 : 2 * half], tx_ss),
            (x_all.at[0 : 3 * half], tw_ss),
            (give, sw_ss),
            (s1, r1_ss),
            (s2, r2_ss),
        )
        for ref, sem in sends:
            remote(ref, ref, sem, e_rs.at[0], to_x).wait_send()
        for copy in (
            decay_p(), decay_x(0), decay_x(1), init_x(0), init_x(1), message(0), message(1), edge_x()
        ):
            copy.wait_send()
        edges(lambda copy: copy.wait_send())


def by_group(
    tokens, norm_gain, query_weight, key_weight, value_weight, outgate_weight, gate_weight,
    gate_bias, decay_extra, init_memory, init_normalizer, head_gain, pool_weight, mem_out_weight,
    pool_out_weight,
):
    n_sp = lax.axis_size("sp")
    block, width = tokens.shape[1:]
    rows = query_weight.shape[0]
    hw = head_gain.shape[1]
    feat = pool_weight.shape[1] // 4
    columns = 3 * hw
    half, span, everything = block // 2, 2 * block, 4 * block
    count, pieces = 8, 4
    tile = width // count
    f32, bf16 = jnp.float32, jnp.bfloat16
    dma = pltpu.SemaphoreType.DMA
    anywhere = pl.BlockSpec(memory_space=pl.ANY)
    mixed = pl.pallas_call(
        functools.partial(layer_kernel, n_sp),
        out_shape=pltpu.VMEM((half, width), bf16),
        in_specs=[anywhere] * 15,
        out_specs=pl.BlockSpec(memory_space=pltpu.VMEM),
        scratch_shapes=[
            pltpu.VMEM((1, width), f32),
            pltpu.VMEM(gate_weight.shape, bf16),
            pltpu.SMEM(gate_bias.shape, f32),
            pltpu.VMEM(head_gain.shape, f32),
            pltpu.VMEM((everything, width), bf16),
            pltpu.VMEM((everything + 16, width), bf16),
            pltpu.VMEM((3, width, columns), bf16),
            pltpu.VMEM((3, 3, rows, columns), bf16),
            pltpu.VMEM((3, rows, columns), bf16),
            pltpu.VMEM((128, width), bf16),
            pltpu.VMEM((2, 2) + decay_extra.shape[1:], f32),
            pltpu.VMEM((2, hw, hw), f32),
            pltpu.VMEM((2,) + init_normalizer.shape[1:], f32),
            pltpu.VMEM((everything, columns), bf16),
            pltpu.VMEM((everything, hw), f32),
            pltpu.VMEM((2, span + 16, feat), f32),
            pltpu.VMEM((everything, columns), bf16),
            pltpu.VMEM((2, 2, hw, span), f32),
            pltpu.VMEM((2, 8, span), f32),
            pltpu.VMEM((2, hw, span), bf16),
            pltpu.VMEM((4, 8, block), f32),
            pltpu.VMEM((128, span), f32),
            pltpu.VMEM((span, 128), f32),
            pltpu.VMEM((2, 8, span), f32),
            pltpu.VMEM((3, 8, hw), f32),
            pltpu.VMEM((3, 8, hw), f32),
            pltpu.VMEM((2, hw, hw), bf16),
            pltpu.VMEM((2, hw, hw), bf16),
            pltpu.VMEM((2, 8, width), bf16),
            pltpu.VMEM((count, 4, half, tile), bf16),
            pltpu.VMEM((count, 4, half, tile), bf16),
            pltpu.VMEM((count, 4, half, tile), f32),
            pltpu.VMEM((count, 2, half, tile), bf16),
            pltpu.VMEM((count, 2, half, tile), bf16),
            pltpu.VMEM((count, half, tile), bf16),
            pltpu.VMEM((count, half, tile), bf16),
            dma((3, 4)),
            dma((4,)),
            dma((4,)),
            dma(()), dma((3, 2)),
            dma(()), dma((3, 2)),
            dma(()), dma((3, 2, 2)),
            dma(()), dma((6,)),
            dma(()), dma((pieces,)),
            dma(()), dma((2, pieces)),
            dma(()), dma((3,)),
            dma((3,)), dma((3,)),
            dma((2,)), dma((2,)),
            dma((2,)), dma((2,)),
            dma((3,)), dma((2,)),
            dma(()), dma((count,)),
            dma(()), dma((count, 2)),
            dma(()), dma((count,)),
        ],
        compiler_params=pltpu.CompilerParams(
            collective_id=0, has_side_effects=True, vmem_limit_bytes=60 * 2**20
        ),
        name="layer",
    )(
        tokens[0], norm_gain[None], query_weight, key_weight, value_weight, outgate_weight,
        gate_weight, gate_bias, decay_extra[0], init_memory[0], init_normalizer[0], head_gain,
        pool_weight, mem_out_weight, pool_out_weight,
    )
    return mixed[None]


def solution(mesh):
    placed = (
        P("fs", "sp", None),
        P(),
        P(("sp", "fs"), "tp"),
        P(("sp", "fs"), "tp"),
        P(("sp", "fs"), "tp"),
        P(("sp", "fs"), "tp"),
        P(None, "tp", None),
        P(None, "tp"),
        P("fs", None, "tp", "sp"),
        P("fs", None, "tp", None, None),
        P("fs", None, "tp", None),
        P("tp", None),
        P(("sp", "fs"), "tp"),
        P(("sp", "fs"), "tp"),
        P(("sp", "fs"), "tp"),
    )

    def body(*args):
        heads, width = args[11].shape
        features = args[12].shape[1]
        block, model_width = args[0].shape[1:]
        fits = (
            lax.axis_size("tp") == 2
            and lax.axis_size("fs") == 4
            and lax.axis_size("sp") == 4
            and heads == 4
            and width == 128
            and features == 8 * width
            and model_width == 2 * features
            and block == 2 * width
        )
        return (by_group if fits else per_device)(*args)

    return jax.shard_map(
        body,
        mesh=mesh,
        in_specs=placed,
        out_specs=P("fs", ("sp", "tp"), None),
        check_vma=False,
    )
```

```python
import functools
import math

import jax
import jax.numpy as jnp
from jax import lax
from jax.experimental import pallas as pl
from jax.experimental.pallas import tpu as pltpu
from jax.sharding import PartitionSpec as P

MESH = pl.DeviceIdType.MESH

HALO = 8


norm_eps = 1e-06
exact_mode = lax.Precision.HIGHEST


def carried_in(x, axis, combine, identity, reverse):
    length, position = (lax.axis_size(axis), lax.axis_index(axis))
    everything = jax.tree.map(lambda part: lax.all_gather(part, axis), x)
    start = jax.tree.map(
        lambda part, zero: jnp.broadcast_to(jnp.asarray(zero, part.dtype), part.shape), x, identity
    )

    def lap(k, before):
        at = length - 1 - k if reverse else k
        reached = at > position if reverse else at < position
        new = combine(before, jax.tree.map(lambda part: part[at], everything))
        return jax.tree.map(lambda a, b: jnp.where(reached, a, b), new, before)

    return lax.fori_loop(0, length, lap, start)


def padded_2(block, sides, width):
    for axis, dim in sides:
        count = lax.axis_size(axis)
        forward = [(i, i + 1) for i in range(count - 1)]
        backward = [(target, source) for source, target in forward]
        low = lax.ppermute(
            lax.slice_in_dim(block, block.shape[dim] - width, None, axis=dim), axis, forward
        )
        high = lax.ppermute(lax.slice_in_dim(block, 0, width, axis=dim), axis, backward)
        block = jnp.concatenate([low, block, high], axis=dim)
    return block


def block_output(
    query_rows, key_rows, value_rows, input_gate, log_forget, memory, normalizer, stabilizer
):
    block_len = query_rows.shape[1]
    key_scale = key_rows.shape[-1] ** (-0.5)
    lower_mask = jnp.tril(jnp.ones((block_len, block_len), dtype=bool))
    summed = jnp.cumsum(log_forget, axis=-1)
    log_decay = jnp.where(
        lower_mask, summed[:, :, None] - summed[:, None, :] + input_gate[:, None, :], -jnp.inf
    )
    log_carry = stabilizer[:, None] + summed
    running_max = jnp.maximum(log_carry, jnp.max(log_decay, axis=-1))
    scores = (
        jnp.einsum("btd,bsd->bts", query_rows, key_rows, preferred_element_type=jnp.float32)
        * key_scale
    )
    inner_weight = jnp.exp(log_decay - running_max[:, :, None]) * scores
    weight_rounded = inner_weight.astype(jnp.bfloat16)
    carry_weight = jnp.exp(log_carry - running_max)
    query_wide = query_rows.astype(jnp.float32)
    numerator = carry_weight[:, :, None] * jnp.einsum(
        "bed,btd->bte", memory, query_wide, precision=exact_mode
    )
    numerator = numerator + jnp.einsum(
        "bts,bse->bte", weight_rounded, value_rows, preferred_element_type=jnp.float32
    )
    denominator = carry_weight * jnp.einsum(
        "bd,btd->bt", normalizer, query_wide, precision=exact_mode
    )
    denominator = denominator + jnp.sum(inner_weight, axis=-1)
    return numerator / jnp.maximum(jnp.abs(denominator), jnp.exp(-running_max))[:, :, None]


def block_summary(key_rows, value_rows, input_gate, log_forget):
    key_wide = key_rows.astype(jnp.float32) * key_rows.shape[-1] ** (-0.5)
    summed = jnp.cumsum(log_forget, axis=-1)
    forget_total = summed[:, -1]
    log_weight = forget_total[:, None] - summed + input_gate
    running_max = jnp.max(log_weight, axis=-1)
    weights = jnp.exp(log_weight - running_max[:, None])
    memory = jnp.einsum(
        "bse,bsd->bed",
        weights[:, :, None] * value_rows.astype(jnp.float32),
        key_wide,
        precision=exact_mode,
    )
    normalizer = jnp.einsum("bs,bsd->bd", weights, key_wide, precision=exact_mode)
    return (memory, normalizer, running_max, forget_total)


def combine(earlier, latter):
    early_memory, early_norm, early_max, early_total = earlier
    late_memory, late_norm, late_max, late_total = latter
    joint_max = jnp.maximum(early_max + late_total, late_max)
    early_scale = jnp.exp(early_max + late_total - joint_max)
    late_scale = jnp.exp(late_max - joint_max)
    memory = early_scale[:, None, None] * early_memory + late_scale[:, None, None] * late_memory
    normalizer = early_scale[:, None] * early_norm + late_scale[:, None] * late_norm
    return (memory, normalizer, joint_max, early_total + late_total)


def span_sweep(
    query_rows, key_rows, value_rows, input_gate, log_forget, memory, normalizer, stabilizer, span
):
    block_count = query_rows.shape[1] // span

    def to_blocks(array):
        shaped = array.reshape((array.shape[0], block_count, span) + array.shape[2:])
        return jnp.moveaxis(shaped, 1, 0)

    def advance(carried, pieces):
        query_blk, key_blk, value_blk, gate_blk, forget_blk = pieces
        result = block_output(
            query_blk, key_blk, value_blk, gate_blk, forget_blk, carried[0], carried[1], carried[2]
        )
        return (combine(carried, block_summary(key_blk, value_blk, gate_blk, forget_blk)), result)

    initial = (memory, normalizer, stabilizer, jnp.zeros_like(stabilizer))
    ignored, outputs = lax.scan(
        advance,
        initial,
        tuple(
            (
                to_blocks(array)
                for array in (query_rows, key_rows, value_rows, input_gate, log_forget)
            )
        ),
    )
    return jnp.moveaxis(outputs, 0, 1).reshape(query_rows.shape[:2] + (value_rows.shape[2],))


def reverse_time(array):
    return jnp.flip(array, axis=1)


def to_heads(matrix, head_count):
    shaped = matrix.reshape(matrix.shape[0], head_count, matrix.shape[1] // head_count)
    return shaped.transpose(1, 0, 2)


def pool_window(padded, positions, channels, seq_len, group_size):
    row_count = positions.shape[0]
    group_index = channels // group_size
    reach_left = jnp.left_shift(jnp.ones_like(group_index), group_index)
    reach_right = reach_left - 1
    window_sum = jnp.zeros((row_count, channels.shape[0]), jnp.float32)
    for offset in range(-HALO, HALO):
        inside = ((offset >= -reach_left) & (offset <= reach_right)).astype(jnp.float32)
        window_sum = window_sum + inside * padded[HALO + offset : HALO + offset + row_count]
    first_pos = jnp.maximum(positions[:, None] - reach_left[None, :], 0)
    last_pos = jnp.minimum(positions[:, None] + reach_right[None, :], seq_len - 1)
    counted = (last_pos - first_pos + 1).astype(jnp.float32)
    centre = padded[HALO : HALO + row_count]
    return (window_sum / counted - centre).astype(jnp.bfloat16)


def per_device(
    tokens,
    norm_gain,
    query_weight,
    key_weight,
    value_weight,
    outgate_weight,
    gate_weight,
    gate_bias,
    decay_extra,
    init_memory,
    init_normalizer,
    head_gain,
    pool_weight,
    mem_out_weight,
    pool_out_weight,
):
    block_len = tokens.shape[1]
    model_width = tokens.shape[2]
    head_count, head_width = head_gain.shape
    span = math.gcd(block_len, 256)
    flattened = tokens[0].astype(jnp.float32)
    normed = (
        flattened
        * lax.rsqrt(jnp.mean(flattened * flattened, axis=-1, keepdims=True) + norm_eps)
        * norm_gain
    ).astype(jnp.bfloat16)
    zero_start = tuple(
        (
            jnp.zeros((block_len, weight.shape[1]), jnp.float32)
            for weight in (query_weight, key_weight, value_weight, outgate_weight, pool_weight)
        )
    )
    zero_start = zero_start + (
        jnp.zeros((model_width, mem_out_weight.shape[1]), jnp.bfloat16),
        jnp.zeros((model_width, pool_out_weight.shape[1]), jnp.bfloat16),
    )
    line_query, line_key, line_value, line_outgate, line_pool, line_mem_out, line_pool_out = (
        lax.all_gather(query_weight, "fs", axis=0, tiled=True),
        lax.all_gather(key_weight, "fs", axis=0, tiled=True),
        lax.all_gather(value_weight, "fs", axis=0, tiled=True),
        lax.all_gather(outgate_weight, "fs", axis=0, tiled=True),
        lax.all_gather(pool_weight, "fs", axis=0, tiled=True),
        lax.all_gather(mem_out_weight, "fs", axis=0, tiled=True),
        lax.all_gather(pool_out_weight, "fs", axis=0, tiled=True),
    )
    pieces = (
        lax.all_gather(line_query, "sp", axis=0, tiled=True),
        lax.all_gather(line_key, "sp", axis=0, tiled=True),
        lax.all_gather(line_value, "sp", axis=0, tiled=True),
        lax.all_gather(line_outgate, "sp", axis=0, tiled=True),
        lax.all_gather(line_pool, "sp", axis=0, tiled=True),
        lax.all_gather(line_mem_out, "sp", axis=0, tiled=True),
        lax.all_gather(line_pool_out, "sp", axis=0, tiled=True),
    )
    partial_sums = tuple(
        (
            jnp.dot(normed, weight_rows, preferred_element_type=jnp.float32)
            for weight_rows in pieces[:5]
        )
    )
    collected = tuple((weight_rows for weight_rows in pieces[5:]))
    folded = partial_sums + collected
    query_proj, key_proj, value_proj, outgate, pool_input = tuple(
        (running.astype(jnp.bfloat16) for running in folded[:5])
    )
    mem_weight_all = folded[5]
    pool_weight_all = folded[6]
    gate_pre = lax.dot_general(
        normed,
        gate_weight.reshape(4 * head_count, model_width),
        (((1,), (1,)), ((), ())),
        preferred_element_type=jnp.float32,
    ) + gate_bias.reshape(4 * head_count)
    gate_pre = gate_pre.reshape(block_len, 4, head_count).transpose(1, 2, 0)
    query_heads = to_heads(query_proj, head_count)
    key_heads = to_heads(key_proj, head_count)
    value_heads = to_heads(value_proj, head_count)
    forward_forget = jax.nn.log_sigmoid(gate_pre[1]) + decay_extra[0, 0]
    backward_forget = jax.nn.log_sigmoid(gate_pre[3]) + decay_extra[0, 1]
    zero_rows = jnp.zeros((head_count,), jnp.float32)
    identity = (
        jnp.zeros((head_count, head_width, head_width), jnp.float32),
        jnp.zeros((head_count, head_width), jnp.float32),
        jnp.full((head_count,), -1e30, jnp.float32),
        zero_rows,
    )
    front_memory, front_norm, front_max, front_total = block_summary(
        key_heads, value_heads, gate_pre[0], forward_forget
    )
    prefix = carried_in(
        (front_memory, front_norm, front_max, front_total), "sp", combine, identity, False
    )
    incoming = combine((init_memory[0, 0], init_normalizer[0, 0], zero_rows, zero_rows), prefix)
    forward_out = span_sweep(
        query_heads,
        key_heads,
        value_heads,
        gate_pre[0],
        forward_forget,
        incoming[0],
        incoming[1],
        incoming[2],
        span,
    )
    back_query = reverse_time(query_heads)
    back_key = reverse_time(key_heads)
    back_value = reverse_time(value_heads)
    back_gate = reverse_time(gate_pre[2])
    back_forget = reverse_time(backward_forget)
    rear_memory, rear_norm, rear_max, rear_total = block_summary(
        back_key, back_value, back_gate, back_forget
    )
    suffix = carried_in(
        (rear_memory, rear_norm, rear_max, rear_total), "sp", combine, identity, True
    )
    back_incoming = combine(
        (init_memory[0, 1], init_normalizer[0, 1], zero_rows, zero_rows), suffix
    )
    backward_out = reverse_time(
        span_sweep(
            back_query,
            back_key,
            back_value,
            back_gate,
            back_forget,
            back_incoming[0],
            back_incoming[1],
            back_incoming[2],
            span,
        )
    )
    summed_dirs = (forward_out + backward_out).transpose(1, 0, 2)
    normed_heads = (
        summed_dirs
        * lax.rsqrt(jnp.mean(summed_dirs * summed_dirs, axis=-1, keepdims=True) + norm_eps)
        * head_gain
    )
    out_gate = jax.nn.sigmoid(
        outgate.astype(jnp.float32).reshape(block_len, head_count, head_width)
    )
    memory_out = (
        (normed_heads * out_gate).astype(jnp.bfloat16).reshape(block_len, head_count * head_width)
    )
    padded = padded_2(pool_input, (("sp", 0),), HALO).astype(jnp.float32)
    feature_count = pool_input.shape[1]
    positions = lax.axis_index("sp") * block_len + jnp.arange(block_len, dtype=jnp.int32)
    channels = lax.axis_index("tp") * feature_count + jnp.arange(feature_count, dtype=jnp.int32)
    pool_out = pool_window(
        padded, positions, channels, block_len * lax.axis_size("sp"), model_width // 4
    )
    own_rows = block_len // lax.axis_size("tp")
    result = lax.dot_general(
        memory_out, mem_weight_all, (((1,), (1,)), ((), ())), preferred_element_type=jnp.float32
    )
    mixed = lax.psum_scatter(
        (
            result
            + lax.dot_general(
                pool_out,
                pool_weight_all,
                (((1,), (1,)), ((), ())),
                preferred_element_type=jnp.float32,
            )
        ).astype(jnp.bfloat16),
        "tp",
        scatter_dimension=0,
        tiled=True,
    )
    return mixed.reshape(1, own_rows, model_width)


LOG2E = math.log2(math.e)


def scan_lanes(x, combine_, fill, reverse):
    length = x.shape[1]
    lane = lax.broadcasted_iota(jnp.int32, x.shape, 1)
    d = 1
    while d < length:
        if reverse:
            moved = jnp.where(lane < length - d, pltpu.roll(x, length - d, 1), fill)
        else:
            moved = jnp.where(lane >= d, pltpu.roll(x, d, 1), fill)
        x = combine_(x, moved)
        d *= 2
    return x


def transposed_dot(a, b):
    return lax.dot_general(a, b, (((1,), (1,)), ((), ())), preferred_element_type=jnp.float32)


def layer_kernel(
    n_sp,
    token_ref, gain_hbm, qw, kw, vw, ow, gate_hbm, bias_hbm, decay_ref, mem_ref, nrm_ref,
    hgain_hbm, pw, mw, fw,
    o_ref,
    gain_ref, gate_ref, bias_ref, hgain_ref, x_all, normed, w_all, stage, transit, gmat, dec, init, nrm, proj_a, ungated, pool_buf, act,
    within, dens, values_t, pre_rows, flat, cols, run_rows, aux_out, aux_in, state_out, state_in, halo_tok,
    give, take, total, s1, l1, s2, l2,
    loc_w, loc_s, small_sem, x_ss, x_rs, p_ss, p_rs, h_ss, h_rs, y_ss, y_rs,
    token_p_ss, token_p_rs, tx_ss, tx_rs, tw_ss, tw_rs, d_ss, d_rs, i_ss, i_rs, m_ss, m_rs, e_ss, e_rs,
    sw_ss, sw_rs, r1_ss, r1_rs, r2_ss, r2_rs,
):
    block, width = token_ref.shape
    rows = qw.shape[0]
    hw = hgain_hbm.shape[1]
    feat = pw.shape[1] // 4
    half = block // 2
    span = 2 * block
    pieces_t = token_p_rs.shape[0]
    part = half // pieces_t
    z, fs, c = lax.axis_index("sp"), lax.axis_index("fs"), lax.axis_index("tp")
    y, x = fs // 2, lax.rem(fs, 2)
    h, p = z // 2, lax.rem(z, 2)
    zn = z + 1 - 2 * p
    zf = lax.rem(z + 2, n_sp)
    zfn = zf + 1 - 2 * p
    xn, yn = 2 * y + 1 - x, 2 * (1 - y) + x
    other = 1 - c
    low = h == 0
    quarter = 2 * p + x
    to_x, to_y, to_p, to_h, to_c = {"fs": xn}, {"fs": yn}, {"sp": zn}, {"sp": zf}, {"tp": other}

    def remote(src, dst, ss, rs, device):
        return pltpu.make_async_remote_copy(
            src_ref=src, dst_ref=dst, send_sem=ss, recv_sem=rs,
            device_id=device, device_id_type=MESH,
        )

    def at(start, size):
        return pl.ds(pl.multiple_of(start, size), size)

    inner, outer = p != h, p == h
    to_m = {"sp": n_sp - 1 - z}
    barrier = pltpu.get_barrier_semaphore()
    for device in (to_x, to_y, to_p, to_h, to_c):
        pl.semaphore_signal(barrier, inc=1, device_id=device, device_id_type=MESH)

    @pl.when(inner)
    def _():
        pl.semaphore_signal(barrier, inc=1, device_id=to_m, device_id_type=MESH)

    groups = (((qw, hw), (kw, hw), (vw, hw)), ((ow, hw), (pw, feat)), ((mw, hw), (fw, feat)))
    quarters = (quarter, 2 * p + 1 - x, 2 * (1 - p) + 1 - x, 2 * (1 - p) + x)

    def row_block(zs, ys, xs):
        return at((zs * 4 + ys * 2 + xs) * rows, rows)

    def local_weights(g):
        copies = []
        for slot in (1, 2, 3, 0):
            start = 0
            for i, (ref, size) in enumerate(groups[g]):
                columns = pl.ds(start, size)
                if slot:
                    dst = stage.at[g, slot - 1, :, columns]
                else:
                    dst = w_all.at[g, row_block(z, y, x), columns]
                copies.append(
                    pltpu.make_async_copy(
                        ref.at[:, at(quarters[slot] * size, size)], dst, loc_w.at[g, slot]
                    )
                )
                start += size
        return copies

    small = [
        pltpu.make_async_copy(src, dst, small_sem.at[i])
        for i, (src, dst) in enumerate(
            (
                (gain_hbm, gain_ref), (gate_hbm, gate_ref), (bias_hbm, bias_ref),
                (hgain_hbm, hgain_ref),
            )
        )
    ]
    locals_ = [local_weights(g) for g in range(3)]
    own_tokens = pltpu.make_async_copy(
        token_ref, x_all.at[at((2 * x + p) * block, block)], loc_s.at[0]
    )
    own_decay = pltpu.make_async_copy(decay_ref, dec.at[x, p], loc_s.at[1])
    own_init = pltpu.make_async_copy(mem_ref.at[h, quarter], init.at[x], loc_s.at[2])
    own_nrm = pltpu.make_async_copy(nrm_ref, nrm.at[x], loc_s.at[3])
    for copy in locals_[0]:
        copy.start()
    own_tokens.start()
    for copy in locals_[1] + locals_[2]:
        copy.start()
    for copy in small + [own_decay, own_init, own_nrm]:
        copy.start()

    def x_copy(g, s, incoming=False):
        if s == 0:
            dst = w_all.at[g, row_block(z, y, 1 - x if incoming else x)]
        else:
            dst = transit.at[g]
        return remote(dst if incoming else stage.at[g, s], dst, x_ss, x_rs.at[g, s], to_x)

    def p_copy(g, s, incoming=False):
        dst = w_all.at[g, row_block(zn if incoming else z, y, 1 - x if s else x)]
        src = dst if incoming else (transit.at[g] if s else stage.at[g, 2])
        return remote(src, dst, p_ss, p_rs.at[g, s], to_p)

    def h_plane(g, e, s, incoming=False):
        source = 2 * (1 - h if incoming else h) + e
        ref = w_all.at[g, row_block(source, y, 1 - x if s else x)]
        return remote(ref, ref, h_ss, h_rs.at[g, e, s], to_h)

    def h_copy(g, k, s, incoming=False):
        return h_plane(g, 1 - p if k else p, s, incoming)

    def y_copy(g, plane, s, incoming=False):
        ref = w_all.at[g, row_block(plane, 1 - y if incoming else y, 1 - x if s else x)]
        return remote(ref, ref, y_ss, y_rs.at[2 + plane if g == 2 else g], to_y)

    def go(copy):
        copy.start()

    def ready(g, slots):
        for slot in slots:
            ref = stage.at[g, slot - 1] if slot else w_all.at[g, row_block(z, y, x)]
            pltpu.make_async_copy(ref, ref, loc_w.at[g, slot]).wait()

    def go_if(here, copy):
        @pl.when(here)
        def _():
            copy.start()

    def begin_x(g):
        ready(g, (1, 2))
        go(x_copy(g, 1))
        go(x_copy(g, 0))

    def begin_p(g):
        ready(g, (3,))
        go(p_copy(g, 0))

    def begin_y(g):
        ready(g, (0,))
        go(y_copy(g, z, 0))

    def after_x(g):
        x_copy(g, 1, True).wait_recv()
        go(p_copy(g, 1))
        x_copy(g, 0, True).wait_recv()
        if g < 2:
            go(y_copy(g, z, 1))
        else:
            go_if(inner, y_copy(g, z, 1))

    def after_p_y(g):
        for s in range(2):
            p_copy(g, s, True).wait_recv()
            go(y_copy(g, zn, s))

    def all_far_if(here, g):
        @pl.when(here)
        def _():
            for e in range(2):
                for s in range(2):
                    h_plane(g, e, s).start()

    def far_if(here, g):
        @pl.when(here)
        def _():
            for s in range(2):
                h_copy(g, 0, s).start()

    def after_p(g):
        for s in range(2):
            p_copy(g, s, True).wait_recv()
            go(h_copy(g, 1, s))
            go(y_copy(g, zn, s))

    def after_h(g, k):
        for s in range(2):
            h_copy(g, k, s, True).wait_recv()
            go(y_copy(g, (zf, zfn)[k], s))

    def after_plane(g, e):
        for s in range(2):
            h_plane(g, e, s, True).wait_recv()
            go(y_copy(g, 2 * (1 - h) + e, s))

    def arrived_y(ref, sem):
        remote(ref, ref, y_ss, sem, to_y).wait_recv()

    def after_y(g, plane):
        start = pl.multiple_of((plane * 4 + 2 * (1 - y)) * rows, rows)
        arrived_y(w_all.at[g, pl.ds(start, 2 * rows)], y_rs.at[2 + plane])

    def all_y(g):
        arrived_y(w_all.at[g, pl.ds(0, 8 * rows)], y_rs.at[g])

    def token_rows(j, b, side, i):
        return at((2 * j + b) * block + side * half + i * part, part)

    def token_p(i, incoming=False):
        b = 1 - p if incoming else p
        dst = x_all.at[token_rows(x, b, c, i)]
        src = dst if incoming else token_ref.at[at(c * half + i * part, part)]
        return remote(src, dst, token_p_ss, token_p_rs.at[i], to_p)

    def token_x(kind, i, incoming=False):
        b = 1 - p if kind else p
        dst = x_all.at[token_rows(1 - x if incoming else x, b, c, i)]
        src = dst if incoming or kind else token_ref.at[at(c * half + i * part, part)]
        return remote(src, dst, tx_ss, tx_rs.at[kind, i], to_x)

    places = ((x, 1 - p), (1 - x, p), (1 - x, 1 - p))

    def token_swap(which, i, incoming=False):
        j, b = places[which]
        ref = x_all.at[token_rows(j, b, other if incoming else c, i)]
        return remote(ref, ref, tw_ss, tw_rs.at[which], to_c)

    edge_rows = halo_tok.shape[1]

    def edge_copy(which):
        return remote(
            token_ref.at[at((1 - h) * (block - edge_rows), edge_rows)], halo_tok.at[x],
            e_ss.at[which], e_rs.at[0], (to_h, to_m)[which],
        )

    def edges(action):
        @pl.when(inner)
        def _():
            for which in range(2):
                action(edge_copy(which))

    def edge_x(incoming=False):
        ref = halo_tok.at[1 - x if incoming else x]
        return remote(ref, ref, e_ss.at[2], e_rs.at[1], to_x)

    def normalise_edges():
        wide = halo_tok[...].reshape(2 * edge_rows, width).astype(jnp.float32)
        normed[4 * block :, :] = (
            wide
            * lax.rsqrt(jnp.mean(wide * wide, axis=-1, keepdims=True) + norm_eps)
            * gain_ref[...]
        ).astype(jnp.bfloat16)

    def decay_p(incoming=False):
        dst = dec.at[x, 1 - p if incoming else p]
        return remote(dst if incoming else decay_ref, dst, d_ss.at[0], d_rs.at[0], to_p)

    def decay_x(kind, incoming=False):
        dst = dec.at[1 - x if incoming else x, 1 - p if kind else p]
        src = dst if incoming or kind else decay_ref
        return remote(src, dst, d_ss.at[1 + kind], d_rs.at[1 + kind], to_x)

    def init_x(which, incoming=False):
        dst = (init, nrm)[which].at[1 - x if incoming else x]
        src = (mem_ref.at[h, 2 * p + 1 - x], nrm_ref)[which]
        return remote(dst if incoming else src, dst, i_ss.at[which], i_rs.at[which], to_x)

    def normalise(j, b):
        step = 64

        def body(i, carry):
            here = at((2 * j + b) * block + i * step, step)
            wide = x_all[here, :].astype(jnp.float32)
            normed[here, :] = (
                wide
                * lax.rsqrt(jnp.mean(wide * wide, axis=-1, keepdims=True) + norm_eps)
                * gain_ref[...]
            ).astype(jnp.bfloat16)
            return carry

        lax.fori_loop(0, block // step, body, 0)
        here = at((2 * j + b) * block, block)
        pre_rows[2 * j + b] = transposed_dot(normed[here, :], gmat[...]).T[:8]

    def scoped(name, function, *args):
        with jax.named_scope(name):
            return function(*args)

    def token_arrivals_p(these):
        for i in these:
            token_p(i, True).wait_recv()
            go(token_swap(0, i))
            go(token_x(1, i))

    def token_arrivals_x(kind, these):
        for i in these:
            token_x(kind, i, True).wait_recv()
            go(token_swap(1 + kind, i))

    def swapped(which):
        j, b = places[which]
        ref = x_all.at[at((2 * j + b) * block + other * half, half)]
        remote(ref, ref, tw_ss, tw_rs.at[which], to_c).wait_recv()
        normalise(j, b)

    def pick_gates():
        gmat[...] = jnp.zeros_like(gmat)
        pick = lax.broadcasted_iota(jnp.int32, (4, width), 0) == quarter
        row16 = lax.broadcasted_iota(jnp.int32, (16, width), 0)
        gates16 = jnp.zeros((16, width), jnp.float32)
        for i in range(4):
            row = jnp.sum(
                jnp.where(pick, gate_ref[i].astype(jnp.float32), 0.0), axis=0, keepdims=True
            )
            gates16 = jnp.where((row16 == i) | (row16 == i + 4), row, gates16)
        gmat[0:16, :] = gates16.astype(jnp.bfloat16)

    scoped("barrier", pl.semaphore_wait, barrier, 5 + inner.astype(jnp.int32))
    begin_x(0)
    begin_p(0)
    begin_y(0)
    go(h_copy(0, 0, 0))
    edges(lambda copy: copy.start())
    own_decay.wait()
    go(decay_p())
    go(decay_x(0))
    go(token_p(0))
    begin_x(1)
    for i in range(pieces_t):
        go(token_x(0, i))
    begin_y(1)
    for copy in small:
        copy.wait()
    scoped("pick", pick_gates)
    scoped("tok_own", own_tokens.wait)
    scoped("norm_own", normalise, x, p)
    scoped("after_x_0", after_x, 0)
    go(h_copy(0, 0, 1))
    early = 2
    for i in range(1, early):
        go_if(outer, token_p(i))
    remote(halo_tok.at[x], halo_tok.at[x], e_ss.at[0], e_rs.at[0], to_h).wait_recv()
    go(edge_x())
    scoped("after_p_0", after_p, 0)
    for i in range(1, early):
        go_if(inner, token_p(i))
    for i in range(early, pieces_t):
        go(token_p(i))
    begin_p(1)
    scoped("after_x_1", after_x, 1)
    far_if(outer, 1)
    scoped("after_h_0", after_h, 0, 0)
    scoped("tok_p", token_arrivals_p, (0,))
    scoped("tok_x0", token_arrivals_x, 0, (0, 1))
    scoped("after_h_0", after_h, 0, 1)
    scoped("tok_p", token_arrivals_p, (1,))
    scoped("tok_x0", token_arrivals_x, 0, (2, 3))
    scoped("norm_x", swapped, 1)
    far_if(inner, 1)
    edge_x(True).wait_recv()
    normalise_edges()
    scoped("tok_p", token_arrivals_p, (2, 3))
    decay_p(True).wait_recv()
    go(decay_x(1))
    go(init_x(0))
    go(init_x(1))
    begin_x(2)
    begin_y(2)

    scoped("norm_p", swapped, 0)

    @pl.when(outer)
    def _():
        scoped("after_p_1", after_p, 1)

    scoped("after_y_0", all_y, 0)

    def project(g, place, store):
        i = 2 * place[0] + place[1]
        store(i, jnp.dot(
            normed[at(i * block, block), :], w_all[g], preferred_element_type=jnp.float32
        ).astype(jnp.bfloat16))

    def store_a(i, value):
        proj_a[at(i * block, block), :] = value

    for place in ((x, p), places[0], places[1]):
        scoped("project_0", project, 0, place, store_a)
    scoped("tok_x1", token_arrivals_x, 1, (0, 1))

    @pl.when(inner)
    def _():
        scoped("after_p_1i", after_p, 1)

    begin_p(2)

    scoped("tok_x1", token_arrivals_x, 1, (2, 3))

    @pl.when(inner)
    def _():
        scoped("after_h_1i", after_h, 1, 0)

    scoped("norm_px", swapped, 2)
    decay_x(0, True).wait_recv()
    decay_x(1, True).wait_recv()

    scoped("after_x_2", after_x, 2)

    with jax.named_scope("gates"):
        tall = []
        for j in range(2):
            tall.append(jnp.concatenate([pre_rows[2 * j], pre_rows[2 * j + 1]], axis=1))
        row8 = lax.broadcasted_iota(jnp.int32, (8, span), 0)
        gates = jnp.where(row8 < 4, tall[0], tall[1])
        extra = jnp.zeros((8, span), jnp.float32)
        for i in range(4):
            gates = gates + jnp.where((row8 == i) | (row8 == i + 4), bias_ref[i, quarter], 0.0)
        for j in range(2):
            for direction in range(2):
                value = jnp.concatenate(
                    [dec[j, b, direction, pl.ds(quarter, 1), :] for b in range(2)], axis=1
                )
                extra = jnp.where(row8 == 4 * j + 1 + 2 * direction, value, extra)
        forget = jnp.minimum(gates, 0.0) - jnp.log1p(jnp.exp(-jnp.abs(gates))) + extra
        sum_f = pltpu.roll(scan_lanes(forget, jnp.add, 0.0, False), 7, 0)
        sum_b = pltpu.roll(scan_lanes(forget, jnp.add, 0.0, True), 7, 0)
        level_f = gates - sum_f
        level_b = gates - sum_b
        run_f = scan_lanes(level_f, jnp.maximum, -1e30, False)
        run_b = scan_lanes(level_b, jnp.maximum, -1e30, True)
        top_f = jnp.maximum(run_f[:, span - 1 : span], 0.0)
        top_b = jnp.maximum(run_b[:, 0:1], 0.0)
        end_f = sum_f[:, span - 1 : span] + top_f
        end_b = sum_b[:, 0:1] + top_b
        aux_out[2] = jnp.broadcast_to(jnp.where(low, end_f, end_b), (8, hw))

    def message(which, incoming=False):
        src = (aux_out, state_out)[which]
        dst = (aux_in, state_in)[which]
        return remote(dst if incoming else src, dst, m_ss.at[which], m_rs.at[which], to_h)

    @pl.when(outer)
    def _():
        scoped("after_h_1", after_h, 1, 0)

    scoped("project_0", project, 0, places[2], store_a)

    with jax.named_scope("state"):
        scale_bits = -0.5 * math.log2(hw)
        lf2 = level_f * LOG2E + scale_bits
        lb2 = level_b * LOG2E + scale_bits
        own_init.wait()
        own_nrm.wait()
        init_x(0, True).wait_recv()
        init_x(1, True).wait_recv()
        leave_f = jnp.exp2(lf2 - top_f * LOG2E)
        leave_b = jnp.exp2(lb2 - top_b * LOG2E)
        keep_f = jnp.exp(-top_f)
        keep_b = jnp.exp(-top_b)
        for j in range(2):
            here = slice(j * span, (j + 1) * span)
            own = jnp.where(low, leave_f[4 * j : 4 * j + 1], leave_b[4 * j + 2 : 4 * j + 3])
            kept = jnp.where(low, keep_f[4 * j : 4 * j + 1], keep_b[4 * j + 2 : 4 * j + 3])
            values = proj_a[here, 2 * hw : 3 * hw].astype(jnp.float32).T
            values_t[j] = values.astype(jnp.bfloat16)
            values = values * own
            lhs = jnp.concatenate(
                [values, jnp.broadcast_to(own, (8, span))], axis=0
            ).astype(jnp.bfloat16)
            grown = jnp.dot(lhs, proj_a[here, hw : 2 * hw], preferred_element_type=jnp.float32)
            state_out[j] = (kept * init[j] + grown[:hw]).astype(jnp.bfloat16)
            aux_out[j] = kept * nrm[j, h, pl.ds(quarter, 1), :] + grown[hw:]
    go(message(0))
    go(message(1))

    with jax.named_scope("levels"):
        flat[16:, :] = jnp.zeros_like(flat[16:, :])
        flat[0:8, :] = lf2
        flat[8:16, :] = lb2
        cols[...] = flat[...].T
        run_rows[0] = run_f * LOG2E
        run_rows[1] = run_b * LOG2E

    def attend(j):
        here = slice(j * span, (j + 1) * span)
        f, b = 4 * j, 4 * j + 2
        levels = [jnp.broadcast_to(cols[:, k : k + 1], (span, half)) for k in (f, 8 + b)]
        for i in range(4):
            r0 = i * half
            mine = slice(j * span + r0, j * span + r0 + half)
            score = transposed_dot(proj_a[here, hw : 2 * hw], proj_a[mine, 0:hw])
            for which, first, last in ((0, 0, r0 + half), (1, r0, span)):
                row = (f, b)[which]
                peak = run_rows[which, row : row + 1, r0 : r0 + half]
                weight = jnp.exp2(levels[which][first:last] - peak) * score[first:last]
                s = first + lax.broadcasted_iota(jnp.int32, weight.shape, 0)
                t = r0 + lax.broadcasted_iota(jnp.int32, weight.shape, 1)
                weight = jnp.where(s >= t if which else s <= t, weight, 0.0)
                within[which, j, :, r0 : r0 + half] = jnp.dot(
                    values_t[j, :, first:last], weight.astype(jnp.bfloat16),
                    preferred_element_type=jnp.float32,
                )
                dens[which, j : j + 1, r0 : r0 + half] = jnp.sum(weight, axis=0, keepdims=True)

    scoped("attend_0", attend, 0)
    scoped("attend_1", attend, 1)
    scoped("after_h_1", after_h, 1, 1)
    go_if(outer & (p == 0), y_copy(2, z, 1))
    scoped("after_p_2y", after_p_y, 2)
    go_if(outer & (p == 1), y_copy(2, z, 1))
    all_far_if(inner, 2)
    scoped("state_in", message(1, True).wait_recv)
    scoped("aux_in", message(0, True).wait_recv)
    all_far_if(outer, 2)

    with jax.named_scope("enter"):
        arrived = aux_in[2, :, 0:1]
        enter_f = jnp.where(low, 0.0, arrived)
        enter_b = jnp.where(low, arrived, 0.0)
        factors = []
        for run, enter, summed in ((run_f, enter_f, sum_f), (run_b, enter_b, sum_b)):
            peak = jnp.maximum(run, enter)
            factors.append(
                (jnp.exp(run - peak), jnp.exp(enter - peak), jnp.exp(-(summed + peak)))
            )

    def finish(j):
        own_n = jnp.broadcast_to(nrm[j, h, pl.ds(quarter, 1), :], (8, hw))
        there = state_in[j].astype(jnp.float32)
        carry_in = jnp.concatenate(
            [
                jnp.where(low, init[j], there),
                jnp.where(low, there, init[j]),
                jnp.where(low, own_n, aux_in[j]),
                jnp.where(low, aux_in[j], own_n),
            ],
            axis=0,
        )
        coarse = carry_in.astype(jnp.bfloat16)
        fine = (carry_in - coarse.astype(jnp.float32)).astype(jnp.bfloat16)
        q = proj_a[j * span : (j + 1) * span, 0:hw]
        carry = transposed_dot(
            jnp.concatenate([coarse, fine], axis=1), jnp.concatenate([q, q], axis=1)
        )
        both = []
        for which in range(2):
            row = 4 * j + 2 * which
            grow, decay, floor = (part[row : row + 1] for part in factors[which])
            den0 = carry[2 * hw + 8 * which : 2 * hw + 8 * which + 1]
            den = grow * dens[which, j : j + 1, :] + decay * den0
            share = 1.0 / jnp.maximum(jnp.abs(den), floor)
            both.append(
                (grow * share) * within[which, j]
                + (decay * share) * carry[which * hw : (which + 1) * hw]
            )
        summed = both[0] + both[1]
        summed = summed * lax.rsqrt(jnp.mean(summed * summed, axis=0, keepdims=True) + norm_eps)
        ungated[j * span : (j + 1) * span, :] = summed.T * hgain_ref[pl.ds(quarter, 1), :]

    scoped("finish", finish, 0)
    scoped("finish", finish, 1)

    scoped("after_y_1", all_y, 1)

    def project_b():
        for i in range(4):
            last_rows = 2 * edge_rows if i == 3 else 0
            value = jnp.dot(
                normed[i * block : (i + 1) * block + last_rows, :], w_all[1],
                preferred_element_type=jnp.float32,
            ).astype(jnp.bfloat16)
            gate = jax.nn.sigmoid(value[:block, :hw].astype(jnp.float32))
            out = (ungated[i * block : (i + 1) * block, :] * gate).astype(jnp.bfloat16)
            for e in range(2):
                act[e * span + i * half : e * span + (i + 1) * half, 0:hw] = out[
                    e * half : (e + 1) * half
                ]
            start = 8 + (i % 2) * block
            pool_buf[i // 2, start : start + block, :] = value[:block, hw:].astype(jnp.float32)
        beyond = value[block:, hw:].astype(jnp.float32)
        zero = jnp.zeros((8, feat), jnp.float32)
        for j in range(2):
            mine = beyond[j * edge_rows : (j + 1) * edge_rows]
            pool_buf[j, 0:8, :] = jnp.where(low, zero, mine[edge_rows - 8 :])
            pool_buf[j, span + 8 : span + 16, :] = jnp.where(low, mine[:8], zero)

    scoped("project_1", project_b)
    with jax.named_scope("pooling"):
        group = (c * 4 + quarter) * feat * 4 // width
        for k in range(4):

            @pl.when(group == k)
            def _(k=k):
                reach = 2 ** k
                t = h * span + lax.broadcasted_iota(jnp.int32, (span, 1), 0)
                counted = jnp.minimum(t + reach - 1, n_sp * block - 1) - jnp.maximum(t - reach, 0) + 1
                counted = counted.astype(jnp.float32)
                length = span + 16
                for j in range(2):
                    window = pool_buf[j]
                    for e in range(k + 1):
                        window = window + pltpu.roll(window, length - 2 ** e, 0)
                    if reach < 8:
                        window = pltpu.roll(window, length - (8 - reach), 0)
                    value = window[:span] / counted - pool_buf[j, 8 : 8 + span, :]
                    value = value.astype(jnp.bfloat16)
                    for i in range(4):
                        place = (i % 2) * span + (2 * j + i // 2) * half
                        act[place : place + half, hw:] = value[i * half : (i + 1) * half]

    count = give.shape[0]
    tile = width // count
    each = count // 4
    planes = (2 * h, 2 * h + 1, 2 * (1 - h), 2 * (1 - h) + 1)

    def columns_of(n):
        return at(planes[n // each] * (width // 4) + (n % each) * tile, tile)

    def mixed(n):
        return n in (3, 5, 7)

    def swap(n):
        return remote(give.at[n], take.at[n], sw_ss, sw_rs.at[n], to_c)

    def first_stage(n, slot, incoming=False):
        dst = l1.at[n, slot]
        return remote(
            dst if incoming else s1.at[n, slot], dst, r1_ss, r1_rs.at[n, slot],
            to_p if mixed(n) else to_x,
        )

    def second_stage(n, incoming=False):
        return remote(
            l2.at[n] if incoming else s2.at[n], l2.at[n], r2_ss, r2_rs.at[n],
            to_x if mixed(n) else to_p,
        )

    def product(side, n):
        return transposed_dot(act[at(side * span, span), :], w_all[2, columns_of(n), :])

    home = 2 * x + p
    both = 2 * (1 - x) + 1 - p

    def first(n):
        part_sum = product(c, n)
        swap(n).wait_recv()
        total[n] = part_sum.reshape(total.shape[1:]) + take[n].astype(jnp.float32)
        near, middle = 2 * (1 - x) + p, 2 * x + 1 - p
        if mixed(n):
            near, middle = middle, near
        s1[n, 1] = total[n, both].astype(jnp.bfloat16)
        go(first_stage(n, 1))
        s1[n, 0] = total[n, near].astype(jnp.bfloat16)
        go(first_stage(n, 0))

    def second(n):
        middle = 2 * (1 - x) + p if mixed(n) else 2 * x + 1 - p
        first_stage(n, 1, True).wait_recv()
        s2[n] = (total[n, middle] + l1[n, 1].astype(jnp.float32)).astype(jnp.bfloat16)
        go(second_stage(n))

    def last(n):
        first_stage(n, 0, True).wait_recv()
        second_stage(n, True).wait_recv()
        o_ref[:, columns_of(n)] = (
            total[n, home] + l1[n, 0].astype(jnp.float32) + l2[n].astype(jnp.float32)
        ).astype(jnp.bfloat16)

    for q in range(4):
        mine = range(q * each, (q + 1) * each)
        if q == 2:
            with jax.named_scope("second#q=1"):
                for n in range(each, 2 * each):
                    second(n)
        scoped("plane#q=%d" % q, after_y, 2, planes[q])
        with jax.named_scope("give#q=%d" % q):
            for n in mine:
                give[n] = product(other, n).astype(jnp.bfloat16).reshape(give.shape[1:])
                go(swap(n))
        with jax.named_scope("first#q=%d" % q):
            for n in mine:
                first(n)
        if q == 1:
            scoped("after_h_2", after_plane, 2, 0)
            with jax.named_scope("second#q=0"):
                for n in range(each):
                    second(n)
            scoped("after_h_2", after_plane, 2, 1)
        if q > 2:
            with jax.named_scope("second#q=%d" % (q - 1)):
                for n in mine:
                    second(n - each)
    with jax.named_scope("second#q=3"):
        for n in range(3 * each, count):
            second(n)
    with jax.named_scope("last#q=0"):
        for n in range(2 * each):
            last(n)
    with jax.named_scope("last#q=1"):
        for n in range(2 * each, count):
            last(n)

    with jax.named_scope("drain"):
        sends = (
            (w_all.at[:, 0 : 2 * rows], x_ss),
            (w_all.at[:, 0 : 2 * rows], p_ss),
            (w_all.at[:, 0 : 4 * rows], h_ss),
            (w_all.at[:, 0 : 8 * rows], y_ss),
            (x_all.at[0:half], token_p_ss),
            (x_all.at[0 : 2 * half], tx_ss),
            (x_all.at[0 : 3 * half], tw_ss),
            (give, sw_ss),
            (s1, r1_ss),
            (s2, r2_ss),
        )
        for ref, sem in sends:
            remote(ref, ref, sem, e_rs.at[0], to_x).wait_send()
        for copy in (
            decay_p(), decay_x(0), decay_x(1), init_x(0), init_x(1), message(0), message(1), edge_x()
        ):
            copy.wait_send()
        edges(lambda copy: copy.wait_send())


def by_group(
    tokens, norm_gain, query_weight, key_weight, value_weight, outgate_weight, gate_weight,
    gate_bias, decay_extra, init_memory, init_normalizer, head_gain, pool_weight, mem_out_weight,
    pool_out_weight,
):
    n_sp = lax.axis_size("sp")
    block, width = tokens.shape[1:]
    rows = query_weight.shape[0]
    hw = head_gain.shape[1]
    feat = pool_weight.shape[1] // 4
    columns = 3 * hw
    half, span, everything = block // 2, 2 * block, 4 * block
    count, pieces = 8, 4
    tile = width // count
    f32, bf16 = jnp.float32, jnp.bfloat16
    dma = pltpu.SemaphoreType.DMA
    anywhere = pl.BlockSpec(memory_space=pl.ANY)
    mixed = pl.pallas_call(
        functools.partial(layer_kernel, n_sp),
        out_shape=pltpu.VMEM((half, width), bf16),
        in_specs=[anywhere] * 15,
        out_specs=pl.BlockSpec(memory_space=pltpu.VMEM),
        scratch_shapes=[
            pltpu.VMEM((1, width), f32),
            pltpu.VMEM(gate_weight.shape, bf16),
            pltpu.SMEM(gate_bias.shape, f32),
            pltpu.VMEM(head_gain.shape, f32),
            pltpu.VMEM((everything, width), bf16),
            pltpu.VMEM((everything + 16, width), bf16),
            pltpu.VMEM((3, width, columns), bf16),
            pltpu.VMEM((3, 3, rows, columns), bf16),
            pltpu.VMEM((3, rows, columns), bf16),
            pltpu.VMEM((128, width), bf16),
            pltpu.VMEM((2, 2) + decay_extra.shape[1:], f32),
            pltpu.VMEM((2, hw, hw), f32),
            pltpu.VMEM((2,) + init_normalizer.shape[1:], f32),
            pltpu.VMEM((everything, columns), bf16),
            pltpu.VMEM((everything, hw), f32),
            pltpu.VMEM((2, span + 16, feat), f32),
            pltpu.VMEM((everything, columns), bf16),
            pltpu.VMEM((2, 2, hw, span), f32),
            pltpu.VMEM((2, 8, span), f32),
            pltpu.VMEM((2, hw, span), bf16),
            pltpu.VMEM((4, 8, block), f32),
            pltpu.VMEM((128, span), f32),
            pltpu.VMEM((span, 128), f32),
            pltpu.VMEM((2, 8, span), f32),
            pltpu.VMEM((3, 8, hw), f32),
            pltpu.VMEM((3, 8, hw), f32),
            pltpu.VMEM((2, hw, hw), bf16),
            pltpu.VMEM((2, hw, hw), bf16),
            pltpu.VMEM((2, 8, width), bf16),
            pltpu.VMEM((count, 4, half, tile), bf16),
            pltpu.VMEM((count, 4, half, tile), bf16),
            pltpu.VMEM((count, 4, half, tile), f32),
            pltpu.VMEM((count, 2, half, tile), bf16),
            pltpu.VMEM((count, 2, half, tile), bf16),
            pltpu.VMEM((count, half, tile), bf16),
            pltpu.VMEM((count, half, tile), bf16),
            dma((3, 4)),
            dma((4,)),
            dma((4,)),
            dma(()), dma((3, 2)),
            dma(()), dma((3, 2)),
            dma(()), dma((3, 2, 2)),
            dma(()), dma((6,)),
            dma(()), dma((pieces,)),
            dma(()), dma((2, pieces)),
            dma(()), dma((3,)),
            dma((3,)), dma((3,)),
            dma((2,)), dma((2,)),
            dma((2,)), dma((2,)),
            dma((3,)), dma((2,)),
            dma(()), dma((count,)),
            dma(()), dma((count, 2)),
            dma(()), dma((count,)),
        ],
        compiler_params=pltpu.CompilerParams(
            collective_id=0, has_side_effects=True, vmem_limit_bytes=60 * 2**20
        ),
        name="layer",
    )(
        tokens[0], norm_gain[None], query_weight, key_weight, value_weight, outgate_weight,
        gate_weight, gate_bias, decay_extra[0], init_memory[0], init_normalizer[0], head_gain,
        pool_weight, mem_out_weight, pool_out_weight,
    )
    return mixed[None]


def solution(mesh):
    placed = (
        P("fs", "sp", None),
        P(),
        P(("sp", "fs"), "tp"),
        P(("sp", "fs"), "tp"),
        P(("sp", "fs"), "tp"),
        P(("sp", "fs"), "tp"),
        P(None, "tp", None),
        P(None, "tp"),
        P("fs", None, "tp", "sp"),
        P("fs", None, "tp", None, None),
        P("fs", None, "tp", None),
        P("tp", None),
        P(("sp", "fs"), "tp"),
        P(("sp", "fs"), "tp"),
        P(("sp", "fs"), "tp"),
    )

    def body(*args):
        heads, width = args[11].shape
        features = args[12].shape[1]
        block, model_width = args[0].shape[1:]
        fits = (
            lax.axis_size("tp") == 2
            and lax.axis_size("fs") == 4
            and lax.axis_size("sp") == 4
            and heads == 4
            and width == 128
            and features == 8 * width
            and model_width == 2 * features
            and block == 2 * width
        )
        return (by_group if fits else per_device)(*args)

    return jax.shard_map(
        body,
        mesh=mesh,
        in_specs=placed,
        out_specs=P("fs", ("sp", "tp"), None),
        check_vma=False,
    )
```
